32 devices in a mesh: dp: 4 (over y, x), kv: 4 (over z), tp: 2 (over core).
Axes of the slice: x: 2, y: 2, z: 4, core: 2. Of those that a mesh axis runs over, the one named last changes fastest.
Arguments:
- tokens: bfloat16 [16, 4096], P('dp', 'kv'), parts along dimension 0, may hold values from -13 to 13
- norm_gain: float32 [4096], P('kv'), may hold values from 0.1 to 1.9
- query_weight: bfloat16 [4096, 2048], P('kv', 'tp'), may hold values from -0.09375 to 0.09375
- key_weight: bfloat16 [4096, 2048], P('kv', 'tp'), may hold values from -0.09375 to 0.09375
- value_weight: bfloat16 [4096, 4096], P('kv', 'tp'), may hold values from -0.09375 to 0.09375
- gate_weight: bfloat16 [4096, 2, 8], replicated, may hold values from -0.09375 to 0.09375
- forget_bias: float32 [8], P('tp'), may hold values from 0.5 to 4
- state_matrix: float32 [16, 8, 512, 256], P(('dp', 'kv'), 'tp'), parts along dimension 0, may hold values from -1.8 to 1.8
- state_normalizer: float32 [16, 8, 256], P(('dp', 'kv'), 'tp'), parts along dimension 0, may hold values from -1.2 to 1.2
- state_max: float32 [16, 8], P(('dp', 'kv'), 'tp'), parts along dimension 0, may hold values from -2 to 86
- block_keys: bfloat16 [16, 8, 64, 256], P(('dp', 'kv'), 'tp'), parts along dimension 0, may hold values from -5 to 5
- block_values: bfloat16 [16, 8, 64, 512], P(('dp', 'kv'), 'tp'), parts along dimension 0, may hold values from -5 to 5
- block_input: float32 [16, 8, 64], P(('dp', 'kv'), 'tp'), parts along dimension 0, may hold values from -4.5 to 86.5
- block_logf: float32 [16, 8, 64], P(('dp', 'kv'), 'tp'), parts along dimension 0, may hold values from -1 to 0
- lengths: int32 [16], P(('dp', 'kv')), parts along dimension 0, may hold values from 1 to 2048, 4096 in all
- out_weight: bfloat16 [4096, 4096], P('tp', 'kv'), may hold values from -0.09375 to 0.09375
- mixer_gain: float32 [4096], replicated, may hold values from 0.1 to 1.9
- up_weight: bfloat16 [8192, 4096], P(('kv', 'tp')), may hold values from -0.09375 to 0.09375
- down_weight: bfloat16 [8192, 4096], P(('kv', 'tp')), may hold values from -0.09375 to 0.09375
Outputs:
- mixed: bfloat16 [16, 4096], P('dp', ('kv', 'tp')), parts along dimension 0
The draws below stay inside these ranges and needn't reach their ends.
There are 4 independent parts, one for each index of `dp`. The reference program is written for one: setup_inputs(seed, part) draws one part's arguments, and reference() takes and returns one part's arrays. A program takes and returns all parts, laid end to end along the dimension named above; an argument that names none is the same for every part. Nothing has to cross between parts.
Inputs may be any that keep to these rules, and one draw needn't show every extreme that they name: `lengths`: each sequence's count of earlier positions; the state holds the first multiple of 64 of them and the block arrays the rest.
All inputs are finite; a program needn't handle non-finite values.
Results may differ from the reference program's by a relative error of at most 0.016.
Values may be sent and summed in bfloat16 or wider, within the bound.
No kernel may reach another device: no remote copies, remote signals or barrier semaphores. Data moves between devices by JAX's collectives and lax.ppermute only.
A program may use at most 64 MiB of HBM per device.

```python
import math
import jax
import jax.numpy as jnp
import numpy as np
from jax import lax

D = 4096
RECALL_CHANNELS = 8
DK = 256
DV = 512
FF = 8192
SPAN_LOCATIONS = 64
BATCH_STREAMS = 4
N_KV = 4


def draw_tokens(key, part):
    first = jax.random.fold_in(key, 0)
    columns = jnp.arange(D) // (D // N_KV)
    rising = 0.6 * 3.0 ** (columns.astype(jnp.float32) / max(N_KV - 1, 1))
    return (jnp.clip(jax.random.normal(first, (BATCH_STREAMS, D), jnp.float32), -5.0, 5.0) * rising[None, :]).astype(jnp.bfloat16)


def draw_state_max(key, part):
    base = jax.random.uniform(jax.random.fold_in(key, 1), (BATCH_STREAMS, RECALL_CHANNELS), jnp.float32, -2.0, 1.0)
    return base


def draw_block_input(key, part):
    noise = jax.random.normal(jax.random.fold_in(key, 2), (BATCH_STREAMS, RECALL_CHANNELS, SPAN_LOCATIONS), jnp.float32)
    return jnp.clip(noise, -4.5, 4.5)


def draw_block_logf(key, part):
    address_entries = jax.random.split(key, 6)
    quick = 0.5
    fast = jax.random.bernoulli(address_entries[0], quick, (1, RECALL_CHANNELS, 1))
    fast_rate = jnp.exp(jax.random.uniform(address_entries[1], (1, RECALL_CHANNELS, 1), jnp.float32, jnp.log(0.02), jnp.log(0.04)))
    slow_rate = jnp.exp(jax.random.uniform(address_entries[2], (1, RECALL_CHANNELS, 1), jnp.float32, jnp.log(0.001), jnp.log(0.004)))
    fading_factor = jnp.where(fast, fast_rate, slow_rate)
    per_stream_order = jnp.exp(jax.random.uniform(address_entries[3], (BATCH_STREAMS, 1, 1), jnp.float32, -0.7, 0.7))
    approximate_guess = jax.random.uniform(address_entries[4], (BATCH_STREAMS, RECALL_CHANNELS, SPAN_LOCATIONS), jnp.float32, 0.5, 1.5)
    symbol_cluster = jax.random.bernoulli(address_entries[5], 2.0 / SPAN_LOCATIONS, (BATCH_STREAMS, RECALL_CHANNELS, SPAN_LOCATIONS))
    generation_error = jnp.log(jax.random.uniform(jax.random.fold_in(key, 9), (BATCH_STREAMS, RECALL_CHANNELS, SPAN_LOCATIONS), jnp.float32, 0.5, 0.8))
    return -fading_factor * per_stream_order * approximate_guess + jnp.where(symbol_cluster, generation_error, 0.0)


def spiked(values, own_key, source, target, blocks, factor):
    owner, partner = [(jnp.arange(values.shape[axis_at]) // (values.shape[axis_at] // blocks)).reshape([-1 if axis == axis_at else 1 for axis in range(values.ndim)]) for axis_at in (source, target)]
    chosen = jax.random.permutation(own_key, blocks)[partner]
    strong = (owner == chosen) | (owner == (partner + blocks // 2) % blocks)
    return jnp.where(strong, factor * values, values)


def steps_of(stream_key, shape, cuts, low, top_value):
    def one(dim, parts):
        heights = jax.random.uniform(jax.random.fold_in(jax.random.fold_in(stream_key, 6), dim), (parts,), jnp.float32, low / len(cuts), top_value / len(cuts))
        return jnp.repeat(jnp.exp(heights), shape[dim] // parts).reshape((-1,) + (1,) * (len(shape) - dim - 1))

    gain = one(*cuts[0])
    for cut in cuts[1:]:
        gain = gain * one(*cut)
    return gain


def split_up(number_of, total, bound, slope):
    weights = [(1 << 20) // math.isqrt(standing ** slope) + 1 for standing in range(2, number_of + 1)]
    surplus, holding = total - bound - (number_of - 1), [1] * (number_of - 1)
    while surplus > 0:
        free = [i for i in range(number_of - 1) if holding[i] < bound]
        mass, remaining = sum([weights[i] for i in free]), surplus
        for i in free:
            extra = min(bound - holding[i], max(1, remaining * weights[i] // mass), surplus)
            holding[i] = holding[i] + extra
            surplus = surplus - extra
    return np.array([bound] + holding)


def uneven_parts(stream_key, count, total, bound, slope):
    if count == 2:
        one = jax.random.randint(stream_key, (), max(1, total - bound), min(bound, total - 1) + 1)
        return jnp.stack([one, total - one])
    sizes = jnp.asarray(split_up(count, total, bound, slope), jnp.int32)
    twos = (count - 1) // 2
    source_of, sink = sizes[1:1 + 2 * twos:2], sizes[2:2 + 2 * twos:2]
    room = jnp.minimum(source_of - 1, bound - sink)
    passed = jax.random.randint(jax.random.fold_in(stream_key, 1), (twos,), 0, 1 << 20) % (room + 1)
    sizes = sizes.at[1:1 + 2 * twos:2].set(source_of - passed).at[2:2 + 2 * twos:2].set(sink + passed)
    return sizes[jax.random.permutation(jax.random.fold_in(stream_key, 2), count)]


def normal_values(own_key, shape, spread, bound, cuts=(), kind=jnp.bfloat16):
    result = spread * jax.random.normal(own_key, shape, jnp.float32)
    if cuts:
        result = result * steps_of(own_key, shape, cuts, -0.22, 0.18)
    return jnp.clip(result, -bound, bound).astype(kind)


def noise_with(own_key, extent, width, limit, pieces, heavy, held_as=jnp.bfloat16):
    array = width * jax.random.normal(own_key, extent, jnp.float32)
    if pieces:
        array = array * steps_of(own_key, extent, pieces, -0.22, 0.18)
    return jnp.clip(spiked(array, jax.random.fold_in(own_key, 3), *heavy), -limit, limit).astype(held_as)


def setup_inputs(seed: int = 0, part: int = 0) -> dict:
    key_of = jax.random.split(jax.random.key(seed), 20)
    part_keys = jax.random.split(jax.random.fold_in(key_of[19], part), 20)
    tokens = draw_tokens(jax.random.fold_in(jax.random.fold_in(key_of[19], part), 71), part)
    norm_gain = jnp.clip(1.0 + 0.18 * jax.random.normal(key_of[1], (D,), jnp.float32), 0.1, 1.9)
    query_weight = normal_values(key_of[2], (D, RECALL_CHANNELS * DK), D ** -0.5, 0.09375, ((0, 4), (1, 2)))
    key_weight = normal_values(key_of[3], (D, RECALL_CHANNELS * DK), D ** -0.5, 0.09375, ((0, 4), (1, 2)))
    value_weight = normal_values(key_of[4], (D, RECALL_CHANNELS * DV), D ** -0.5, 0.09375, ((0, 4), (1, 2)))
    gate_weight = normal_values(key_of[5], (D, 2, RECALL_CHANNELS), D ** -0.5, 0.09375)
    forget_bias = jnp.clip(0.5 + 3.5 * jax.random.uniform(key_of[6], (RECALL_CHANNELS,), jnp.float32) ** steps_of(key_of[6], (RECALL_CHANNELS,), ((0, 2),), -0.2, 0.2), 0.5, 4.0)
    state_matrix = normal_values(part_keys[7], (BATCH_STREAMS, RECALL_CHANNELS, DV, DK), 0.3, 1.8, ((0, 4), (1, 2)), jnp.float32)
    state_normalizer = normal_values(part_keys[8], (BATCH_STREAMS, RECALL_CHANNELS, DK), 0.2, 1.2, ((0, 4), (1, 2)), jnp.float32)
    state_max = draw_state_max(jax.random.fold_in(jax.random.fold_in(key_of[19], part), 71), part)
    block_keys = normal_values(part_keys[10], (BATCH_STREAMS, RECALL_CHANNELS, SPAN_LOCATIONS, DK), 1.0, 5.0, ((0, 4), (1, 2)))
    block_values = normal_values(part_keys[11], (BATCH_STREAMS, RECALL_CHANNELS, SPAN_LOCATIONS, DV), 1.0, 5.0, ((0, 4), (1, 2)))
    block_input = draw_block_input(jax.random.fold_in(jax.random.fold_in(key_of[19], part), 71), part)
    block_logf = draw_block_logf(jax.random.fold_in(jax.random.fold_in(key_of[19], part), 71), part)
    lengths = uneven_parts(part_keys[14], BATCH_STREAMS, BATCH_STREAMS * 1024, min(8192, BATCH_STREAMS * 512), 2).astype(jnp.int32)
    out_weight = normal_values(key_of[15], (RECALL_CHANNELS * DV, D), (RECALL_CHANNELS * DV) ** -0.5, 0.09375, ((0, 2), (1, 4)))
    mixer_gain = jnp.clip(1.0 + 0.18 * jax.random.normal(key_of[16], (D,), jnp.float32), 0.1, 1.9)
    up_weight = normal_values(key_of[17], (FF, D), D ** -0.5, 0.09375, ((0, 8),))
    down_weight = noise_with(key_of[18], (FF, D), FF ** -0.5, 0.09375, ((0, 8),), (0, 1, 8, 2.0))
    return {"tokens": tokens, "norm_gain": norm_gain, "query_weight": query_weight, "key_weight": key_weight, "value_weight": value_weight, "gate_weight": gate_weight, "forget_bias": forget_bias, "state_matrix": state_matrix, "state_normalizer": state_normalizer, "state_max": state_max, "block_keys": block_keys, "block_values": block_values, "block_input": block_input, "block_logf": block_logf, "lengths": lengths, "out_weight": out_weight, "mixer_gain": mixer_gain, "up_weight": up_weight, "down_weight": down_weight}


epsilon = 1e-06
highest = lax.Precision.HIGHEST

def memory_cell(query, key, value, gates, forget_bias, state_matrix, state_normalizer, state_max, block_keys, block_values, block_input, block_logf, lengths):
    live = lengths % SPAN_LOCATIONS
    positions = jnp.arange(SPAN_LOCATIONS, dtype=jnp.int32)[None, None, :]
    inside = positions < live[:, None, None]
    new_input = gates[:, 0]
    new_logf = jax.nn.log_sigmoid(gates[:, 1] + forget_bias)
    cumulative = jnp.cumsum(jnp.where(inside, block_logf, jnp.float32(0.0)), axis=2)
    total = cumulative[:, :, -1] + new_logf
    carried_log = total + state_max
    cache_log = jnp.where(inside, total[:, :, None] - cumulative + block_input, -jnp.inf)
    stable = jnp.maximum(jnp.maximum(carried_log, lax.optimization_barrier(jnp.max(cache_log, axis=2))), new_input)
    carried_weight = jnp.exp(carried_log - stable)
    new_weight = jnp.exp(new_input - stable)
    cache_weight = jnp.exp(cache_log - stable[:, :, None])
    query_wide = query.astype(jnp.float32)
    scores = jnp.einsum('bhk,bhsk->bhs', query_wide, block_keys.astype(jnp.float32), precision=highest)
    mixing = (scores * DK ** (-0.5) * cache_weight).astype(jnp.bfloat16)
    own_term = lax.optimization_barrier(jnp.sum(query_wide * key.astype(jnp.float32), axis=2)) * DK ** (-0.5) * new_weight
    carried = jnp.einsum('bhvk,bhk->bhv', state_matrix, query_wide, precision=highest)
    from_cache = jnp.einsum('bhs,bhsv->bhv', mixing.astype(jnp.float32), block_values.astype(jnp.float32), precision=highest)
    numerator = carried_weight[:, :, None] * carried + from_cache + own_term[:, :, None] * value.astype(jnp.float32)
    normalizer = carried_weight * lax.optimization_barrier(jnp.sum(state_normalizer * query_wide, axis=2)) + lax.optimization_barrier(jnp.sum(mixing.astype(jnp.float32), axis=2)) + own_term
    divisor = jnp.maximum(jnp.maximum(jnp.abs(normalizer), jnp.exp(-stable)), jnp.float32(1.0))
    hidden = numerator / divisor[:, :, None]
    return hidden.astype(jnp.bfloat16)

def reference(tokens, norm_gain, query_weight, key_weight, value_weight, gate_weight, forget_bias, state_matrix, state_normalizer, state_max, block_keys, block_values, block_input, block_logf, lengths, out_weight, mixer_gain, up_weight, down_weight):
    widened = tokens.astype(jnp.float32)
    squares = lax.optimization_barrier(jnp.sum(widened * widened, axis=1))
    normed = (widened * norm_gain).astype(jnp.bfloat16)
    row_scale = lax.rsqrt(squares / D + epsilon)[:, None]
    query = (jnp.dot(normed, query_weight, preferred_element_type=jnp.float32) * row_scale).astype(jnp.bfloat16)
    key = (jnp.dot(normed, key_weight, preferred_element_type=jnp.float32) * row_scale).astype(jnp.bfloat16)
    value = (jnp.dot(normed, value_weight, preferred_element_type=jnp.float32) * row_scale).astype(jnp.bfloat16)
    gates = jnp.dot(normed, gate_weight.reshape(D, 2 * RECALL_CHANNELS), preferred_element_type=jnp.float32) * row_scale
    hidden = memory_cell(query.reshape(BATCH_STREAMS, RECALL_CHANNELS, DK), key.reshape(BATCH_STREAMS, RECALL_CHANNELS, DK), value.reshape(BATCH_STREAMS, RECALL_CHANNELS, DV), gates.reshape(BATCH_STREAMS, 2, RECALL_CHANNELS), forget_bias, state_matrix, state_normalizer, state_max, block_keys, block_values, block_input, block_logf, lengths)
    flat = hidden.reshape(BATCH_STREAMS, RECALL_CHANNELS * DV)
    group = RECALL_CHANNELS * DV // 2
    attended = jnp.zeros((BATCH_STREAMS, D), jnp.float32)
    for half in range(2):
        part_out = jnp.dot(flat[:, half * group:(half + 1) * group], out_weight[half * group:(half + 1) * group], preferred_element_type=jnp.float32).astype(jnp.bfloat16)
        attended = attended + part_out.astype(jnp.float32)
    residual = (widened + attended).astype(jnp.bfloat16)
    resid_wide = residual.astype(jnp.float32)
    mixer_squares = lax.optimization_barrier(jnp.sum(resid_wide * resid_wide, axis=1))
    mixer_in = (resid_wide * mixer_gain).astype(jnp.bfloat16)
    preact = jnp.dot(mixer_in, up_weight.T, preferred_element_type=jnp.float32) * lax.rsqrt(mixer_squares / D + epsilon)[:, None]
    activated = jnp.square(jax.nn.relu(preact)).astype(jnp.bfloat16)
    return (resid_wide + jnp.dot(activated, down_weight, preferred_element_type=jnp.float32)).astype(jnp.bfloat16)
```

```python
import jax
import jax.numpy as jnp
from jax import lax
from jax.sharding import PartitionSpec as P

D = 4096
DK = 256
DV = 512
SPAN_LOCATIONS = 64


epsilon = 1e-06
highest = lax.Precision.HIGHEST


def memory_cell(
    query,
    key,
    value,
    gates,
    forget_bias,
    state_matrix,
    state_normalizer,
    state_max,
    block_keys,
    block_values,
    block_input,
    block_logf,
    lengths,
):
    live = lengths % SPAN_LOCATIONS
    positions = lax.broadcasted_iota(jnp.int32, (1, 1, SPAN_LOCATIONS), 2)
    inside = positions < live[:, None, None]
    new_input = gates[:, 0]
    new_logf = jax.nn.log_sigmoid(gates[:, 1] + forget_bias)
    cumulative = jnp.cumsum(jnp.where(inside, block_logf, jnp.float32(0.0)), axis=2)
    total = cumulative[:, :, -1] + new_logf
    carried_log = total + state_max
    cache_log = jnp.where(inside, total[:, :, None] - cumulative + block_input, -jnp.inf)
    stable = jnp.maximum(jnp.maximum(carried_log, jnp.max(cache_log, axis=2)), new_input)
    carried_weight = jnp.exp(carried_log - stable)
    new_weight = jnp.exp(new_input - stable)
    cache_weight = jnp.exp(cache_log - stable[:, :, None])
    scores = jnp.einsum("bhk,bhsk->bhs", query, block_keys, preferred_element_type=jnp.float32)
    mixing = (scores * DK ** (-0.5) * cache_weight).astype(jnp.bfloat16)
    query_wide = query.astype(jnp.float32)
    own_term = jnp.sum(query_wide * key.astype(jnp.float32), axis=2) * DK ** (-0.5) * new_weight
    carried = jnp.einsum("bhvk,bhk->bhv", state_matrix, query_wide, precision=highest)
    from_cache = jnp.einsum(
        "bhs,bhsv->bhv", mixing, block_values, preferred_element_type=jnp.float32
    )
    numerator = (
        carried_weight[:, :, None] * carried
        + from_cache
        + own_term[:, :, None] * value.astype(jnp.float32)
    )
    normalizer = (
        carried_weight * jnp.sum(state_normalizer * query_wide, axis=2)
        + jnp.sum(mixing.astype(jnp.float32), axis=2)
        + own_term
    )
    divisor = jnp.maximum(jnp.maximum(jnp.abs(normalizer), jnp.exp(-stable)), jnp.float32(1.0))
    hidden = numerator / divisor[:, :, None]
    return hidden.astype(jnp.bfloat16)


def absorb_columns(mixer_gain, up_weight):

    def absorb(carry, piece, start):
        widened = piece.astype(jnp.float32)
        mixer_in = (widened * mixer_gain).astype(jnp.bfloat16)
        product = lax.dot_general(
            mixer_in, up_weight, (((1,), (1,)), ((), ())), preferred_element_type=jnp.float32
        )
        return (product, jnp.sum(widened * widened, axis=1))

    return absorb


def down_terms(carry, down_weight):
    accumulated, squares = carry
    scaled = accumulated * lax.rsqrt(squares / D + epsilon)[:, None]
    activated = jnp.square(jax.nn.relu(scaled)).astype(jnp.bfloat16)
    return jnp.dot(activated, down_weight, preferred_element_type=jnp.float32)


DIRECT_LIMIT = 8


def partner_pairs(size, distance):
    if size & (size - 1) == 0:
        return [(i, i ^ distance) for i in range(size)]
    return [(i, (i + distance) % size) for i in range(size)]


def partner_of(position, size, distance, receiving):
    if size & (size - 1) == 0:
        return position ^ distance
    return (position - distance) % size if receiving else (position + distance) % size


def gather_direct(piece, axis):
    size = lax.axis_size(axis)
    if size > DIRECT_LIMIT:
        return lax.all_gather(piece, axis, axis=0)
    position = lax.axis_index(axis)
    received = [piece] + [
        lax.ppermute(piece, axis, partner_pairs(size, d)) for d in range(1, size)
    ]
    stacked = jnp.stack(received)
    places = jnp.arange(size)
    if size & (size - 1) == 0:
        order = position ^ places
    else:
        order = (position - places) % size
    return stacked[order]


def scatter_sum_direct(parts, axis):
    size = lax.axis_size(axis)
    if size > DIRECT_LIMIT:
        return lax.psum_scatter(parts, axis, scatter_dimension=0, tiled=False)
    position = lax.axis_index(axis)

    def entry(index):
        return lax.dynamic_index_in_dim(parts, index, 0, keepdims=False)

    total = entry(position)
    for d in range(1, size):
        out = entry(partner_of(position, size, d, False))
        total = total + lax.ppermute(out, axis, partner_pairs(size, d))
    return total


def shards(
    tokens,
    norm_gain,
    query_weight,
    key_weight,
    value_weight,
    gate_weight,
    forget_bias,
    state_matrix,
    state_normalizer,
    state_max,
    block_keys,
    block_values,
    block_input,
    block_logf,
    lengths,
    out_weight,
    mixer_gain,
    up_weight,
    down_weight,
):
    position = lax.axis_index("kv")
    head_half = lax.axis_index("tp")
    columns = tokens.shape[1]
    local_heads = forget_bias.shape[0]
    local_rows = lengths.shape[0]
    widened = tokens.astype(jnp.float32)
    squares = jnp.sum(widened * widened, axis=1)
    normed = (widened * norm_gain).astype(jnp.bfloat16)
    gate_rows = lax.dynamic_slice_in_dim(gate_weight, position * columns, columns, 0)
    gate_rows = lax.dynamic_slice_in_dim(
        gate_rows, head_half * local_heads, local_heads, 2
    ).reshape(columns, 2 * local_heads)
    query_part = jnp.dot(normed, query_weight, preferred_element_type=jnp.float32)
    key_part = jnp.dot(normed, key_weight, preferred_element_type=jnp.float32)
    value_part = jnp.dot(normed, value_weight, preferred_element_type=jnp.float32)
    gate_part = jnp.dot(normed, gate_rows, preferred_element_type=jnp.float32)
    parts = jnp.concatenate(
        [query_part, key_part, value_part, gate_part, squares[:, None]], axis=1
    )
    parts = parts.reshape(-1, local_rows, parts.shape[1])
    sums = scatter_sum_direct(parts, "kv")
    q_end = query_part.shape[1]
    k_end = q_end + key_part.shape[1]
    v_end = k_end + value_part.shape[1]
    g_end = v_end + gate_part.shape[1]
    query_sum, key_sum, value_sum, gate_sum, own_squares = (
        sums[:, :q_end],
        sums[:, q_end:k_end],
        sums[:, k_end:v_end],
        sums[:, v_end:g_end],
        sums[:, g_end],
    )
    row_scale = lax.rsqrt(own_squares / D + epsilon)[:, None]
    query = (query_sum * row_scale).astype(jnp.bfloat16).reshape(local_rows, local_heads, DK)
    key = (key_sum * row_scale).astype(jnp.bfloat16).reshape(local_rows, local_heads, DK)
    value = (value_sum * row_scale).astype(jnp.bfloat16).reshape(local_rows, local_heads, DV)
    gates = (gate_sum * row_scale).reshape(local_rows, 2, local_heads)
    hidden = memory_cell(
        query,
        key,
        value,
        gates,
        forget_bias,
        state_matrix,
        state_normalizer,
        state_max,
        block_keys,
        block_values,
        block_input,
        block_logf,
        lengths,
    )
    hidden = hidden.reshape(local_rows, local_heads * DV)
    every_hidden = gather_direct(hidden, "kv").reshape(-1, hidden.shape[1])
    partial_out = jnp.dot(
        every_hidden, out_weight, preferred_element_type=jnp.float32
    ).astype(jnp.bfloat16)
    attended = jnp.sum(gather_direct(partial_out, "tp").astype(jnp.float32), axis=0)
    residual = (widened + attended).astype(jnp.bfloat16)
    absorb = absorb_columns(mixer_gain, up_weight)
    hidden_units = up_weight.shape[0]
    rows = residual.shape[0]
    initial = (jnp.zeros((rows, hidden_units), jnp.float32), jnp.zeros((rows,), jnp.float32))
    pieces = gather_direct(residual, "kv")
    whole = jnp.moveaxis(pieces, 0, 1).reshape(rows, -1)
    carry = absorb(initial, whole, jnp.int32(0))
    terms = down_terms(carry, down_weight)
    share = columns // lax.axis_size("tp")
    terms = terms.reshape(rows, -1, lax.axis_size("tp"), share)
    by_core = scatter_sum_direct(jnp.moveaxis(terms, 2, 0), "tp")
    mixed_terms = scatter_sum_direct(jnp.moveaxis(by_core, 1, 0), "kv")
    own_residual = lax.dynamic_slice_in_dim(residual, head_half * share, share, 1)
    return (own_residual.astype(jnp.float32) + mixed_terms).astype(jnp.bfloat16)


def solution(mesh):
    return jax.shard_map(
        shards,
        mesh=mesh,
        in_specs=(
            P("dp", "kv"),
            P("kv"),
            P("kv", "tp"),
            P("kv", "tp"),
            P("kv", "tp"),
            P(),
            P("tp"),
            P(("dp", "kv"), "tp", None, None),
            P(("dp", "kv"), "tp", None),
            P(("dp", "kv"), "tp"),
            P(("dp", "kv"), "tp", None, None),
            P(("dp", "kv"), "tp", None, None),
            P(("dp", "kv"), "tp", None),
            P(("dp", "kv"), "tp", None),
            P(("dp", "kv")),
            P("tp", "kv"),
            P(),
            P(("kv", "tp"), None),
            P(("kv", "tp"), None),
        ),
        out_specs=P("dp", ("kv", "tp")),
        check_vma=False,
    )
```

```python
import jax
import jax.numpy as jnp
from jax import lax
from jax.experimental import pallas as pl
from jax.experimental.pallas import tpu as pltpu
from jax.sharding import PartitionSpec as P

D = 4096
DK = 256
DV = 512
SPAN_LOCATIONS = 64


epsilon = 1e-06
highest = lax.Precision.HIGHEST


def memory_cell(
    query,
    key,
    value,
    gates,
    forget_bias,
    state_matrix,
    state_normalizer,
    state_max,
    block_keys,
    block_values,
    block_input,
    block_logf,
    lengths,
):
    live = lengths % SPAN_LOCATIONS
    positions = lax.broadcasted_iota(jnp.int32, (1, 1, SPAN_LOCATIONS), 2)
    inside = positions < live[:, None, None]
    new_input = gates[:, 0]
    new_logf = jax.nn.log_sigmoid(gates[:, 1] + forget_bias)
    cumulative = jnp.cumsum(jnp.where(inside, block_logf, jnp.float32(0.0)), axis=2)
    total = cumulative[:, :, -1] + new_logf
    carried_log = total + state_max
    cache_log = jnp.where(inside, total[:, :, None] - cumulative + block_input, -jnp.inf)
    stable = jnp.maximum(jnp.maximum(carried_log, jnp.max(cache_log, axis=2)), new_input)
    carried_weight = jnp.exp(carried_log - stable)
    new_weight = jnp.exp(new_input - stable)
    cache_weight = jnp.exp(cache_log - stable[:, :, None])
    scores = jnp.einsum("bhk,bhsk->bhs", query, block_keys, preferred_element_type=jnp.float32)
    mixing = (scores * DK ** (-0.5) * cache_weight).astype(jnp.bfloat16)
    query_wide = query.astype(jnp.float32)
    own_term = jnp.sum(query_wide * key.astype(jnp.float32), axis=2) * DK ** (-0.5) * new_weight
    carried = jnp.einsum("bhvk,bhk->bhv", state_matrix, query_wide, precision=highest)
    from_cache = jnp.einsum(
        "bhs,bhsv->bhv", mixing, block_values, preferred_element_type=jnp.float32
    )
    numerator = (
        carried_weight[:, :, None] * carried
        + from_cache
        + own_term[:, :, None] * value.astype(jnp.float32)
    )
    normalizer = (
        carried_weight * jnp.sum(state_normalizer * query_wide, axis=2)
        + jnp.sum(mixing.astype(jnp.float32), axis=2)
        + own_term
    )
    divisor = jnp.maximum(jnp.maximum(jnp.abs(normalizer), jnp.exp(-stable)), jnp.float32(1.0))
    hidden = numerator / divisor[:, :, None]
    return hidden.astype(jnp.bfloat16)


def absorb_columns(mixer_gain, up_weight):

    def absorb(carry, piece, start):
        widened = piece.astype(jnp.float32)
        mixer_in = (widened * mixer_gain).astype(jnp.bfloat16)
        product = lax.dot_general(
            mixer_in, up_weight, (((1,), (1,)), ((), ())), preferred_element_type=jnp.float32
        )
        return (product, jnp.sum(widened * widened, axis=1))

    return absorb


def down_terms(carry, down_weight):
    accumulated, squares = carry
    scaled = accumulated * lax.rsqrt(squares / D + epsilon)[:, None]
    activated = jnp.square(jax.nn.relu(scaled)).astype(jnp.bfloat16)
    return jnp.dot(activated, down_weight, preferred_element_type=jnp.float32)


DIRECT_LIMIT = 8


def partner_pairs(size, distance):
    if size & (size - 1) == 0:
        return [(i, i ^ distance) for i in range(size)]
    return [(i, (i + distance) % size) for i in range(size)]


def partner_of(position, size, distance, receiving):
    if size & (size - 1) == 0:
        return position ^ distance
    return (position - distance) % size if receiving else (position + distance) % size


def gather_direct(piece, axis):
    size = lax.axis_size(axis)
    if size > DIRECT_LIMIT:
        return lax.all_gather(piece, axis, axis=0)
    position = lax.axis_index(axis)
    received = [piece] + [
        lax.ppermute(piece, axis, partner_pairs(size, d)) for d in range(1, size)
    ]
    stacked = jnp.stack(received)
    places = jnp.arange(size)
    if size & (size - 1) == 0:
        order = position ^ places
    else:
        order = (position - places) % size
    return stacked[order]


def scatter_sum_direct(parts, axis):
    size = lax.axis_size(axis)
    if size > DIRECT_LIMIT:
        return lax.psum_scatter(parts, axis, scatter_dimension=0, tiled=False)
    position = lax.axis_index(axis)

    def entry(index):
        return lax.dynamic_index_in_dim(parts, index, 0, keepdims=False)

    total = entry(position)
    for d in range(1, size):
        out = entry(partner_of(position, size, d, False))
        total = total + lax.ppermute(out, axis, partner_pairs(size, d))
    return total


def shards_general(
    tokens,
    norm_gain,
    query_weight,
    key_weight,
    value_weight,
    gate_weight,
    forget_bias,
    state_matrix,
    state_normalizer,
    state_max,
    block_keys,
    block_values,
    block_input,
    block_logf,
    lengths,
    out_weight,
    mixer_gain,
    up_weight,
    down_weight,
):
    position = lax.axis_index("kv")
    head_half = lax.axis_index("tp")
    columns = tokens.shape[1]
    local_heads = forget_bias.shape[0]
    local_rows = lengths.shape[0]
    widened = tokens.astype(jnp.float32)
    squares = jnp.sum(widened * widened, axis=1)
    normed = (widened * norm_gain).astype(jnp.bfloat16)
    gate_rows = lax.dynamic_slice_in_dim(gate_weight, position * columns, columns, 0)
    gate_rows = lax.dynamic_slice_in_dim(
        gate_rows, head_half * local_heads, local_heads, 2
    ).reshape(columns, 2 * local_heads)
    query_part = jnp.dot(normed, query_weight, preferred_element_type=jnp.float32)
    key_part = jnp.dot(normed, key_weight, preferred_element_type=jnp.float32)
    value_part = jnp.dot(normed, value_weight, preferred_element_type=jnp.float32)
    gate_part = jnp.dot(normed, gate_rows, preferred_element_type=jnp.float32)
    parts = jnp.concatenate(
        [query_part, key_part, value_part, gate_part, squares[:, None]], axis=1
    )
    parts = parts.reshape(-1, local_rows, parts.shape[1])
    sums = scatter_sum_direct(parts, "kv")
    q_end = query_part.shape[1]
    k_end = q_end + key_part.shape[1]
    v_end = k_end + value_part.shape[1]
    g_end = v_end + gate_part.shape[1]
    query_sum, key_sum, value_sum, gate_sum, own_squares = (
        sums[:, :q_end],
        sums[:, q_end:k_end],
        sums[:, k_end:v_end],
        sums[:, v_end:g_end],
        sums[:, g_end],
    )
    row_scale = lax.rsqrt(own_squares / D + epsilon)[:, None]
    query = (query_sum * row_scale).astype(jnp.bfloat16).reshape(local_rows, local_heads, DK)
    key = (key_sum * row_scale).astype(jnp.bfloat16).reshape(local_rows, local_heads, DK)
    value = (value_sum * row_scale).astype(jnp.bfloat16).reshape(local_rows, local_heads, DV)
    gates = (gate_sum * row_scale).reshape(local_rows, 2, local_heads)
    hidden = memory_cell(
        query,
        key,
        value,
        gates,
        forget_bias,
        state_matrix,
        state_normalizer,
        state_max,
        block_keys,
        block_values,
        block_input,
        block_logf,
        lengths,
    )
    hidden = hidden.reshape(local_rows, local_heads * DV)
    every_hidden = gather_direct(hidden, "kv").reshape(-1, hidden.shape[1])
    partial_out = jnp.dot(
        every_hidden, out_weight, preferred_element_type=jnp.float32
    ).astype(jnp.bfloat16)
    attended = jnp.sum(gather_direct(partial_out, "tp").astype(jnp.float32), axis=0)
    residual = (widened + attended).astype(jnp.bfloat16)
    absorb = absorb_columns(mixer_gain, up_weight)
    hidden_units = up_weight.shape[0]
    rows = residual.shape[0]
    initial = (jnp.zeros((rows, hidden_units), jnp.float32), jnp.zeros((rows,), jnp.float32))
    pieces = gather_direct(residual, "kv")
    whole = jnp.moveaxis(pieces, 0, 1).reshape(rows, -1)
    carry = absorb(initial, whole, jnp.int32(0))
    terms = down_terms(carry, down_weight)
    share = columns // lax.axis_size("tp")
    terms = terms.reshape(rows, -1, lax.axis_size("tp"), share)
    by_core = scatter_sum_direct(jnp.moveaxis(terms, 2, 0), "tp")
    mixed_terms = scatter_sum_direct(jnp.moveaxis(by_core, 1, 0), "kv")
    own_residual = lax.dynamic_slice_in_dim(residual, head_half * share, share, 1)
    return (own_residual.astype(jnp.float32) + mixed_terms).astype(jnp.bfloat16)


def dot_nt(left, right):
    return lax.dot_general(
        left, right, (((1,), (1,)), ((), ())), preferred_element_type=jnp.float32
    )


VMEM_SPEC = pl.BlockSpec(memory_space=pltpu.VMEM)
SMEM_SPEC = pl.BlockSpec(memory_space=pltpu.SMEM)
ANY_SPEC = pl.BlockSpec(memory_space=pl.ANY)


def call(body, outs, in_specs, args, scratch=(), limit=8, flops=20000000000, name=None):
    return pl.pallas_call(
        body,
        out_shape=outs,
        in_specs=in_specs,
        out_specs=[VMEM_SPEC] * len(outs),
        scratch_shapes=list(scratch),
        compiler_params=pltpu.CompilerParams(vmem_limit_bytes=limit << 20),
        cost_estimate=pl.CostEstimate(flops=flops, bytes_accessed=1000000, transcendentals=0),
        name=name,
    )(*args)


def resident(weight):
    return pltpu.with_memory_space_constraint(weight, pltpu.VMEM)


def streamed(weight):
    return pltpu.with_memory_space_constraint(weight, pltpu.HBM)


def struct(shape, kind):
    return jax.ShapeDtypeStruct(shape, kind)


LANES = 128


def project(tokens, norm_gain, query_weight, key_weight, value_weight, gate_weight):
    rows, columns = tokens.shape
    size = lax.axis_size("kv")
    weights = (query_weight, key_weight, value_weight)
    widths = [w.shape[1] for w in weights]
    starts = [sum(widths[:i]) for i in range(3)]
    width = sum(widths)
    gate_count = gate_weight.shape[1] * gate_weight.shape[2]
    gates = jnp.transpose(gate_weight, (1, 2, 0)).reshape(gate_count, -1)
    chunks = 4 if columns % 512 == 0 else 1
    chunk = columns // chunks

    def body(tokens_ref, gain_ref, q_hbm, k_hbm, v_hbm, gate_hbm, *rest):
        outs = rest[:size]
        q_ref, k_ref, v_ref, gate_ref, sums_ref, sems, gate_sem = rest[size:]
        position = lax.axis_index("kv")
        gate_copy = pltpu.make_async_copy(
            gate_hbm.at[:, pl.ds(pl.multiple_of(position * columns, columns), columns)],
            gate_ref,
            gate_sem,
        )
        copies = []
        for c in range(chunks):
            at = pl.ds(c * chunk, chunk)
            for w, (source, target) in enumerate(
                ((q_hbm, q_ref), (k_hbm, k_ref), (v_hbm, v_ref))
            ):
                copy = pltpu.make_async_copy(source.at[at, :], target.at[at, :], sems.at[c, w])
                copy.start()
                copies.append(copy)
            if c == 0:
                gate_copy.start()
        widened = tokens_ref[...].astype(jnp.float32)
        squares = jnp.sum(widened * widened, axis=1, keepdims=True)
        normed = (widened * gain_ref[...]).astype(jnp.bfloat16)
        sums = [jnp.zeros((rows, n), jnp.float32) for n in widths]
        for c in range(chunks):
            piece = normed[:, c * chunk : (c + 1) * chunk]
            for w, ref in enumerate((q_ref, k_ref, v_ref)):
                copies[3 * c + w].wait()
                sums[w] = sums[w] + jnp.dot(
                    piece,
                    ref[c * chunk : (c + 1) * chunk, :],
                    preferred_element_type=jnp.float32,
                )
        gate_copy.wait()
        gate_sums = dot_nt(normed, gate_ref[...])
        pad = jnp.zeros((rows, LANES - gate_count), jnp.float32)
        extra = jnp.concatenate([gate_sums, pad], axis=1)
        lane = lax.broadcasted_iota(jnp.int32, (rows, LANES), 1)
        extra = jnp.where(lane == gate_count, squares, extra)
        for w in range(3):
            sums_ref[:, starts[w] : starts[w] + widths[w]] = sums[w]
        sums_ref[:, width:] = extra
        for d in range(size):
            outs[d][...] = sums_ref[pl.ds(partner_of(position, size, d, False), 1), :]

    return call(
        body,
        [struct((1, width + LANES), jnp.float32)] * size,
        [VMEM_SPEC, VMEM_SPEC] + [ANY_SPEC] * 4,
        (tokens, norm_gain.reshape(1, -1), *[streamed(w) for w in weights], streamed(gates)),
        [pltpu.VMEM(w.shape, w.dtype) for w in weights]
        + [
            pltpu.VMEM((gate_count, columns), gates.dtype),
            pltpu.VMEM((rows, width + LANES), jnp.float32),
            pltpu.SemaphoreType.DMA((chunks, 3)),
            pltpu.SemaphoreType.DMA(()),
        ],
        limit=16,
        name="project",
    )


def recall(
    parts,
    forget_bias,
    state_matrix,
    state_normalizer,
    state_max,
    block_keys,
    block_values,
    block_input,
    block_logf,
    lengths,
):
    _, heads, dv, dk = state_matrix.shape
    all_heads = heads * lax.axis_size("tp")
    scale = dk ** (-0.5)
    count = len(parts)

    def body(*refs):
        (
            bias_ref,
            state_ref,
            normalizer_ref,
            max_ref,
            keys_ref,
            values_ref,
            input_ref,
            logf_ref,
            lengths_ref,
            out_ref,
        ) = refs[count:]
        half = lax.axis_index("tp")
        row = refs[0][...]
        for r in refs[1:count]:
            row = row + r[...]
        q_end, k_end = heads * dk, 2 * heads * dk
        v_end = k_end + heads * dv
        extra = row[:, v_end:]
        squares = extra[:, 2 * all_heads : 2 * all_heads + 1]
        row_scale = lax.rsqrt(squares / D + epsilon)
        row = row[:, :v_end] * row_scale

        def by_head(start, size):
            return jnp.concatenate(
                [row[:, start + h * size : start + (h + 1) * size] for h in range(heads)], axis=0
            ).astype(jnp.bfloat16)

        query, key, value = by_head(0, dk), by_head(q_end, dk), by_head(k_end, dv)
        gates = jnp.broadcast_to(extra * row_scale, (heads, LANES))
        lane = lax.broadcasted_iota(jnp.int32, (heads, LANES), 1)
        head = lax.broadcasted_iota(jnp.int32, (heads, LANES), 0)

        def column(values, first):
            return jnp.sum(jnp.where(lane == head + first, values, 0.0), axis=1, keepdims=True)

        lane_h = lax.broadcasted_iota(jnp.int32, (heads, heads), 1)
        head_h = lax.broadcasted_iota(jnp.int32, (heads, heads), 0)

        def own_column(ref):
            values = jnp.broadcast_to(ref[...], (heads, heads))
            return jnp.sum(jnp.where(lane_h == head_h, values, 0.0), axis=1, keepdims=True)

        new_input = column(gates, half * heads)
        new_logf = jax.nn.log_sigmoid(
            column(gates, all_heads + half * heads) + own_column(bias_ref)
        )
        live = lax.rem(lengths_ref[0], jnp.int32(SPAN_LOCATIONS))
        span = (heads, SPAN_LOCATIONS)
        inside = lax.broadcasted_iota(jnp.int32, span, 1) < live
        logf = jnp.where(inside, logf_ref[0], 0.0)
        square = (SPAN_LOCATIONS, SPAN_LOCATIONS)
        upto = (
            lax.broadcasted_iota(jnp.int32, square, 0) <= lax.broadcasted_iota(jnp.int32, square, 1)
        ).astype(jnp.float32).astype(jnp.bfloat16)
        cumulative = jnp.zeros(span, jnp.float32)
        rest = logf
        for _ in range(3):
            term = rest.astype(jnp.bfloat16)
            rest = rest - term.astype(jnp.float32)
            cumulative = cumulative + jnp.dot(term, upto, preferred_element_type=jnp.float32)
        total = cumulative[:, SPAN_LOCATIONS - 1 :] + new_logf
        carried_log = total + own_column(max_ref)
        cache_log = jnp.where(inside, total - cumulative + input_ref[0], -jnp.inf)
        stable = jnp.maximum(
            jnp.maximum(carried_log, jnp.max(cache_log, axis=1, keepdims=True)), new_input
        )
        carried_weight = jnp.exp(carried_log - stable)
        new_weight = jnp.exp(new_input - stable)
        cache_weight = jnp.exp(cache_log - stable)

        def pick(make, size):
            rows = lax.broadcasted_iota(jnp.int32, (heads, size), 0)
            out = jnp.zeros((heads, size), jnp.float32)
            for h in range(heads):
                out = jnp.where(rows == h, make(h), out)
            return out

        scores = pick(lambda h: dot_nt(query, keys_ref[0, h]), SPAN_LOCATIONS)
        mixing = (scores * scale * cache_weight).astype(jnp.bfloat16)
        query_wide = query.astype(jnp.float32)
        own_term = (
            jnp.sum(query_wide * key.astype(jnp.float32), axis=1, keepdims=True)
            * scale
            * new_weight
        )

        def carry(h):
            state = state_ref[0, h]
            high = state.astype(jnp.bfloat16)
            low = (state - high.astype(jnp.float32)).astype(jnp.bfloat16)
            return dot_nt(query, high) + dot_nt(query, low)

        carried = pick(carry, dv)
        from_cache = pick(
            lambda h: jnp.dot(mixing, values_ref[0, h], preferred_element_type=jnp.float32), dv
        )
        numerator = carried_weight * carried + from_cache + own_term * value.astype(jnp.float32)
        normalizer = (
            carried_weight * jnp.sum(normalizer_ref[0] * query_wide, axis=1, keepdims=True)
            + jnp.sum(mixing.astype(jnp.float32), axis=1, keepdims=True)
            + own_term
        )
        divisor = jnp.maximum(jnp.maximum(jnp.abs(normalizer), jnp.exp(-stable)), 1.0)
        out_ref[...] = (numerator / divisor).astype(jnp.bfloat16)

    return call(
        body,
        [struct((heads, dv), jnp.bfloat16)],
        [VMEM_SPEC] * (count + 8) + [SMEM_SPEC],
        (
            *parts,
            forget_bias.reshape(1, -1),
            resident(state_matrix),
            state_normalizer,
            state_max,
            resident(block_keys),
            resident(block_values),
            block_input,
            block_logf,
            lengths,
        ),
        name="recall",
    )[0]


def attend(pieces, out_weight):
    size = len(pieces)
    heads, dv = pieces[0].shape

    def body(*refs):
        weight_ref, out_ref, hidden_ref = refs[size:]
        position = lax.axis_index("kv")
        for d in range(size):
            piece = refs[d][...].astype(jnp.float32)
            at = pl.ds(partner_of(position, size, d, True), 1)
            for h in range(heads):
                hidden_ref[at, h * dv : (h + 1) * dv] = piece[h : h + 1]
        out_ref[...] = jnp.dot(
            hidden_ref[...].astype(jnp.bfloat16),
            weight_ref[...],
            preferred_element_type=jnp.float32,
        ).astype(jnp.bfloat16)

    return call(
        body,
        [struct((size, out_weight.shape[1]), jnp.bfloat16)],
        [VMEM_SPEC] * (size + 1),
        (*pieces, resident(out_weight)),
        [pltpu.VMEM((size, heads * dv), jnp.float32)],
        name="attend",
    )[0]


def mix(pieces, mixer_gain, up_weight, down_weight):
    size = len(pieces)
    rows, columns = pieces[0].shape

    def body(*refs):
        gain_ref, up_ref, down_ref = refs[size : size + 3]
        outs = refs[size + 3 : 2 * size + 3]
        in_ref, terms_ref = refs[2 * size + 3 :]
        position = lax.axis_index("kv")
        squares = jnp.zeros((rows, 1), jnp.float32)
        for d in range(size):
            j = partner_of(position, size, d, True)
            at = pl.ds(pl.multiple_of(j * columns, columns), columns)
            wide = refs[d][...].astype(jnp.float32)
            squares = squares + jnp.sum(wide * wide, axis=1, keepdims=True)
            in_ref[:, at] = wide
        mixer_in = (in_ref[...] * gain_ref[...]).astype(jnp.bfloat16)
        scaled = dot_nt(mixer_in, up_ref[...]) * lax.rsqrt(squares / D + epsilon)
        activated = jnp.square(jnp.maximum(scaled, 0.0)).astype(jnp.bfloat16)
        terms_ref[...] = jnp.dot(activated, down_ref[...], preferred_element_type=jnp.float32)
        for d in range(size):
            j = partner_of(position, size, d, False)
            outs[d][...] = terms_ref[:, pl.ds(pl.multiple_of(j * columns, columns), columns)]

    wide = (rows, size * columns)
    return call(
        body,
        [struct((rows, columns), jnp.float32)] * size,
        [VMEM_SPEC] * (size + 3),
        (*pieces, mixer_gain.reshape(1, -1), resident(up_weight), resident(down_weight)),
        [pltpu.VMEM(wide, jnp.float32), pltpu.VMEM(wide, jnp.float32)],
        name="mix",
    )


def exchange_pairs(size, cores, distance):
    return [
        (i * cores + t, j * cores + (cores - 1 - t))
        for i, j in partner_pairs(size, distance)
        for t in range(cores)
    ]


def to_partners(outgoing, crossed):
    size, cores = lax.axis_size("kv"), lax.axis_size("tp")
    if crossed:
        return [
            lax.ppermute(outgoing[d], ("kv", "tp"), exchange_pairs(size, cores, d))
            for d in range(1, size)
        ]
    return [lax.ppermute(outgoing[d], "kv", partner_pairs(size, d)) for d in range(1, size)]


def shards(*arrays):
    tokens, up_weight, lengths = arrays[0], arrays[17], arrays[14]
    size, cores = lax.axis_size("kv"), lax.axis_size("tp")
    columns = tokens.shape[1]
    if size > DIRECT_LIMIT or cores != 2 or lengths.shape[0] != 1 or columns % (2 * LANES):
        return shards_general(*arrays)
    return shards_direct(*arrays)


def shards_direct(
    tokens,
    norm_gain,
    query_weight,
    key_weight,
    value_weight,
    gate_weight,
    forget_bias,
    state_matrix,
    state_normalizer,
    state_max,
    block_keys,
    block_values,
    block_input,
    block_logf,
    lengths,
    out_weight,
    mixer_gain,
    up_weight,
    down_weight,
):
    head_half = lax.axis_index("tp")
    size = lax.axis_size("kv")
    swap = [(0, 1), (1, 0)]
    parts = project(tokens, norm_gain, query_weight, key_weight, value_weight, gate_weight)
    parts = [parts[0]] + to_partners(parts, False)
    hidden = recall(
        parts,
        forget_bias,
        state_matrix,
        state_normalizer,
        state_max,
        block_keys,
        block_values,
        block_input,
        block_logf,
        lengths,
    )
    pieces = [hidden] + to_partners([hidden] * size, False)
    partial_out = attend(pieces, out_weight)
    other_out = lax.ppermute(partial_out, "tp", swap)
    attended = partial_out.astype(jnp.float32) + other_out.astype(jnp.float32)
    residual = (tokens.astype(jnp.float32) + attended).astype(jnp.bfloat16)
    pieces = [residual] + to_partners([residual] * size, True)
    terms = mix(pieces, mixer_gain, up_weight, down_weight)
    received = to_partners(terms, True)
    total = terms[0]
    for term in received:
        total = total + term
    share = tokens.shape[1] // 2
    other = lax.dynamic_slice_in_dim(total, (1 - head_half) * share, share, 1)
    kept = lax.dynamic_slice_in_dim(total, head_half * share, share, 1)
    own_residual = lax.dynamic_slice_in_dim(residual, head_half * share, share, 1)
    kept = kept + own_residual.astype(jnp.float32)
    return (kept + lax.ppermute(other, "tp", swap)).astype(jnp.bfloat16)


def solution(mesh):
    return jax.shard_map(
        shards,
        mesh=mesh,
        in_specs=(
            P("dp", "kv"),
            P("kv"),
            P("kv", "tp"),
            P("kv", "tp"),
            P("kv", "tp"),
            P(),
            P("tp"),
            P(("dp", "kv"), "tp", None, None),
            P(("dp", "kv"), "tp", None),
            P(("dp", "kv"), "tp"),
            P(("dp", "kv"), "tp", None, None),
            P(("dp", "kv"), "tp", None, None),
            P(("dp", "kv"), "tp", None),
            P(("dp", "kv"), "tp", None),
            P(("dp", "kv")),
            P("tp", "kv"),
            P(),
            P(("kv", "tp"), None),
            P(("kv", "tp"), None),
        ),
        out_specs=P("dp", ("kv", "tp")),
        check_vma=False,
    )
```

```python
import jax
import jax.numpy as jnp
from jax import lax
from jax.experimental import pallas as pl
from jax.experimental.pallas import tpu as pltpu
from jax.sharding import PartitionSpec as P

D = 4096
DK = 256
DV = 512
SPAN_LOCATIONS = 64


epsilon = 1e-06
highest = lax.Precision.HIGHEST


def memory_cell(
    query,
    key,
    value,
    gates,
    forget_bias,
    state_matrix,
    state_normalizer,
    state_max,
    block_keys,
    block_values,
    block_input,
    block_logf,
    lengths,
):
    live = lengths % SPAN_LOCATIONS
    positions = lax.broadcasted_iota(jnp.int32, (1, 1, SPAN_LOCATIONS), 2)
    inside = positions < live[:, None, None]
    new_input = gates[:, 0]
    new_logf = jax.nn.log_sigmoid(gates[:, 1] + forget_bias)
    cumulative = jnp.cumsum(jnp.where(inside, block_logf, jnp.float32(0.0)), axis=2)
    total = cumulative[:, :, -1] + new_logf
    carried_log = total + state_max
    cache_log = jnp.where(inside, total[:, :, None] - cumulative + block_input, -jnp.inf)
    stable = jnp.maximum(jnp.maximum(carried_log, jnp.max(cache_log, axis=2)), new_input)
    carried_weight = jnp.exp(carried_log - stable)
    new_weight = jnp.exp(new_input - stable)
    cache_weight = jnp.exp(cache_log - stable[:, :, None])
    scores = jnp.einsum("bhk,bhsk->bhs", query, block_keys, preferred_element_type=jnp.float32)
    mixing = (scores * DK ** (-0.5) * cache_weight).astype(jnp.bfloat16)
    query_wide = query.astype(jnp.float32)
    own_term = jnp.sum(query_wide * key.astype(jnp.float32), axis=2) * DK ** (-0.5) * new_weight
    carried = jnp.einsum("bhvk,bhk->bhv", state_matrix, query_wide, precision=highest)
    from_cache = jnp.einsum(
        "bhs,bhsv->bhv", mixing, block_values, preferred_element_type=jnp.float32
    )
    numerator = (
        carried_weight[:, :, None] * carried
        + from_cache
        + own_term[:, :, None] * value.astype(jnp.float32)
    )
    normalizer = (
        carried_weight * jnp.sum(state_normalizer * query_wide, axis=2)
        + jnp.sum(mixing.astype(jnp.float32), axis=2)
        + own_term
    )
    divisor = jnp.maximum(jnp.maximum(jnp.abs(normalizer), jnp.exp(-stable)), jnp.float32(1.0))
    hidden = numerator / divisor[:, :, None]
    return hidden.astype(jnp.bfloat16)


def absorb_columns(mixer_gain, up_weight):

    def absorb(carry, piece, start):
        widened = piece.astype(jnp.float32)
        mixer_in = (widened * mixer_gain).astype(jnp.bfloat16)
        product = lax.dot_general(
            mixer_in, up_weight, (((1,), (1,)), ((), ())), preferred_element_type=jnp.float32
        )
        return (product, jnp.sum(widened * widened, axis=1))

    return absorb


def down_terms(carry, down_weight):
    accumulated, squares = carry
    scaled = accumulated * lax.rsqrt(squares / D + epsilon)[:, None]
    activated = jnp.square(jax.nn.relu(scaled)).astype(jnp.bfloat16)
    return jnp.dot(activated, down_weight, preferred_element_type=jnp.float32)


DIRECT_LIMIT = 8


def partner_pairs(size, distance):
    if size & (size - 1) == 0:
        return [(i, i ^ distance) for i in range(size)]
    return [(i, (i + distance) % size) for i in range(size)]


def partner_of(position, size, distance, receiving):
    if size & (size - 1) == 0:
        return position ^ distance
    return (position - distance) % size if receiving else (position + distance) % size


def gather_direct(piece, axis):
    size = lax.axis_size(axis)
    if size > DIRECT_LIMIT:
        return lax.all_gather(piece, axis, axis=0)
    position = lax.axis_index(axis)
    received = [piece] + [
        lax.ppermute(piece, axis, partner_pairs(size, d)) for d in range(1, size)
    ]
    stacked = jnp.stack(received)
    places = jnp.arange(size)
    if size & (size - 1) == 0:
        order = position ^ places
    else:
        order = (position - places) % size
    return stacked[order]


def scatter_sum_direct(parts, axis):
    size = lax.axis_size(axis)
    if size > DIRECT_LIMIT:
        return lax.psum_scatter(parts, axis, scatter_dimension=0, tiled=False)
    position = lax.axis_index(axis)

    def entry(index):
        return lax.dynamic_index_in_dim(parts, index, 0, keepdims=False)

    total = entry(position)
    for d in range(1, size):
        out = entry(partner_of(position, size, d, False))
        total = total + lax.ppermute(out, axis, partner_pairs(size, d))
    return total


def shards_general(
    tokens,
    norm_gain,
    query_weight,
    key_weight,
    value_weight,
    gate_weight,
    forget_bias,
    state_matrix,
    state_normalizer,
    state_max,
    block_keys,
    block_values,
    block_input,
    block_logf,
    lengths,
    out_weight,
    mixer_gain,
    up_weight,
    down_weight,
):
    position = lax.axis_index("kv")
    head_half = lax.axis_index("tp")
    columns = tokens.shape[1]
    local_heads = forget_bias.shape[0]
    local_rows = lengths.shape[0]
    widened = tokens.astype(jnp.float32)
    squares = jnp.sum(widened * widened, axis=1)
    normed = (widened * norm_gain).astype(jnp.bfloat16)
    gate_rows = lax.dynamic_slice_in_dim(gate_weight, position * columns, columns, 0)
    gate_rows = lax.dynamic_slice_in_dim(
        gate_rows, head_half * local_heads, local_heads, 2
    ).reshape(columns, 2 * local_heads)
    query_part = jnp.dot(normed, query_weight, preferred_element_type=jnp.float32)
    key_part = jnp.dot(normed, key_weight, preferred_element_type=jnp.float32)
    value_part = jnp.dot(normed, value_weight, preferred_element_type=jnp.float32)
    gate_part = jnp.dot(normed, gate_rows, preferred_element_type=jnp.float32)
    parts = jnp.concatenate(
        [query_part, key_part, value_part, gate_part, squares[:, None]], axis=1
    )
    parts = parts.reshape(-1, local_rows, parts.shape[1])
    sums = scatter_sum_direct(parts, "kv")
    q_end = query_part.shape[1]
    k_end = q_end + key_part.shape[1]
    v_end = k_end + value_part.shape[1]
    g_end = v_end + gate_part.shape[1]
    query_sum, key_sum, value_sum, gate_sum, own_squares = (
        sums[:, :q_end],
        sums[:, q_end:k_end],
        sums[:, k_end:v_end],
        sums[:, v_end:g_end],
        sums[:, g_end],
    )
    row_scale = lax.rsqrt(own_squares / D + epsilon)[:, None]
    query = (query_sum * row_scale).astype(jnp.bfloat16).reshape(local_rows, local_heads, DK)
    key = (key_sum * row_scale).astype(jnp.bfloat16).reshape(local_rows, local_heads, DK)
    value = (value_sum * row_scale).astype(jnp.bfloat16).reshape(local_rows, local_heads, DV)
    gates = (gate_sum * row_scale).reshape(local_rows, 2, local_heads)
    hidden = memory_cell(
        query,
        key,
        value,
        gates,
        forget_bias,
        state_matrix,
        state_normalizer,
        state_max,
        block_keys,
        block_values,
        block_input,
        block_logf,
        lengths,
    )
    hidden = hidden.reshape(local_rows, local_heads * DV)
    every_hidden = gather_direct(hidden, "kv").reshape(-1, hidden.shape[1])
    partial_out = jnp.dot(
        every_hidden, out_weight, preferred_element_type=jnp.float32
    ).astype(jnp.bfloat16)
    attended = jnp.sum(gather_direct(partial_out, "tp").astype(jnp.float32), axis=0)
    residual = (widened + attended).astype(jnp.bfloat16)
    absorb = absorb_columns(mixer_gain, up_weight)
    hidden_units = up_weight.shape[0]
    rows = residual.shape[0]
    initial = (jnp.zeros((rows, hidden_units), jnp.float32), jnp.zeros((rows,), jnp.float32))
    pieces = gather_direct(residual, "kv")
    whole = jnp.moveaxis(pieces, 0, 1).reshape(rows, -1)
    carry = absorb(initial, whole, jnp.int32(0))
    terms = down_terms(carry, down_weight)
    share = columns // lax.axis_size("tp")
    terms = terms.reshape(rows, -1, lax.axis_size("tp"), share)
    by_core = scatter_sum_direct(jnp.moveaxis(terms, 2, 0), "tp")
    mixed_terms = scatter_sum_direct(jnp.moveaxis(by_core, 1, 0), "kv")
    own_residual = lax.dynamic_slice_in_dim(residual, head_half * share, share, 1)
    return (own_residual.astype(jnp.float32) + mixed_terms).astype(jnp.bfloat16)


def dot_nt(left, right):
    return lax.dot_general(
        left, right, (((1,), (1,)), ((), ())), preferred_element_type=jnp.float32
    )


VMEM_SPEC = pl.BlockSpec(memory_space=pltpu.VMEM)
SMEM_SPEC = pl.BlockSpec(memory_space=pltpu.SMEM)
ANY_SPEC = pl.BlockSpec(memory_space=pl.ANY)


def call(body, outs, in_specs, args, scratch=(), limit=8, flops=20000000000, name=None):
    return pl.pallas_call(
        body,
        out_shape=outs,
        in_specs=in_specs,
        out_specs=[VMEM_SPEC] * len(outs),
        scratch_shapes=list(scratch),
        compiler_params=pltpu.CompilerParams(vmem_limit_bytes=limit << 20),
        cost_estimate=pl.CostEstimate(flops=flops, bytes_accessed=1000000, transcendentals=0),
        name=name,
    )(*args)


def resident(weight):
    return pltpu.with_memory_space_constraint(weight, pltpu.VMEM)


def streamed(weight):
    return pltpu.with_memory_space_constraint(weight, pltpu.HBM)


def struct(shape, kind):
    return jax.ShapeDtypeStruct(shape, kind)


LANES = 128


def project(tokens, norm_gain, query_weight, key_weight, value_weight, gate_weight):
    rows, columns = tokens.shape
    size = lax.axis_size("kv")
    weights = (query_weight, key_weight, value_weight)
    widths = [w.shape[1] for w in weights]
    starts = [sum(widths[:i]) for i in range(3)]
    width = sum(widths)
    gate_count = gate_weight.shape[1] * gate_weight.shape[2]
    gates = jnp.transpose(gate_weight, (1, 2, 0)).reshape(gate_count, -1)
    chunks = 4 if columns % 512 == 0 else 1
    chunk = columns // chunks

    def body(tokens_hbm, gain_hbm, q_hbm, k_hbm, v_hbm, gate_hbm, *rest):
        outs = rest[:size]
        tokens_ref, gain_ref, q_ref, k_ref, v_ref, gate_ref, sums_ref = rest[size : size + 7]
        sems, gate_sem, tokens_sem, gain_sem = rest[size + 7 :]
        position = lax.axis_index("kv")
        tokens_copy = pltpu.make_async_copy(tokens_hbm, tokens_ref, tokens_sem)
        gain_copy = pltpu.make_async_copy(gain_hbm, gain_ref, gain_sem)
        tokens_copy.start()
        gain_copy.start()
        gate_copy = pltpu.make_async_copy(
            gate_hbm.at[:, pl.ds(pl.multiple_of(position * columns, columns), columns)],
            gate_ref,
            gate_sem,
        )
        copies = []
        for c in range(chunks):
            at = pl.ds(c * chunk, chunk)
            for w, (source, target) in enumerate(
                ((q_hbm, q_ref), (k_hbm, k_ref), (v_hbm, v_ref))
            ):
                copy = pltpu.make_async_copy(source.at[at, :], target.at[at, :], sems.at[c, w])
                copy.start()
                copies.append(copy)
            if c == 0:
                gate_copy.start()
        tokens_copy.wait()
        gain_copy.wait()
        widened = tokens_ref[...].astype(jnp.float32)
        squares = jnp.sum(widened * widened, axis=1, keepdims=True)
        normed = (widened * gain_ref[...]).astype(jnp.bfloat16)
        sums = [jnp.zeros((rows, n), jnp.float32) for n in widths]
        for c in range(chunks):
            piece = normed[:, c * chunk : (c + 1) * chunk]
            for w, ref in enumerate((q_ref, k_ref, v_ref)):
                copies[3 * c + w].wait()
                sums[w] = sums[w] + jnp.dot(
                    piece,
                    ref[c * chunk : (c + 1) * chunk, :],
                    preferred_element_type=jnp.float32,
                )
        gate_copy.wait()
        gate_sums = dot_nt(normed, gate_ref[...])
        pad = jnp.zeros((rows, LANES - gate_count), jnp.float32)
        extra = jnp.concatenate([gate_sums, pad], axis=1)
        lane = lax.broadcasted_iota(jnp.int32, (rows, LANES), 1)
        extra = jnp.where(lane == gate_count, squares, extra)
        for w in range(3):
            sums_ref[:, starts[w] : starts[w] + widths[w]] = sums[w]
        sums_ref[:, width:] = extra
        for d in range(size):
            outs[d][...] = sums_ref[pl.ds(partner_of(position, size, d, False), 1), :]

    return call(
        body,
        [struct((1, width + LANES), jnp.float32)] * size,
        [ANY_SPEC] * 6,
        [streamed(a) for a in (tokens, norm_gain.reshape(1, -1), *weights, gates)],
        [pltpu.VMEM(tokens.shape, tokens.dtype), pltpu.VMEM((1, columns), norm_gain.dtype)]
        + [pltpu.VMEM(w.shape, w.dtype) for w in weights]
        + [
            pltpu.VMEM((gate_count, columns), gates.dtype),
            pltpu.VMEM((rows, width + LANES), jnp.float32),
            pltpu.SemaphoreType.DMA((chunks, 3)),
            pltpu.SemaphoreType.DMA(()),
            pltpu.SemaphoreType.DMA(()),
            pltpu.SemaphoreType.DMA(()),
        ],
        limit=16,
        name="project",
    )


def split_state(state_matrix):
    _, heads, dv, dk = state_matrix.shape

    def body(state_hbm, high_ref, low_ref, state_ref, sems):
        copies = [
            pltpu.make_async_copy(state_hbm.at[0, h], state_ref.at[h], sems.at[h])
            for h in range(heads)
        ]
        for copy in copies:
            copy.start()
        for h in range(heads):
            copies[h].wait()
            state = state_ref[h]
            high = state.astype(jnp.bfloat16)
            high_ref[h] = high
            low_ref[h] = (state - high.astype(jnp.float32)).astype(jnp.bfloat16)

    term = struct((heads, dv, dk), jnp.bfloat16)
    return call(
        body,
        [term, term],
        [ANY_SPEC],
        [streamed(state_matrix)],
        [
            pltpu.VMEM((heads, dv, dk), state_matrix.dtype),
            pltpu.SemaphoreType.DMA((heads,)),
        ],
        name="split_state",
    )


def recall(
    parts,
    forget_bias,
    state_terms,
    state_normalizer,
    state_max,
    block_keys,
    block_values,
    block_input,
    block_logf,
    lengths,
):
    heads, dv, dk = state_terms[0].shape
    all_heads = heads * lax.axis_size("tp")
    scale = dk ** (-0.5)
    count = len(parts)

    def body(*refs):
        (
            bias_ref,
            high_ref,
            low_ref,
            normalizer_ref,
            max_ref,
            keys_ref,
            values_ref,
            input_ref,
            logf_ref,
            lengths_ref,
            out_ref,
        ) = refs[count:]
        half = lax.axis_index("tp")
        row = refs[0][...]
        for r in refs[1:count]:
            row = row + r[...]
        q_end, k_end = heads * dk, 2 * heads * dk
        v_end = k_end + heads * dv
        extra = row[:, v_end:]
        squares = extra[:, 2 * all_heads : 2 * all_heads + 1]
        row_scale = lax.rsqrt(squares / D + epsilon)
        row = row[:, :v_end] * row_scale

        def by_head(start, size):
            return jnp.concatenate(
                [row[:, start + h * size : start + (h + 1) * size] for h in range(heads)], axis=0
            ).astype(jnp.bfloat16)

        query, key, value = by_head(0, dk), by_head(q_end, dk), by_head(k_end, dv)
        gates = jnp.broadcast_to(extra * row_scale, (heads, LANES))
        lane = lax.broadcasted_iota(jnp.int32, (heads, LANES), 1)
        head = lax.broadcasted_iota(jnp.int32, (heads, LANES), 0)

        def column(values, first):
            return jnp.sum(jnp.where(lane == head + first, values, 0.0), axis=1, keepdims=True)

        lane_h = lax.broadcasted_iota(jnp.int32, (heads, heads), 1)
        head_h = lax.broadcasted_iota(jnp.int32, (heads, heads), 0)

        def own_column(ref):
            values = jnp.broadcast_to(ref[...], (heads, heads))
            return jnp.sum(jnp.where(lane_h == head_h, values, 0.0), axis=1, keepdims=True)

        new_input = column(gates, half * heads)
        new_logf = jax.nn.log_sigmoid(
            column(gates, all_heads + half * heads) + own_column(bias_ref)
        )
        live = lax.rem(lengths_ref[0], jnp.int32(SPAN_LOCATIONS))
        span = (heads, SPAN_LOCATIONS)
        inside = lax.broadcasted_iota(jnp.int32, span, 1) < live
        logf = jnp.where(inside, logf_ref[0], 0.0)
        square = (SPAN_LOCATIONS, SPAN_LOCATIONS)
        upto = (
            lax.broadcasted_iota(jnp.int32, square, 0) <= lax.broadcasted_iota(jnp.int32, square, 1)
        ).astype(jnp.float32).astype(jnp.bfloat16)
        cumulative = jnp.zeros(span, jnp.float32)
        rest = logf
        for _ in range(3):
            term = rest.astype(jnp.bfloat16)
            rest = rest - term.astype(jnp.float32)
            cumulative = cumulative + jnp.dot(term, upto, preferred_element_type=jnp.float32)
        total = cumulative[:, SPAN_LOCATIONS - 1 :] + new_logf
        carried_log = total + own_column(max_ref)
        cache_log = jnp.where(inside, total - cumulative + input_ref[0], -jnp.inf)
        stable = jnp.maximum(
            jnp.maximum(carried_log, jnp.max(cache_log, axis=1, keepdims=True)), new_input
        )
        carried_weight = jnp.exp(carried_log - stable)
        new_weight = jnp.exp(new_input - stable)
        cache_weight = jnp.exp(cache_log - stable)

        def pick(make, size):
            rows = lax.broadcasted_iota(jnp.int32, (heads, size), 0)
            out = jnp.zeros((heads, size), jnp.float32)
            for h in range(heads):
                out = jnp.where(rows == h, make(h), out)
            return out

        scores = pick(lambda h: dot_nt(query, keys_ref[0, h]), SPAN_LOCATIONS)
        mixing = (scores * scale * cache_weight).astype(jnp.bfloat16)
        query_wide = query.astype(jnp.float32)
        own_term = (
            jnp.sum(query_wide * key.astype(jnp.float32), axis=1, keepdims=True)
            * scale
            * new_weight
        )

        def carry(h):
            return dot_nt(query, high_ref[h]) + dot_nt(query, low_ref[h])

        carried = pick(carry, dv)
        from_cache = pick(
            lambda h: jnp.dot(mixing, values_ref[0, h], preferred_element_type=jnp.float32), dv
        )
        numerator = carried_weight * carried + from_cache + own_term * value.astype(jnp.float32)
        normalizer = (
            carried_weight * jnp.sum(normalizer_ref[0] * query_wide, axis=1, keepdims=True)
            + jnp.sum(mixing.astype(jnp.float32), axis=1, keepdims=True)
            + own_term
        )
        divisor = jnp.maximum(jnp.maximum(jnp.abs(normalizer), jnp.exp(-stable)), 1.0)
        out_ref[...] = (numerator / divisor).astype(jnp.bfloat16)

    return call(
        body,
        [struct((heads, dv), jnp.bfloat16)],
        [VMEM_SPEC] * (count + 9) + [SMEM_SPEC],
        (
            *parts,
            forget_bias.reshape(1, -1),
            *[resident(term) for term in state_terms],
            state_normalizer,
            state_max,
            resident(block_keys),
            resident(block_values),
            block_input,
            block_logf,
            lengths,
        ),
        name="recall",
    )[0]


def attend(pieces, out_weight):
    size = len(pieces)
    heads, dv = pieces[0].shape

    def body(*refs):
        weight_ref, out_ref, hidden_ref = refs[size:]
        position = lax.axis_index("kv")
        for n, d in enumerate([0, *distances(size)]):
            piece = refs[n][...].astype(jnp.float32)
            at = pl.ds(partner_of(position, size, d, True), 1)
            for h in range(heads):
                hidden_ref[at, h * dv : (h + 1) * dv] = piece[h : h + 1]
        out_ref[...] = jnp.dot(
            hidden_ref[...].astype(jnp.bfloat16),
            weight_ref[...],
            preferred_element_type=jnp.float32,
        ).astype(jnp.bfloat16)

    return call(
        body,
        [struct((size, out_weight.shape[1]), jnp.bfloat16)],
        [VMEM_SPEC] * (size + 1),
        (*pieces, resident(out_weight)),
        [pltpu.VMEM((size, heads * dv), jnp.float32)],
        name="attend",
    )[0]


def absorb_own(residual, mixer_gain, up_weight):
    rows, columns = residual.shape
    units = up_weight.shape[0]

    def body(piece_ref, gain_ref, up_ref, product_ref, squares_ref):
        position = lax.axis_index("kv")
        at = pl.ds(pl.multiple_of(position * columns, columns), columns)
        wide = piece_ref[...].astype(jnp.float32)
        squares = jnp.sum(wide * wide, axis=1, keepdims=True)
        squares_ref[...] = jnp.broadcast_to(squares, (rows, LANES))
        mixer_in = (wide * gain_ref[:, at]).astype(jnp.bfloat16)
        product_ref[...] = dot_nt(mixer_in, up_ref[:, at])

    return call(
        body,
        [struct((rows, units), jnp.float32), struct((rows, LANES), jnp.float32)],
        [VMEM_SPEC] * 3,
        (residual, mixer_gain, up_weight),
        name="absorb_own",
    )


def mix(pieces, own, mixer_gain, up_weight, down_weight):
    size = len(pieces) + 1
    rows, columns = pieces[0].shape

    def body(*refs):
        product_ref, squares_ref, gain_ref, up_ref, down_ref = refs[size - 1 : size + 4]
        outs = refs[size + 4 : 2 * size + 4]
        (terms_ref,) = refs[2 * size + 4 :]
        position = lax.axis_index("kv")
        squares = squares_ref[:, :1]
        product = product_ref[...]
        for n, d in enumerate(distances(size)):
            j = partner_of(position, size, d, True)
            at = pl.ds(pl.multiple_of(j * columns, columns), columns)
            wide = refs[n][...].astype(jnp.float32)
            squares = squares + jnp.sum(wide * wide, axis=1, keepdims=True)
            mixer_in = (wide * gain_ref[:, at]).astype(jnp.bfloat16)
            product = product + dot_nt(mixer_in, up_ref[:, at])
        scaled = product * lax.rsqrt(squares / D + epsilon)
        activated = jnp.square(jnp.maximum(scaled, 0.0)).astype(jnp.bfloat16)
        terms_ref[...] = jnp.dot(activated, down_ref[...], preferred_element_type=jnp.float32)
        for d in range(size):
            j = partner_of(position, size, d, False)
            outs[d][...] = terms_ref[:, pl.ds(pl.multiple_of(j * columns, columns), columns)]

    return call(
        body,
        [struct((rows, columns), jnp.float32)] * size,
        [VMEM_SPEC] * (size + 4),
        (*pieces, *own, mixer_gain, up_weight, down_weight),
        [pltpu.VMEM((rows, size * columns), jnp.float32)],
        name="mix",
    )


def exchange_pairs(size, cores, distance):
    return [
        (i * cores + t, j * cores + (cores - 1 - t))
        for i, j in partner_pairs(size, distance)
        for t in range(cores)
    ]


def distances(size):
    return [*range(size // 2, size), *range(1, size // 2)]


def to_partners(outgoing, crossed):
    size, cores = lax.axis_size("kv"), lax.axis_size("tp")
    if crossed:
        return [
            lax.ppermute(outgoing[d], ("kv", "tp"), exchange_pairs(size, cores, d))
            for d in distances(size)
        ]
    return [lax.ppermute(outgoing[d], "kv", partner_pairs(size, d)) for d in distances(size)]


def shards(*arrays):
    tokens, up_weight, lengths = arrays[0], arrays[17], arrays[14]
    size, cores = lax.axis_size("kv"), lax.axis_size("tp")
    columns = tokens.shape[1]
    if size > DIRECT_LIMIT or cores != 2 or lengths.shape[0] != 1 or columns % (2 * LANES):
        return shards_general(*arrays)
    return shards_direct(*arrays)


def shards_direct(
    tokens,
    norm_gain,
    query_weight,
    key_weight,
    value_weight,
    gate_weight,
    forget_bias,
    state_matrix,
    state_normalizer,
    state_max,
    block_keys,
    block_values,
    block_input,
    block_logf,
    lengths,
    out_weight,
    mixer_gain,
    up_weight,
    down_weight,
):
    head_half = lax.axis_index("tp")
    size = lax.axis_size("kv")
    swap = [(0, 1), (1, 0)]
    parts = project(tokens, norm_gain, query_weight, key_weight, value_weight, gate_weight)
    state_terms = split_state(state_matrix)
    parts = [parts[0]] + to_partners(parts, False)
    hidden = recall(
        parts,
        forget_bias,
        state_terms,
        state_normalizer,
        state_max,
        block_keys,
        block_values,
        block_input,
        block_logf,
        lengths,
    )
    pieces = [hidden] + to_partners([hidden] * size, False)
    partial_out = attend(pieces, out_weight)
    other_out = lax.ppermute(partial_out, "tp", swap)
    attended = partial_out.astype(jnp.float32) + other_out.astype(jnp.float32)
    residual = (tokens.astype(jnp.float32) + attended).astype(jnp.bfloat16)
    gain = mixer_gain.reshape(1, -1)
    up_weight, down_weight = resident(up_weight), resident(down_weight)
    pieces = to_partners([residual] * size, True)
    own = absorb_own(residual, gain, up_weight)
    terms = mix(pieces, own, gain, up_weight, down_weight)
    received = to_partners(terms, True)
    total = terms[0]
    for term in received:
        total = total + term
    share = tokens.shape[1] // 2
    other = lax.dynamic_slice_in_dim(total, (1 - head_half) * share, share, 1)
    kept = lax.dynamic_slice_in_dim(total, head_half * share, share, 1)
    own_residual = lax.dynamic_slice_in_dim(residual, head_half * share, share, 1)
    kept = kept + own_residual.astype(jnp.float32)
    return (kept + lax.ppermute(other, "tp", swap)).astype(jnp.bfloat16)


def solution(mesh):
    return jax.shard_map(
        shards,
        mesh=mesh,
        in_specs=(
            P("dp", "kv"),
            P("kv"),
            P("kv", "tp"),
            P("kv", "tp"),
            P("kv", "tp"),
            P(),
            P("tp"),
            P(("dp", "kv"), "tp", None, None),
            P(("dp", "kv"), "tp", None),
            P(("dp", "kv"), "tp"),
            P(("dp", "kv"), "tp", None, None),
            P(("dp", "kv"), "tp", None, None),
            P(("dp", "kv"), "tp", None),
            P(("dp", "kv"), "tp", None),
            P(("dp", "kv")),
            P("tp", "kv"),
            P(),
            P(("kv", "tp"), None),
            P(("kv", "tp"), None),
        ),
        out_specs=P("dp", ("kv", "tp")),
        check_vma=False,
    )
```

```python
import jax
import jax.numpy as jnp
from jax import lax
from jax.experimental import pallas as pl
from jax.experimental.pallas import tpu as pltpu
from jax.sharding import PartitionSpec as P

D = 4096
DK = 256
DV = 512
SPAN_LOCATIONS = 64


epsilon = 1e-06
highest = lax.Precision.HIGHEST


def memory_cell(
    query,
    key,
    value,
    gates,
    forget_bias,
    state_matrix,
    state_normalizer,
    state_max,
    block_keys,
    block_values,
    block_input,
    block_logf,
    lengths,
):
    live = lengths % SPAN_LOCATIONS
    positions = lax.broadcasted_iota(jnp.int32, (1, 1, SPAN_LOCATIONS), 2)
    inside = positions < live[:, None, None]
    new_input = gates[:, 0]
    new_logf = jax.nn.log_sigmoid(gates[:, 1] + forget_bias)
    cumulative = jnp.cumsum(jnp.where(inside, block_logf, jnp.float32(0.0)), axis=2)
    total = cumulative[:, :, -1] + new_logf
    carried_log = total + state_max
    cache_log = jnp.where(inside, total[:, :, None] - cumulative + block_input, -jnp.inf)
    stable = jnp.maximum(jnp.maximum(carried_log, jnp.max(cache_log, axis=2)), new_input)
    carried_weight = jnp.exp(carried_log - stable)
    new_weight = jnp.exp(new_input - stable)
    cache_weight = jnp.exp(cache_log - stable[:, :, None])
    scores = jnp.einsum("bhk,bhsk->bhs", query, block_keys, preferred_element_type=jnp.float32)
    mixing = (scores * DK ** (-0.5) * cache_weight).astype(jnp.bfloat16)
    query_wide = query.astype(jnp.float32)
    own_term = jnp.sum(query_wide * key.astype(jnp.float32), axis=2) * DK ** (-0.5) * new_weight
    carried = jnp.einsum("bhvk,bhk->bhv", state_matrix, query_wide, precision=highest)
    from_cache = jnp.einsum(
        "bhs,bhsv->bhv", mixing, block_values, preferred_element_type=jnp.float32
    )
    numerator = (
        carried_weight[:, :, None] * carried
        + from_cache
        + own_term[:, :, None] * value.astype(jnp.float32)
    )
    normalizer = (
        carried_weight * jnp.sum(state_normalizer * query_wide, axis=2)
        + jnp.sum(mixing.astype(jnp.float32), axis=2)
        + own_term
    )
    divisor = jnp.maximum(jnp.maximum(jnp.abs(normalizer), jnp.exp(-stable)), jnp.float32(1.0))
    hidden = numerator / divisor[:, :, None]
    return hidden.astype(jnp.bfloat16)


def absorb_columns(mixer_gain, up_weight):

    def absorb(carry, piece, start):
        widened = piece.astype(jnp.float32)
        mixer_in = (widened * mixer_gain).astype(jnp.bfloat16)
        product = lax.dot_general(
            mixer_in, up_weight, (((1,), (1,)), ((), ())), preferred_element_type=jnp.float32
        )
        return (product, jnp.sum(widened * widened, axis=1))

    return absorb


def down_terms(carry, down_weight):
    accumulated, squares = carry
    scaled = accumulated * lax.rsqrt(squares / D + epsilon)[:, None]
    activated = jnp.square(jax.nn.relu(scaled)).astype(jnp.bfloat16)
    return jnp.dot(activated, down_weight, preferred_element_type=jnp.float32)


DIRECT_LIMIT = 8


def partner_pairs(size, distance):
    if size & (size - 1) == 0:
        return [(i, i ^ distance) for i in range(size)]
    return [(i, (i + distance) % size) for i in range(size)]


def partner_of(position, size, distance, receiving):
    if size & (size - 1) == 0:
        return position ^ distance
    return (position - distance) % size if receiving else (position + distance) % size


def gather_direct(piece, axis):
    size = lax.axis_size(axis)
    if size > DIRECT_LIMIT:
        return lax.all_gather(piece, axis, axis=0)
    position = lax.axis_index(axis)
    received = [piece] + [
        lax.ppermute(piece, axis, partner_pairs(size, d)) for d in range(1, size)
    ]
    stacked = jnp.stack(received)
    places = jnp.arange(size)
    if size & (size - 1) == 0:
        order = position ^ places
    else:
        order = (position - places) % size
    return stacked[order]


def scatter_sum_direct(parts, axis):
    size = lax.axis_size(axis)
    if size > DIRECT_LIMIT:
        return lax.psum_scatter(parts, axis, scatter_dimension=0, tiled=False)
    position = lax.axis_index(axis)

    def entry(index):
        return lax.dynamic_index_in_dim(parts, index, 0, keepdims=False)

    total = entry(position)
    for d in range(1, size):
        out = entry(partner_of(position, size, d, False))
        total = total + lax.ppermute(out, axis, partner_pairs(size, d))
    return total


def shards_general(
    tokens,
    norm_gain,
    query_weight,
    key_weight,
    value_weight,
    gate_weight,
    forget_bias,
    state_matrix,
    state_normalizer,
    state_max,
    block_keys,
    block_values,
    block_input,
    block_logf,
    lengths,
    out_weight,
    mixer_gain,
    up_weight,
    down_weight,
):
    position = lax.axis_index("kv")
    head_half = lax.axis_index("tp")
    columns = tokens.shape[1]
    local_heads = forget_bias.shape[0]
    local_rows = lengths.shape[0]
    widened = tokens.astype(jnp.float32)
    squares = jnp.sum(widened * widened, axis=1)
    normed = (widened * norm_gain).astype(jnp.bfloat16)
    gate_rows = lax.dynamic_slice_in_dim(gate_weight, position * columns, columns, 0)
    gate_rows = lax.dynamic_slice_in_dim(
        gate_rows, head_half * local_heads, local_heads, 2
    ).reshape(columns, 2 * local_heads)
    query_part = jnp.dot(normed, query_weight, preferred_element_type=jnp.float32)
    key_part = jnp.dot(normed, key_weight, preferred_element_type=jnp.float32)
    value_part = jnp.dot(normed, value_weight, preferred_element_type=jnp.float32)
    gate_part = jnp.dot(normed, gate_rows, preferred_element_type=jnp.float32)
    parts = jnp.concatenate(
        [query_part, key_part, value_part, gate_part, squares[:, None]], axis=1
    )
    parts = parts.reshape(-1, local_rows, parts.shape[1])
    sums = scatter_sum_direct(parts, "kv")
    q_end = query_part.shape[1]
    k_end = q_end + key_part.shape[1]
    v_end = k_end + value_part.shape[1]
    g_end = v_end + gate_part.shape[1]
    query_sum, key_sum, value_sum, gate_sum, own_squares = (
        sums[:, :q_end],
        sums[:, q_end:k_end],
        sums[:, k_end:v_end],
        sums[:, v_end:g_end],
        sums[:, g_end],
    )
    row_scale = lax.rsqrt(own_squares / D + epsilon)[:, None]
    query = (query_sum * row_scale).astype(jnp.bfloat16).reshape(local_rows, local_heads, DK)
    key = (key_sum * row_scale).astype(jnp.bfloat16).reshape(local_rows, local_heads, DK)
    value = (value_sum * row_scale).astype(jnp.bfloat16).reshape(local_rows, local_heads, DV)
    gates = (gate_sum * row_scale).reshape(local_rows, 2, local_heads)
    hidden = memory_cell(
        query,
        key,
        value,
        gates,
        forget_bias,
        state_matrix,
        state_normalizer,
        state_max,
        block_keys,
        block_values,
        block_input,
        block_logf,
        lengths,
    )
    hidden = hidden.reshape(local_rows, local_heads * DV)
    every_hidden = gather_direct(hidden, "kv").reshape(-1, hidden.shape[1])
    partial_out = jnp.dot(
        every_hidden, out_weight, preferred_element_type=jnp.float32
    ).astype(jnp.bfloat16)
    attended = jnp.sum(gather_direct(partial_out, "tp").astype(jnp.float32), axis=0)
    residual = (widened + attended).astype(jnp.bfloat16)
    absorb = absorb_columns(mixer_gain, up_weight)
    hidden_units = up_weight.shape[0]
    rows = residual.shape[0]
    initial = (jnp.zeros((rows, hidden_units), jnp.float32), jnp.zeros((rows,), jnp.float32))
    pieces = gather_direct(residual, "kv")
    whole = jnp.moveaxis(pieces, 0, 1).reshape(rows, -1)
    carry = absorb(initial, whole, jnp.int32(0))
    terms = down_terms(carry, down_weight)
    share = columns // lax.axis_size("tp")
    terms = terms.reshape(rows, -1, lax.axis_size("tp"), share)
    by_core = scatter_sum_direct(jnp.moveaxis(terms, 2, 0), "tp")
    mixed_terms = scatter_sum_direct(jnp.moveaxis(by_core, 1, 0), "kv")
    own_residual = lax.dynamic_slice_in_dim(residual, head_half * share, share, 1)
    return (own_residual.astype(jnp.float32) + mixed_terms).astype(jnp.bfloat16)


def dot_nt(left, right):
    return lax.dot_general(
        left, right, (((1,), (1,)), ((), ())), preferred_element_type=jnp.float32
    )


VMEM_SPEC = pl.BlockSpec(memory_space=pltpu.VMEM)
SMEM_SPEC = pl.BlockSpec(memory_space=pltpu.SMEM)
ANY_SPEC = pl.BlockSpec(memory_space=pl.ANY)


def call(body, outs, in_specs, args, scratch=(), limit=8, flops=20000000000, aliases=None):
    return pl.pallas_call(
        body,
        out_shape=outs,
        in_specs=in_specs,
        out_specs=[VMEM_SPEC] * len(outs),
        scratch_shapes=list(scratch),
        input_output_aliases=aliases or {},
        compiler_params=pltpu.CompilerParams(vmem_limit_bytes=limit << 20),
        cost_estimate=pl.CostEstimate(flops=flops, bytes_accessed=1000000, transcendentals=0),
    )(*args)


def resident(weight):
    return pltpu.with_memory_space_constraint(weight, pltpu.VMEM)


def streamed(weight):
    return pltpu.with_memory_space_constraint(weight, pltpu.HBM)


def struct(shape, kind):
    return jax.ShapeDtypeStruct(shape, kind)


LANES = 128


def project(tokens, norm_gain, query_weight, key_weight, value_weight, gate_weight):
    rows, columns = tokens.shape
    size = lax.axis_size("kv")
    weights = (query_weight, key_weight, value_weight)
    widths = [w.shape[1] for w in weights]
    starts = [sum(widths[:i]) for i in range(3)]
    width = sum(widths)
    gate_count = gate_weight.shape[1] * gate_weight.shape[2]
    gates = jnp.transpose(gate_weight, (1, 2, 0)).reshape(gate_count, -1)
    cuts = [0, columns]

    def body(tokens_hbm, gain_hbm, q_hbm, k_hbm, v_hbm, gate_hbm, *rest):
        outs = rest[:size]
        tokens_ref, gain_ref, weight_ref, gate_ref, sums_ref = rest[size : size + 5]
        sems, gate_sem, tokens_sem, gain_sem = rest[size + 5 :]
        position = lax.axis_index("kv")
        tokens_copy = pltpu.make_async_copy(tokens_hbm, tokens_ref, tokens_sem)
        gain_copy = pltpu.make_async_copy(gain_hbm, gain_ref, gain_sem)
        tokens_copy.start()
        gain_copy.start()
        copies = []
        for c in range(len(cuts) - 1):
            at = pl.ds(cuts[c], cuts[c + 1] - cuts[c])
            for w, source in enumerate((q_hbm, k_hbm, v_hbm)):
                copy = pltpu.make_async_copy(
                    source.at[at, :],
                    weight_ref.at[at, pl.ds(starts[w], widths[w])],
                    sems.at[c, w],
                )
                copy.start()
                copies.append(copy)
        gate_copy = pltpu.make_async_copy(
            gate_hbm.at[:, pl.ds(pl.multiple_of(position * columns, columns), columns)],
            gate_ref,
            gate_sem,
        )
        gate_copy.start()
        tokens_copy.wait()
        gain_copy.wait()
        widened = tokens_ref[...].astype(jnp.float32)
        squares = jnp.sum(widened * widened, axis=1, keepdims=True)
        normed = (widened * gain_ref[...]).astype(jnp.bfloat16)
        for c in range(len(cuts) - 1):
            piece = normed[:, cuts[c] : cuts[c + 1]]
            for w in range(3):
                copies[3 * c + w].wait()
                at = slice(starts[w], starts[w] + widths[w])
                product = jnp.dot(
                    piece,
                    weight_ref[cuts[c] : cuts[c + 1], at],
                    preferred_element_type=jnp.float32,
                )
                if c:
                    product = product + sums_ref[:, at]
                sums_ref[:, at] = product
        gate_copy.wait()
        gate_sums = dot_nt(normed, gate_ref[...])
        pad = jnp.zeros((rows, LANES - gate_count), jnp.float32)
        extra = jnp.concatenate([gate_sums, pad], axis=1)
        lane = lax.broadcasted_iota(jnp.int32, (rows, LANES), 1)
        sums_ref[:, width:] = jnp.where(lane == gate_count, squares, extra)
        for d in range(size):
            outs[d][...] = sums_ref[pl.ds(partner_of(position, size, d, False), 1), :]

    return call(
        body,
        [struct((1, width + LANES), jnp.float32)] * size,
        [ANY_SPEC] * 6,
        [streamed(a) for a in (tokens, norm_gain.reshape(1, -1), *weights, gates)],
        [
            pltpu.VMEM(tokens.shape, tokens.dtype),
            pltpu.VMEM((1, columns), norm_gain.dtype),
            pltpu.VMEM((columns, width), query_weight.dtype),
            pltpu.VMEM((gate_count, columns), gates.dtype),
            pltpu.VMEM((rows, width + LANES), jnp.float32),
            pltpu.SemaphoreType.DMA((len(cuts) - 1, 3)),
            pltpu.SemaphoreType.DMA(()),
            pltpu.SemaphoreType.DMA(()),
            pltpu.SemaphoreType.DMA(()),
        ],
        limit=16,
    )


def prepare(state_matrix, block_input, block_logf, lengths):
    _, heads, dv, dk = state_matrix.shape
    span = (heads, SPAN_LOCATIONS)

    def body(state_hbm, input_ref, logf_ref, lengths_ref, high_ref, low_ref, log_ref, *rest):
        sum_ref, state_ref, sems = rest
        copies = [
            pltpu.make_async_copy(state_hbm.at[0, h], state_ref.at[h], sems.at[h])
            for h in range(heads)
        ]
        for copy in copies:
            copy.start()
        live = jnp.broadcast_to(lengths_ref[...] & (SPAN_LOCATIONS - 1), span)
        inside = lax.broadcasted_iota(jnp.int32, span, 1) < live
        rest = jnp.where(inside, logf_ref[0], 0.0)
        square = (SPAN_LOCATIONS, SPAN_LOCATIONS)
        upto = (
            lax.broadcasted_iota(jnp.int32, square, 0) <= lax.broadcasted_iota(jnp.int32, square, 1)
        ).astype(jnp.float32).astype(jnp.bfloat16)
        cumulative = jnp.zeros(span, jnp.float32)
        for _ in range(3):
            term = rest.astype(jnp.bfloat16)
            rest = rest - term.astype(jnp.float32)
            cumulative = cumulative + jnp.dot(term, upto, preferred_element_type=jnp.float32)
        total = cumulative[:, SPAN_LOCATIONS - 1 :]
        sum_ref[...] = jnp.broadcast_to(total, (heads, LANES))
        log_ref[...] = jnp.where(inside, total - cumulative + input_ref[0], -jnp.inf)
        for h in range(heads):
            copies[h].wait()
            state = state_ref[h]
            high = state.astype(jnp.bfloat16)
            high_ref[h] = high
            low_ref[h] = (state - high.astype(jnp.float32)).astype(jnp.bfloat16)

    term = struct((heads, dv, dk), jnp.bfloat16)
    return call(
        body,
        [term, term, struct(span, jnp.float32), struct((heads, LANES), jnp.float32)],
        [ANY_SPEC] + [VMEM_SPEC] * 3,
        [streamed(state_matrix), block_input, block_logf, lengths.reshape(1, 1)],
        [
            pltpu.VMEM((heads, dv, dk), state_matrix.dtype),
            pltpu.SemaphoreType.DMA((heads,)),
        ],
    )


def recall(
    parts,
    forget_bias,
    prepared,
    state_normalizer,
    state_max,
    block_keys,
    block_values,
):
    *state_terms, cache_base, logf_sum = prepared
    heads, dv, dk = state_terms[0].shape
    all_heads = heads * lax.axis_size("tp")
    scale = dk ** (-0.5)
    count = len(parts)

    def body(*refs):
        (
            bias_ref,
            high_ref,
            low_ref,
            normalizer_ref,
            max_ref,
            keys_ref,
            values_ref,
            base_ref,
            sum_ref,
            out_ref,
        ) = refs[count:]
        half = lax.axis_index("tp")
        row = refs[0][...]
        for r in refs[1:count]:
            row = row + r[...]
        q_end, k_end = heads * dk, 2 * heads * dk
        v_end = k_end + heads * dv
        extra = row[:, v_end:]
        squares = extra[:, 2 * all_heads : 2 * all_heads + 1]
        row_scale = lax.rsqrt(squares / D + epsilon)
        row = row[:, :v_end] * row_scale

        def by_head(start, size):
            return jnp.concatenate(
                [row[:, start + h * size : start + (h + 1) * size] for h in range(heads)], axis=0
            ).astype(jnp.bfloat16)

        query, key, value = by_head(0, dk), by_head(q_end, dk), by_head(k_end, dv)
        gates = jnp.broadcast_to(extra * row_scale, (heads, LANES))
        lane = lax.broadcasted_iota(jnp.int32, (heads, LANES), 1)
        head = lax.broadcasted_iota(jnp.int32, (heads, LANES), 0)

        def column(values, first):
            return jnp.sum(jnp.where(lane == head + first, values, 0.0), axis=1, keepdims=True)

        lane_h = lax.broadcasted_iota(jnp.int32, (heads, heads), 1)
        head_h = lax.broadcasted_iota(jnp.int32, (heads, heads), 0)

        def own_column(ref):
            values = jnp.broadcast_to(ref[...], (heads, heads))
            return jnp.sum(jnp.where(lane_h == head_h, values, 0.0), axis=1, keepdims=True)

        new_input = column(gates, half * heads)
        new_logf = jax.nn.log_sigmoid(
            column(gates, all_heads + half * heads) + own_column(bias_ref)
        )
        total = sum_ref[:, :1] + new_logf
        carried_log = total + own_column(max_ref)
        cache_log = base_ref[...] + new_logf
        stable = jnp.maximum(
            jnp.maximum(carried_log, jnp.max(cache_log, axis=1, keepdims=True)), new_input
        )
        carried_weight = jnp.exp(carried_log - stable)
        new_weight = jnp.exp(new_input - stable)
        cache_weight = jnp.exp(cache_log - stable)

        def pick(make, size):
            rows = lax.broadcasted_iota(jnp.int32, (heads, size), 0)
            out = jnp.zeros((heads, size), jnp.float32)
            for h in range(heads):
                out = jnp.where(rows == h, make(h), out)
            return out

        scores = pick(lambda h: dot_nt(query, keys_ref[0, h]), SPAN_LOCATIONS)
        mixing = (scores * scale * cache_weight).astype(jnp.bfloat16)
        query_wide = query.astype(jnp.float32)
        own_term = (
            jnp.sum(query_wide * key.astype(jnp.float32), axis=1, keepdims=True)
            * scale
            * new_weight
        )

        def carry(h):
            return dot_nt(query, high_ref[h]) + dot_nt(query, low_ref[h])

        carried = pick(carry, dv)
        from_cache = pick(
            lambda h: jnp.dot(mixing, values_ref[0, h], preferred_element_type=jnp.float32), dv
        )
        numerator = carried_weight * carried + from_cache + own_term * value.astype(jnp.float32)
        normalizer = (
            carried_weight * jnp.sum(normalizer_ref[0] * query_wide, axis=1, keepdims=True)
            + jnp.sum(mixing.astype(jnp.float32), axis=1, keepdims=True)
            + own_term
        )
        divisor = jnp.maximum(jnp.maximum(jnp.abs(normalizer), jnp.exp(-stable)), 1.0)
        out_ref[...] = (numerator / divisor).astype(jnp.bfloat16)

    return call(
        body,
        [struct((heads, dv), jnp.bfloat16)],
        [VMEM_SPEC] * (count + 9),
        (
            *parts,
            forget_bias.reshape(1, -1),
            *[resident(term) for term in state_terms],
            state_normalizer,
            state_max,
            resident(block_keys),
            resident(block_values),
            cache_base,
            logf_sum,
        ),
    )[0]


def attend(pieces, out_weight):
    size = len(pieces)
    heads, dv = pieces[0].shape

    def body(*refs):
        weight_ref, out_ref, hidden_ref = refs[size:]
        position = lax.axis_index("kv")
        for n, d in enumerate([0, *distances(size)]):
            piece = refs[n][...].astype(jnp.float32)
            at = pl.ds(partner_of(position, size, d, True), 1)
            for h in range(heads):
                hidden_ref[at, h * dv : (h + 1) * dv] = piece[h : h + 1]
        out_ref[...] = jnp.dot(
            hidden_ref[...].astype(jnp.bfloat16),
            weight_ref[...],
            preferred_element_type=jnp.float32,
        ).astype(jnp.bfloat16)

    return call(
        body,
        [struct((size, out_weight.shape[1]), jnp.bfloat16)],
        [VMEM_SPEC] * (size + 1),
        (*pieces, resident(out_weight)),
        [pltpu.VMEM((size, heads * dv), jnp.float32)],
    )[0]


def add_features(refs, partners, gain_ref, up_ref, product, squares):
    size = lax.axis_size("kv")
    for ref, d in zip(refs, partners):
        columns = ref.shape[1]
        j = partner_of(lax.axis_index("kv"), size, d, True)
        at = pl.ds(pl.multiple_of(j * columns, columns), columns)
        wide = ref[...].astype(jnp.float32)
        squares = squares + jnp.sum(wide * wide, axis=1, keepdims=True)
        mixer_in = (wide * gain_ref[:, at]).astype(jnp.bfloat16)
        product = product + dot_nt(mixer_in, up_ref[:, at])
    return product, squares


def absorb(pieces, partners, mixer_gain, up_weight):
    rows = pieces[0].shape[0]
    units = up_weight.shape[0]
    count = len(pieces)

    def body(*refs):
        gain_ref, up_ref, product_ref, squares_ref = refs[count:]
        product, squares = add_features(
            refs[:count],
            partners,
            gain_ref,
            up_ref,
            jnp.zeros((rows, units), jnp.float32),
            jnp.zeros((rows, 1), jnp.float32),
        )
        product_ref[...] = product
        squares_ref[...] = jnp.broadcast_to(squares, (rows, LANES))

    return call(
        body,
        [struct((rows, units), jnp.float32), struct((rows, LANES), jnp.float32)],
        [VMEM_SPEC] * (count + 2),
        (*pieces, mixer_gain, up_weight),
        flops=20000000000,
    )


def mix(pieces, partners, before, residual, mixer_gain, up_weight, down_weight):
    size = lax.axis_size("kv")
    count = len(pieces)
    rows, columns = residual.shape
    blocks = [*distances(size), 0]
    share = columns // 2

    def body(*refs):
        product_ref, squares_ref, residual_ref, gain_ref, up_ref, down_ref, *outs = refs[count:]
        position = lax.axis_index("kv")
        product, squares = add_features(
            refs[:count], partners, gain_ref, up_ref, product_ref[...], squares_ref[:, :1]
        )
        scaled = product * lax.rsqrt(squares / D + epsilon)
        activated = jnp.square(jnp.maximum(scaled, 0.0)).astype(jnp.bfloat16)
        for n, d in enumerate(blocks):
            j = partner_of(position, size, d, False)
            at = pl.ds(pl.multiple_of(j * columns, columns), columns)
            terms = jnp.dot(activated, down_ref[:, at], preferred_element_type=jnp.float32)
            if d == 0:
                half = lax.broadcasted_iota(jnp.int32, (rows, columns), 1) // share
                kept = residual_ref[...].astype(jnp.float32)
                terms = terms + jnp.where(half == lax.axis_index("tp"), kept, 0.0)
            outs[n][...] = terms

    return call(
        body,
        [struct((rows, columns), jnp.float32)] * len(blocks),
        [VMEM_SPEC] * (count + 6),
        (*pieces, *before, residual, mixer_gain, up_weight, down_weight),
        flops=20000000000,
    )


def exchange_pairs(size, cores, distance):
    return [
        (i * cores + t, j * cores + (cores - 1 - t))
        for i, j in partner_pairs(size, distance)
        for t in range(cores)
    ]


def distances(size):
    return [*range(size // 2, size), *range(1, size // 2)]


def to_partners(outgoing, crossed):
    size, cores = lax.axis_size("kv"), lax.axis_size("tp")
    received = []
    for d in distances(size):
        if crossed:
            pairs = exchange_pairs(size, cores, d)
            received.append(lax.ppermute(outgoing[d], ("kv", "tp"), pairs))
        else:
            received.append(lax.ppermute(outgoing[d], "kv", partner_pairs(size, d)))
    return received


def direct(mesh, arrays_shape):
    size, cores = mesh["kv"], mesh["tp"]
    sequences, features = arrays_shape
    groups = mesh["dp"] * size
    return (
        2 < size <= DIRECT_LIMIT
        and cores == 2
        and sequences == groups
        and features % (size * 2 * LANES) == 0
    )


def shards_direct(
    tokens,
    norm_gain,
    query_weight,
    key_weight,
    value_weight,
    gate_weight,
    forget_bias,
    state_matrix,
    state_normalizer,
    state_max,
    block_keys,
    block_values,
    block_input,
    block_logf,
    lengths,
    out_weight,
    mixer_gain,
    up_weight,
    down_weight,
):
    head_half = lax.axis_index("tp")
    size = lax.axis_size("kv")
    swap = [(0, 1), (1, 0)]
    parts = project(tokens, norm_gain, query_weight, key_weight, value_weight, gate_weight)
    prepared = prepare(state_matrix, block_input, block_logf, lengths)
    parts = [parts[0]] + to_partners(parts, False)
    hidden = recall(
        parts,
        forget_bias,
        prepared,
        state_normalizer,
        state_max,
        block_keys,
        block_values,
    )
    pieces = [hidden] + to_partners([hidden] * size, False)
    partial_out = attend(pieces, out_weight)
    other_out = lax.ppermute(partial_out, "tp", swap)
    attended = partial_out.astype(jnp.float32) + other_out.astype(jnp.float32)
    residual = (tokens.astype(jnp.float32) + attended).astype(jnp.bfloat16)
    gain = mixer_gain.reshape(1, -1)
    pieces = to_partners([residual] * size, True)
    order = distances(size)
    up_weight, down_weight = resident(up_weight), resident(down_weight)
    absorbed = absorb([residual, pieces[0]], [0, order[0]], gain, up_weight)
    *terms, own = mix(
        pieces[1:], order[1:], absorbed, residual, gain, up_weight, down_weight
    )
    outgoing = dict(zip(order, terms))
    total = own
    for term in to_partners(outgoing, True):
        total = total + term
    share = tokens.shape[1] // 2
    other = lax.dynamic_slice_in_dim(total, (1 - head_half) * share, share, 1)
    kept = lax.dynamic_slice_in_dim(total, head_half * share, share, 1)
    return (kept + lax.ppermute(other, "tp", swap)).astype(jnp.bfloat16)


def mapped(mesh, function):
    return jax.shard_map(
        function,
        mesh=mesh,
        in_specs=(
            P("dp", "kv"),
            P("kv"),
            P("kv", "tp"),
            P("kv", "tp"),
            P("kv", "tp"),
            P(),
            P("tp"),
            P(("dp", "kv"), "tp", None, None),
            P(("dp", "kv"), "tp", None),
            P(("dp", "kv"), "tp"),
            P(("dp", "kv"), "tp", None, None),
            P(("dp", "kv"), "tp", None, None),
            P(("dp", "kv"), "tp", None),
            P(("dp", "kv"), "tp", None),
            P(("dp", "kv")),
            P("tp", "kv"),
            P(),
            P(("kv", "tp"), None),
            P(("kv", "tp"), None),
        ),
        out_specs=P("dp", ("kv", "tp")),
        check_vma=False,
    )


def solution(mesh):
    sizes = dict(mesh.shape)

    def whole(*arrays):
        return mapped(mesh, shards_general)(*arrays)

    def small(*arrays):
        if not direct(sizes, arrays[0].shape):
            return whole(*arrays)
        return mapped(mesh, shards_direct)(*arrays)

    if not 2 < sizes["kv"] <= DIRECT_LIMIT:
        return whole
    return small
```

```python
import jax
import jax.numpy as jnp
from jax import lax
from jax.experimental import pallas as pl
from jax.experimental.pallas import tpu as pltpu
from jax.sharding import PartitionSpec as P

D = 4096
DK = 256
DV = 512
SPAN_LOCATIONS = 64


epsilon = 1e-06
highest = lax.Precision.HIGHEST


def memory_cell(
    query,
    key,
    value,
    gates,
    forget_bias,
    state_matrix,
    state_normalizer,
    state_max,
    block_keys,
    block_values,
    block_input,
    block_logf,
    lengths,
):
    live = lengths % SPAN_LOCATIONS
    positions = lax.broadcasted_iota(jnp.int32, (1, 1, SPAN_LOCATIONS), 2)
    inside = positions < live[:, None, None]
    new_input = gates[:, 0]
    new_logf = jax.nn.log_sigmoid(gates[:, 1] + forget_bias)
    cumulative = jnp.cumsum(jnp.where(inside, block_logf, jnp.float32(0.0)), axis=2)
    total = cumulative[:, :, -1] + new_logf
    carried_log = total + state_max
    cache_log = jnp.where(inside, total[:, :, None] - cumulative + block_input, -jnp.inf)
    stable = jnp.maximum(jnp.maximum(carried_log, jnp.max(cache_log, axis=2)), new_input)
    carried_weight = jnp.exp(carried_log - stable)
    new_weight = jnp.exp(new_input - stable)
    cache_weight = jnp.exp(cache_log - stable[:, :, None])
    scores = jnp.einsum("bhk,bhsk->bhs", query, block_keys, preferred_element_type=jnp.float32)
    mixing = (scores * DK ** (-0.5) * cache_weight).astype(jnp.bfloat16)
    query_wide = query.astype(jnp.float32)
    own_term = jnp.sum(query_wide * key.astype(jnp.float32), axis=2) * DK ** (-0.5) * new_weight
    carried = jnp.einsum("bhvk,bhk->bhv", state_matrix, query_wide, precision=highest)
    from_cache = jnp.einsum(
        "bhs,bhsv->bhv", mixing, block_values, preferred_element_type=jnp.float32
    )
    numerator = (
        carried_weight[:, :, None] * carried
        + from_cache
        + own_term[:, :, None] * value.astype(jnp.float32)
    )
    normalizer = (
        carried_weight * jnp.sum(state_normalizer * query_wide, axis=2)
        + jnp.sum(mixing.astype(jnp.float32), axis=2)
        + own_term
    )
    divisor = jnp.maximum(jnp.maximum(jnp.abs(normalizer), jnp.exp(-stable)), jnp.float32(1.0))
    hidden = numerator / divisor[:, :, None]
    return hidden.astype(jnp.bfloat16)


def absorb_columns(mixer_gain, up_weight):

    def absorb(carry, piece, start):
        widened = piece.astype(jnp.float32)
        mixer_in = (widened * mixer_gain).astype(jnp.bfloat16)
        product = lax.dot_general(
            mixer_in, up_weight, (((1,), (1,)), ((), ())), preferred_element_type=jnp.float32
        )
        return (product, jnp.sum(widened * widened, axis=1))

    return absorb


def down_terms(carry, down_weight):
    accumulated, squares = carry
    scaled = accumulated * lax.rsqrt(squares / D + epsilon)[:, None]
    activated = jnp.square(jax.nn.relu(scaled)).astype(jnp.bfloat16)
    return jnp.dot(activated, down_weight, preferred_element_type=jnp.float32)


DIRECT_LIMIT = 8


def partner_pairs(size, distance):
    if size & (size - 1) == 0:
        return [(i, i ^ distance) for i in range(size)]
    return [(i, (i + distance) % size) for i in range(size)]


def partner_of(position, size, distance, receiving):
    if size & (size - 1) == 0:
        return position ^ distance
    return (position - distance) % size if receiving else (position + distance) % size


def gather_direct(piece, axis):
    size = lax.axis_size(axis)
    if size > DIRECT_LIMIT:
        return lax.all_gather(piece, axis, axis=0)
    position = lax.axis_index(axis)
    received = [piece] + [
        lax.ppermute(piece, axis, partner_pairs(size, d)) for d in range(1, size)
    ]
    stacked = jnp.stack(received)
    places = jnp.arange(size)
    if size & (size - 1) == 0:
        order = position ^ places
    else:
        order = (position - places) % size
    return stacked[order]


def scatter_sum_direct(parts, axis):
    size = lax.axis_size(axis)
    if size > DIRECT_LIMIT:
        return lax.psum_scatter(parts, axis, scatter_dimension=0, tiled=False)
    position = lax.axis_index(axis)

    def entry(index):
        return lax.dynamic_index_in_dim(parts, index, 0, keepdims=False)

    total = entry(position)
    for d in range(1, size):
        out = entry(partner_of(position, size, d, False))
        total = total + lax.ppermute(out, axis, partner_pairs(size, d))
    return total


def shards_general(
    tokens,
    norm_gain,
    query_weight,
    key_weight,
    value_weight,
    gate_weight,
    forget_bias,
    state_matrix,
    state_normalizer,
    state_max,
    block_keys,
    block_values,
    block_input,
    block_logf,
    lengths,
    out_weight,
    mixer_gain,
    up_weight,
    down_weight,
):
    position = lax.axis_index("kv")
    head_half = lax.axis_index("tp")
    columns = tokens.shape[1]
    local_heads = forget_bias.shape[0]
    local_rows = lengths.shape[0]
    widened = tokens.astype(jnp.float32)
    squares = jnp.sum(widened * widened, axis=1)
    normed = (widened * norm_gain).astype(jnp.bfloat16)
    gate_rows = lax.dynamic_slice_in_dim(gate_weight, position * columns, columns, 0)
    gate_rows = lax.dynamic_slice_in_dim(
        gate_rows, head_half * local_heads, local_heads, 2
    ).reshape(columns, 2 * local_heads)
    query_part = jnp.dot(normed, query_weight, preferred_element_type=jnp.float32)
    key_part = jnp.dot(normed, key_weight, preferred_element_type=jnp.float32)
    value_part = jnp.dot(normed, value_weight, preferred_element_type=jnp.float32)
    gate_part = jnp.dot(normed, gate_rows, preferred_element_type=jnp.float32)
    parts = jnp.concatenate(
        [query_part, key_part, value_part, gate_part, squares[:, None]], axis=1
    )
    parts = parts.reshape(-1, local_rows, parts.shape[1])
    sums = scatter_sum_direct(parts, "kv")
    q_end = query_part.shape[1]
    k_end = q_end + key_part.shape[1]
    v_end = k_end + value_part.shape[1]
    g_end = v_end + gate_part.shape[1]
    query_sum, key_sum, value_sum, gate_sum, own_squares = (
        sums[:, :q_end],
        sums[:, q_end:k_end],
        sums[:, k_end:v_end],
        sums[:, v_end:g_end],
        sums[:, g_end],
    )
    row_scale = lax.rsqrt(own_squares / D + epsilon)[:, None]
    query = (query_sum * row_scale).astype(jnp.bfloat16).reshape(local_rows, local_heads, DK)
    key = (key_sum * row_scale).astype(jnp.bfloat16).reshape(local_rows, local_heads, DK)
    value = (value_sum * row_scale).astype(jnp.bfloat16).reshape(local_rows, local_heads, DV)
    gates = (gate_sum * row_scale).reshape(local_rows, 2, local_heads)
    hidden = memory_cell(
        query,
        key,
        value,
        gates,
        forget_bias,
        state_matrix,
        state_normalizer,
        state_max,
        block_keys,
        block_values,
        block_input,
        block_logf,
        lengths,
    )
    hidden = hidden.reshape(local_rows, local_heads * DV)
    every_hidden = gather_direct(hidden, "kv").reshape(-1, hidden.shape[1])
    partial_out = jnp.dot(
        every_hidden, out_weight, preferred_element_type=jnp.float32
    ).astype(jnp.bfloat16)
    attended = jnp.sum(gather_direct(partial_out, "tp").astype(jnp.float32), axis=0)
    residual = (widened + attended).astype(jnp.bfloat16)
    absorb = absorb_columns(mixer_gain, up_weight)
    hidden_units = up_weight.shape[0]
    rows = residual.shape[0]
    initial = (jnp.zeros((rows, hidden_units), jnp.float32), jnp.zeros((rows,), jnp.float32))
    pieces = gather_direct(residual, "kv")
    whole = jnp.moveaxis(pieces, 0, 1).reshape(rows, -1)
    carry = absorb(initial, whole, jnp.int32(0))
    terms = down_terms(carry, down_weight)
    share = columns // lax.axis_size("tp")
    terms = terms.reshape(rows, -1, lax.axis_size("tp"), share)
    by_core = scatter_sum_direct(jnp.moveaxis(terms, 2, 0), "tp")
    mixed_terms = scatter_sum_direct(jnp.moveaxis(by_core, 1, 0), "kv")
    own_residual = lax.dynamic_slice_in_dim(residual, head_half * share, share, 1)
    return (own_residual.astype(jnp.float32) + mixed_terms).astype(jnp.bfloat16)


def dot_nt(left, right):
    return lax.dot_general(
        left, right, (((1,), (1,)), ((), ())), preferred_element_type=jnp.float32
    )


VMEM_SPEC = pl.BlockSpec(memory_space=pltpu.VMEM)
SMEM_SPEC = pl.BlockSpec(memory_space=pltpu.SMEM)
ANY_SPEC = pl.BlockSpec(memory_space=pl.ANY)


def call(body, outs, in_specs, args, scratch=(), limit=8, flops=20000000000, aliases=None):
    return pl.pallas_call(
        body,
        out_shape=outs,
        in_specs=in_specs,
        out_specs=[VMEM_SPEC] * len(outs),
        scratch_shapes=list(scratch),
        input_output_aliases=aliases or {},
        compiler_params=pltpu.CompilerParams(vmem_limit_bytes=limit << 20),
        cost_estimate=pl.CostEstimate(flops=flops, bytes_accessed=1000000, transcendentals=0),
    )(*args)


def resident(weight):
    return pltpu.with_memory_space_constraint(weight, pltpu.VMEM)


def streamed(weight):
    return pltpu.with_memory_space_constraint(weight, pltpu.HBM)


def struct(shape, kind):
    return jax.ShapeDtypeStruct(shape, kind)


LANES = 128


def project(tokens, norm_gain, query_weight, key_weight, value_weight, gate_weight):
    rows, columns = tokens.shape
    size = lax.axis_size("kv")
    weights = (query_weight, key_weight, value_weight)
    widths = [w.shape[1] for w in weights]
    starts = [sum(widths[:i]) for i in range(3)]
    width = sum(widths)
    gate_count = gate_weight.shape[1] * gate_weight.shape[2]
    gates = jnp.transpose(gate_weight, (1, 2, 0)).reshape(gate_count, -1)
    cuts = [0, columns]

    def body(tokens_hbm, gain_hbm, q_hbm, k_hbm, v_hbm, gate_hbm, *rest):
        outs = rest[:size]
        tokens_ref, gain_ref, weight_ref, gate_ref, sums_ref = rest[size : size + 5]
        sems, gate_sem, tokens_sem, gain_sem = rest[size + 5 :]
        position = lax.axis_index("kv")
        tokens_copy = pltpu.make_async_copy(tokens_hbm, tokens_ref, tokens_sem)
        gain_copy = pltpu.make_async_copy(gain_hbm, gain_ref, gain_sem)
        tokens_copy.start()
        gain_copy.start()
        copies = []
        for c in range(len(cuts) - 1):
            at = pl.ds(cuts[c], cuts[c + 1] - cuts[c])
            for w, source in enumerate((q_hbm, k_hbm, v_hbm)):
                copy = pltpu.make_async_copy(
                    source.at[at, :],
                    weight_ref.at[at, pl.ds(starts[w], widths[w])],
                    sems.at[c, w],
                )
                copy.start()
                copies.append(copy)
        gate_copy = pltpu.make_async_copy(
            gate_hbm.at[:, pl.ds(pl.multiple_of(position * columns, columns), columns)],
            gate_ref,
            gate_sem,
        )
        gate_copy.start()
        tokens_copy.wait()
        gain_copy.wait()
        widened = tokens_ref[...].astype(jnp.float32)
        squares = jnp.sum(widened * widened, axis=1, keepdims=True)
        normed = (widened * gain_ref[...]).astype(jnp.bfloat16)
        for c in range(len(cuts) - 1):
            piece = normed[:, cuts[c] : cuts[c + 1]]
            for w in range(3):
                copies[3 * c + w].wait()
                at = slice(starts[w], starts[w] + widths[w])
                product = jnp.dot(
                    piece,
                    weight_ref[cuts[c] : cuts[c + 1], at],
                    preferred_element_type=jnp.float32,
                )
                if c:
                    product = product + sums_ref[:, at]
                sums_ref[:, at] = product
        gate_copy.wait()
        gate_sums = dot_nt(normed, gate_ref[...])
        pad = jnp.zeros((rows, LANES - gate_count), jnp.float32)
        extra = jnp.concatenate([gate_sums, pad], axis=1)
        lane = lax.broadcasted_iota(jnp.int32, (rows, LANES), 1)
        sums_ref[:, width:] = jnp.where(lane == gate_count, squares, extra)
        for d in range(size):
            outs[d][...] = sums_ref[pl.ds(partner_of(position, size, d, False), 1), :]

    return call(
        body,
        [struct((1, width + LANES), jnp.float32)] * size,
        [ANY_SPEC] * 6,
        [streamed(a) for a in (tokens, norm_gain.reshape(1, -1), *weights, gates)],
        [
            pltpu.VMEM(tokens.shape, tokens.dtype),
            pltpu.VMEM((1, columns), norm_gain.dtype),
            pltpu.VMEM((columns, width), query_weight.dtype),
            pltpu.VMEM((gate_count, columns), gates.dtype),
            pltpu.VMEM((rows, width + LANES), jnp.float32),
            pltpu.SemaphoreType.DMA((len(cuts) - 1, 3)),
            pltpu.SemaphoreType.DMA(()),
            pltpu.SemaphoreType.DMA(()),
            pltpu.SemaphoreType.DMA(()),
        ],
        limit=16,
    )


def prepare(forget_bias, state_normalizer, state_max, block_input, block_logf, lengths):
    _, heads, dk = state_normalizer.shape
    span = (heads, SPAN_LOCATIONS)

    def body(
        bias_ref, normalizer_ref, max_ref, input_ref, logf_ref, lengths_ref, out_ref
    ):
        live = jnp.broadcast_to(lengths_ref[:, :1] & (SPAN_LOCATIONS - 1), span)
        inside = lax.broadcasted_iota(jnp.int32, span, 1) < live
        rest = jnp.where(inside, logf_ref[0], 0.0)
        square = (SPAN_LOCATIONS, SPAN_LOCATIONS)
        upto = (
            lax.broadcasted_iota(jnp.int32, square, 0) <= lax.broadcasted_iota(jnp.int32, square, 1)
        ).astype(jnp.float32).astype(jnp.bfloat16)
        cumulative = jnp.zeros(span, jnp.float32)
        for _ in range(3):
            term = rest.astype(jnp.bfloat16)
            rest = rest - term.astype(jnp.float32)
            cumulative = cumulative + jnp.dot(term, upto, preferred_element_type=jnp.float32)
        total = cumulative[:, SPAN_LOCATIONS - 1 :]
        base = jnp.where(inside, total - cumulative + input_ref[0], -jnp.inf)
        lane_h = lax.broadcasted_iota(jnp.int32, (heads, heads), 1)
        head_h = lax.broadcasted_iota(jnp.int32, (heads, heads), 0)

        def column(ref):
            values = jnp.broadcast_to(ref[...], (heads, heads))
            return jnp.sum(jnp.where(lane_h == head_h, values, 0.0), axis=1, keepdims=True)

        lane = lax.broadcasted_iota(jnp.int32, (heads, LANES), 1)
        scalars = jnp.where(lane == 0, total, 0.0)
        scalars = jnp.where(lane == 1, column(max_ref), scalars)
        scalars = jnp.where(lane == 2, column(bias_ref), scalars)
        out_ref[:, :dk] = normalizer_ref[0]
        pad = jnp.zeros((heads, LANES - SPAN_LOCATIONS), jnp.float32)
        out_ref[:, dk : dk + LANES] = jnp.concatenate([base, pad], axis=1)
        out_ref[:, dk + LANES :] = scalars

    return call(
        body,
        [struct((heads, dk + 2 * LANES), jnp.float32)],
        [VMEM_SPEC] * 6,
        [
            forget_bias.reshape(1, -1),
            state_normalizer,
            state_max,
            block_input,
            block_logf,
            jnp.pad(lengths, (0, LANES - 1)).reshape(1, -1),
        ],
    )[0]


def recall(parts, prepared, state_matrix, block_keys, block_values):
    _, heads, dv, dk = state_matrix.shape
    all_heads = heads * lax.axis_size("tp")
    scale = dk ** (-0.5)
    count = len(parts)

    def body(*refs):
        small_ref, state_ref, keys_ref, values_ref, out_ref = refs[count:]
        half = 1 - lax.axis_index("tp")
        row = refs[0][...]
        for r in refs[1:count]:
            row = row + r[...]
        q_end, k_end = heads * dk, 2 * heads * dk
        v_end = k_end + heads * dv
        extra = row[:, v_end:]
        squares = extra[:, 2 * all_heads : 2 * all_heads + 1]
        row_scale = lax.rsqrt(squares / D + epsilon)
        row = row[:, :v_end] * row_scale

        def by_head(start, size):
            return jnp.concatenate(
                [row[:, start + h * size : start + (h + 1) * size] for h in range(heads)], axis=0
            ).astype(jnp.bfloat16)

        query, key, value = by_head(0, dk), by_head(q_end, dk), by_head(k_end, dv)
        gates = jnp.broadcast_to(extra * row_scale, (heads, LANES))
        lane = lax.broadcasted_iota(jnp.int32, (heads, LANES), 1)
        head = lax.broadcasted_iota(jnp.int32, (heads, LANES), 0)

        def column(values, first):
            return jnp.sum(jnp.where(lane == head + first, values, 0.0), axis=1, keepdims=True)

        small = small_ref[...]
        cache_base = small[:, dk : dk + SPAN_LOCATIONS]
        logf_sum, state_max, bias = (
            small[:, dk + LANES + i : dk + LANES + i + 1] for i in range(3)
        )
        new_input = column(gates, half * heads)
        new_logf = jax.nn.log_sigmoid(column(gates, all_heads + half * heads) + bias)
        carried_log = logf_sum + new_logf + state_max
        cache_log = cache_base + new_logf
        stable = jnp.maximum(
            jnp.maximum(carried_log, jnp.max(cache_log, axis=1, keepdims=True)), new_input
        )
        carried_weight = jnp.exp(carried_log - stable)
        new_weight = jnp.exp(new_input - stable)
        cache_weight = jnp.exp(cache_log - stable)

        def pick(make, size):
            rows = lax.broadcasted_iota(jnp.int32, (heads, size), 0)
            out = jnp.zeros((heads, size), jnp.float32)
            for h in range(heads):
                out = jnp.where(rows == h, make(h), out)
            return out

        scores = pick(lambda h: dot_nt(query, keys_ref[0, h]), SPAN_LOCATIONS)
        mixing = (scores * scale * cache_weight).astype(jnp.bfloat16)
        query_wide = query.astype(jnp.float32)
        own_term = (
            jnp.sum(query_wide * key.astype(jnp.float32), axis=1, keepdims=True)
            * scale
            * new_weight
        )

        def carry(h):
            state = state_ref[0, h]
            high = state.astype(jnp.bfloat16)
            low = (state - high.astype(jnp.float32)).astype(jnp.bfloat16)
            return dot_nt(query, high) + dot_nt(query, low)

        carried = pick(carry, dv)
        from_cache = pick(
            lambda h: jnp.dot(mixing, values_ref[0, h], preferred_element_type=jnp.float32), dv
        )
        numerator = carried_weight * carried + from_cache + own_term * value.astype(jnp.float32)
        normalizer = (
            carried_weight * jnp.sum(small[:, :dk] * query_wide, axis=1, keepdims=True)
            + jnp.sum(mixing.astype(jnp.float32), axis=1, keepdims=True)
            + own_term
        )
        divisor = jnp.maximum(jnp.maximum(jnp.abs(normalizer), jnp.exp(-stable)), 1.0)
        out_ref[...] = (numerator / divisor).astype(jnp.bfloat16)

    return call(
        body,
        [struct((heads, dv), jnp.bfloat16)],
        [VMEM_SPEC] * (count + 4),
        (*parts, prepared, *[resident(w) for w in (state_matrix, block_keys, block_values)]),
    )[0]


def attend(pieces, out_weight):
    size = len(pieces)
    heads, dv = pieces[0].shape

    def body(*refs):
        weight_ref, out_ref, hidden_ref = refs[size:]
        position = lax.axis_index("kv")
        for n, d in enumerate([*distances(size), 0]):
            piece = refs[n][...].astype(jnp.float32)
            at = pl.ds(partner_of(position, size, d, True), 1)
            for h in range(heads):
                hidden_ref[at, h * dv : (h + 1) * dv] = piece[h : h + 1]
        out_ref[...] = jnp.dot(
            hidden_ref[...].astype(jnp.bfloat16),
            weight_ref[...],
            preferred_element_type=jnp.float32,
        ).astype(jnp.bfloat16)

    return call(
        body,
        [struct((size, out_weight.shape[1]), jnp.bfloat16)],
        [VMEM_SPEC] * (size + 1),
        (*pieces, resident(out_weight)),
        [pltpu.VMEM((size, heads * dv), jnp.float32)],
    )[0]


def add_features(refs, partners, gain_ref, up_ref, product, squares):
    size = lax.axis_size("kv")
    for ref, d in zip(refs, partners):
        columns = ref.shape[1]
        j = partner_of(lax.axis_index("kv"), size, d, True)
        at = pl.ds(pl.multiple_of(j * columns, columns), columns)
        wide = ref[...].astype(jnp.float32)
        squares = squares + jnp.sum(wide * wide, axis=1, keepdims=True)
        mixer_in = (wide * gain_ref[:, at]).astype(jnp.bfloat16)
        product = product + dot_nt(mixer_in, up_ref[:, at])
    return product, squares


def absorb(pieces, partners, mixer_gain, up_weight):
    rows = pieces[0].shape[0]
    units = up_weight.shape[0]
    count = len(pieces)

    def body(*refs):
        gain_ref, up_ref, product_ref, squares_ref = refs[count:]
        product, squares = add_features(
            refs[:count],
            partners,
            gain_ref,
            up_ref,
            jnp.zeros((rows, units), jnp.float32),
            jnp.zeros((rows, 1), jnp.float32),
        )
        product_ref[...] = product
        squares_ref[...] = jnp.broadcast_to(squares, (rows, LANES))

    return call(
        body,
        [struct((rows, units), jnp.float32), struct((rows, LANES), jnp.float32)],
        [VMEM_SPEC] * (count + 2),
        (*pieces, mixer_gain, up_weight),
        flops=20000000000,
    )


def mix(pieces, partners, before, residual, mixer_gain, up_weight, down_weight):
    size = lax.axis_size("kv")
    count = len(pieces)
    rows, columns = residual.shape
    blocks = [*distances(size), 0]
    share = columns // 2

    def body(*refs):
        product_ref, squares_ref, residual_ref, gain_ref, up_ref, down_ref, *outs = refs[count:]
        position = lax.axis_index("kv")
        product, squares = add_features(
            refs[:count], partners, gain_ref, up_ref, product_ref[...], squares_ref[:, :1]
        )
        scaled = product * lax.rsqrt(squares / D + epsilon)
        activated = jnp.square(jnp.maximum(scaled, 0.0)).astype(jnp.bfloat16)
        for n, d in enumerate(blocks):
            j = partner_of(position, size, d, False)
            at = pl.ds(pl.multiple_of(j * columns, columns), columns)
            terms = jnp.dot(activated, down_ref[:, at], preferred_element_type=jnp.float32)
            if d == 0:
                half = lax.broadcasted_iota(jnp.int32, (rows, columns), 1) // share
                kept = residual_ref[...].astype(jnp.float32)
                terms = terms + jnp.where(half == lax.axis_index("tp"), kept, 0.0)
            outs[n][...] = terms

    return call(
        body,
        [struct((rows, columns), jnp.float32)] * len(blocks),
        [VMEM_SPEC] * (count + 6),
        (*pieces, *before, residual, mixer_gain, up_weight, down_weight),
        flops=20000000000,
    )


def exchange_pairs(size, cores, distance):
    return [
        (i * cores + t, j * cores + (cores - 1 - t))
        for i, j in partner_pairs(size, distance)
        for t in range(cores)
    ]


def distances(size):
    return [*range(size // 2, size), *range(1, size // 2)]


def to_partners(outgoing, partners):
    size, cores = lax.axis_size("kv"), lax.axis_size("tp")
    received = []
    for d in partners:
        pairs = exchange_pairs(size, cores, d)
        received.append(lax.ppermute(outgoing[d], ("kv", "tp"), pairs))
    return received


def swapped(array):
    return lax.ppermute(array, "tp", [(0, 1), (1, 0)])


def direct(mesh, arrays_shape):
    size, cores = mesh["kv"], mesh["tp"]
    sequences, features = arrays_shape
    groups = mesh["dp"] * size
    return (
        2 < size <= DIRECT_LIMIT
        and cores == 2
        and sequences == groups
        and features % (size * 2 * LANES) == 0
    )


def shards_direct(
    tokens,
    norm_gain,
    query_weight,
    key_weight,
    value_weight,
    gate_weight,
    forget_bias,
    state_matrix,
    state_normalizer,
    state_max,
    block_keys,
    block_values,
    block_input,
    block_logf,
    lengths,
    out_weight,
    mixer_gain,
    up_weight,
    down_weight,
):
    head_half = lax.axis_index("tp")
    size = lax.axis_size("kv")
    order = distances(size)
    state_matrix = swapped(state_matrix)
    parts = project(
        tokens, norm_gain, query_weight, key_weight, value_weight, gate_weight
    )
    prepared = prepare(
        forget_bias, state_normalizer, state_max, block_input, block_logf, lengths
    )
    parts = to_partners(parts, [*order, 0])
    hidden = recall(
        parts, swapped(prepared), state_matrix, swapped(block_keys), swapped(block_values)
    )
    pieces = to_partners([hidden] * size, [*order, 0])
    partial_out = attend(pieces, out_weight)
    other_out = swapped(partial_out)
    attended = partial_out.astype(jnp.float32) + other_out.astype(jnp.float32)
    residual = (tokens.astype(jnp.float32) + attended).astype(jnp.bfloat16)
    gain = mixer_gain.reshape(1, -1)
    pieces = to_partners([residual] * size, order)
    order = distances(size)
    up_weight, down_weight = resident(up_weight), resident(down_weight)
    absorbed = absorb([residual, pieces[0]], [0, order[0]], gain, up_weight)
    *terms, own = mix(
        pieces[1:], order[1:], absorbed, residual, gain, up_weight, down_weight
    )
    outgoing = dict(zip(order, terms))
    total = own
    for term in to_partners(outgoing, order):
        total = total + term
    share = tokens.shape[1] // 2
    other = lax.dynamic_slice_in_dim(total, (1 - head_half) * share, share, 1)
    kept = lax.dynamic_slice_in_dim(total, head_half * share, share, 1)
    return (kept + swapped(other)).astype(jnp.bfloat16)


def mapped(mesh, function):
    return jax.shard_map(
        function,
        mesh=mesh,
        in_specs=(
            P("dp", "kv"),
            P("kv"),
            P("kv", "tp"),
            P("kv", "tp"),
            P("kv", "tp"),
            P(),
            P("tp"),
            P(("dp", "kv"), "tp", None, None),
            P(("dp", "kv"), "tp", None),
            P(("dp", "kv"), "tp"),
            P(("dp", "kv"), "tp", None, None),
            P(("dp", "kv"), "tp", None, None),
            P(("dp", "kv"), "tp", None),
            P(("dp", "kv"), "tp", None),
            P(("dp", "kv")),
            P("tp", "kv"),
            P(),
            P(("kv", "tp"), None),
            P(("kv", "tp"), None),
        ),
        out_specs=P("dp", ("kv", "tp")),
        check_vma=False,
    )


def solution(mesh):
    sizes = dict(mesh.shape)

    def whole(*arrays):
        return mapped(mesh, shards_general)(*arrays)

    def small(*arrays):
        if not direct(sizes, arrays[0].shape):
            return whole(*arrays)
        return mapped(mesh, shards_direct)(*arrays)

    if not 2 < sizes["kv"] <= DIRECT_LIMIT:
        return whole
    return small
```

```python
import jax
import jax.numpy as jnp
from jax import lax
from jax.experimental import pallas as pl
from jax.experimental.pallas import tpu as pltpu
from jax.sharding import PartitionSpec as P

D = 4096
DK = 256
DV = 512
SPAN_LOCATIONS = 64


epsilon = 1e-06
highest = lax.Precision.HIGHEST


def memory_cell(
    query,
    key,
    value,
    gates,
    forget_bias,
    state_matrix,
    state_normalizer,
    state_max,
    block_keys,
    block_values,
    block_input,
    block_logf,
    lengths,
):
    live = lengths % SPAN_LOCATIONS
    positions = lax.broadcasted_iota(jnp.int32, (1, 1, SPAN_LOCATIONS), 2)
    inside = positions < live[:, None, None]
    new_input = gates[:, 0]
    new_logf = jax.nn.log_sigmoid(gates[:, 1] + forget_bias)
    cumulative = jnp.cumsum(jnp.where(inside, block_logf, jnp.float32(0.0)), axis=2)
    total = cumulative[:, :, -1] + new_logf
    carried_log = total + state_max
    cache_log = jnp.where(inside, total[:, :, None] - cumulative + block_input, -jnp.inf)
    stable = jnp.maximum(jnp.maximum(carried_log, jnp.max(cache_log, axis=2)), new_input)
    carried_weight = jnp.exp(carried_log - stable)
    new_weight = jnp.exp(new_input - stable)
    cache_weight = jnp.exp(cache_log - stable[:, :, None])
    scores = jnp.einsum("bhk,bhsk->bhs", query, block_keys, preferred_element_type=jnp.float32)
    mixing = (scores * DK ** (-0.5) * cache_weight).astype(jnp.bfloat16)
    query_wide = query.astype(jnp.float32)
    own_term = jnp.sum(query_wide * key.astype(jnp.float32), axis=2) * DK ** (-0.5) * new_weight
    carried = jnp.einsum("bhvk,bhk->bhv", state_matrix, query_wide, precision=highest)
    from_cache = jnp.einsum(
        "bhs,bhsv->bhv", mixing, block_values, preferred_element_type=jnp.float32
    )
    numerator = (
        carried_weight[:, :, None] * carried
        + from_cache
        + own_term[:, :, None] * value.astype(jnp.float32)
    )
    normalizer = (
        carried_weight * jnp.sum(state_normalizer * query_wide, axis=2)
        + jnp.sum(mixing.astype(jnp.float32), axis=2)
        + own_term
    )
    divisor = jnp.maximum(jnp.maximum(jnp.abs(normalizer), jnp.exp(-stable)), jnp.float32(1.0))
    hidden = numerator / divisor[:, :, None]
    return hidden.astype(jnp.bfloat16)


def absorb_columns(mixer_gain, up_weight):

    def absorb(carry, piece, start):
        widened = piece.astype(jnp.float32)
        mixer_in = (widened * mixer_gain).astype(jnp.bfloat16)
        product = lax.dot_general(
            mixer_in, up_weight, (((1,), (1,)), ((), ())), preferred_element_type=jnp.float32
        )
        return (product, jnp.sum(widened * widened, axis=1))

    return absorb


def down_terms(carry, down_weight):
    accumulated, squares = carry
    scaled = accumulated * lax.rsqrt(squares / D + epsilon)[:, None]
    activated = jnp.square(jax.nn.relu(scaled)).astype(jnp.bfloat16)
    return jnp.dot(activated, down_weight, preferred_element_type=jnp.float32)


DIRECT_LIMIT = 8


def partner_pairs(size, distance):
    if size & (size - 1) == 0:
        return [(i, i ^ distance) for i in range(size)]
    return [(i, (i + distance) % size) for i in range(size)]


def partner_of(position, size, distance, receiving):
    if size & (size - 1) == 0:
        return position ^ distance
    return (position - distance) % size if receiving else (position + distance) % size


def gather_direct(piece, axis):
    size = lax.axis_size(axis)
    if size > DIRECT_LIMIT:
        return lax.all_gather(piece, axis, axis=0)
    position = lax.axis_index(axis)
    received = [piece] + [
        lax.ppermute(piece, axis, partner_pairs(size, d)) for d in range(1, size)
    ]
    stacked = jnp.stack(received)
    places = jnp.arange(size)
    if size & (size - 1) == 0:
        order = position ^ places
    else:
        order = (position - places) % size
    return stacked[order]


def scatter_sum_direct(parts, axis):
    size = lax.axis_size(axis)
    if size > DIRECT_LIMIT:
        return lax.psum_scatter(parts, axis, scatter_dimension=0, tiled=False)
    position = lax.axis_index(axis)

    def entry(index):
        return lax.dynamic_index_in_dim(parts, index, 0, keepdims=False)

    total = entry(position)
    for d in range(1, size):
        out = entry(partner_of(position, size, d, False))
        total = total + lax.ppermute(out, axis, partner_pairs(size, d))
    return total


def shards_general(
    tokens,
    norm_gain,
    query_weight,
    key_weight,
    value_weight,
    gate_weight,
    forget_bias,
    state_matrix,
    state_normalizer,
    state_max,
    block_keys,
    block_values,
    block_input,
    block_logf,
    lengths,
    out_weight,
    mixer_gain,
    up_weight,
    down_weight,
):
    position = lax.axis_index("kv")
    head_half = lax.axis_index("tp")
    columns = tokens.shape[1]
    local_heads = forget_bias.shape[0]
    local_rows = lengths.shape[0]
    widened = tokens.astype(jnp.float32)
    squares = jnp.sum(widened * widened, axis=1)
    normed = (widened * norm_gain).astype(jnp.bfloat16)
    gate_rows = lax.dynamic_slice_in_dim(gate_weight, position * columns, columns, 0)
    gate_rows = lax.dynamic_slice_in_dim(
        gate_rows, head_half * local_heads, local_heads, 2
    ).reshape(columns, 2 * local_heads)
    query_part = jnp.dot(normed, query_weight, preferred_element_type=jnp.float32)
    key_part = jnp.dot(normed, key_weight, preferred_element_type=jnp.float32)
    value_part = jnp.dot(normed, value_weight, preferred_element_type=jnp.float32)
    gate_part = jnp.dot(normed, gate_rows, preferred_element_type=jnp.float32)
    parts = jnp.concatenate(
        [query_part, key_part, value_part, gate_part, squares[:, None]], axis=1
    )
    parts = parts.reshape(-1, local_rows, parts.shape[1])
    sums = scatter_sum_direct(parts, "kv")
    q_end = query_part.shape[1]
    k_end = q_end + key_part.shape[1]
    v_end = k_end + value_part.shape[1]
    g_end = v_end + gate_part.shape[1]
    query_sum, key_sum, value_sum, gate_sum, own_squares = (
        sums[:, :q_end],
        sums[:, q_end:k_end],
        sums[:, k_end:v_end],
        sums[:, v_end:g_end],
        sums[:, g_end],
    )
    row_scale = lax.rsqrt(own_squares / D + epsilon)[:, None]
    query = (query_sum * row_scale).astype(jnp.bfloat16).reshape(local_rows, local_heads, DK)
    key = (key_sum * row_scale).astype(jnp.bfloat16).reshape(local_rows, local_heads, DK)
    value = (value_sum * row_scale).astype(jnp.bfloat16).reshape(local_rows, local_heads, DV)
    gates = (gate_sum * row_scale).reshape(local_rows, 2, local_heads)
    hidden = memory_cell(
        query,
        key,
        value,
        gates,
        forget_bias,
        state_matrix,
        state_normalizer,
        state_max,
        block_keys,
        block_values,
        block_input,
        block_logf,
        lengths,
    )
    hidden = hidden.reshape(local_rows, local_heads * DV)
    every_hidden = gather_direct(hidden, "kv").reshape(-1, hidden.shape[1])
    partial_out = jnp.dot(
        every_hidden, out_weight, preferred_element_type=jnp.float32
    ).astype(jnp.bfloat16)
    attended = jnp.sum(gather_direct(partial_out, "tp").astype(jnp.float32), axis=0)
    residual = (widened + attended).astype(jnp.bfloat16)
    absorb = absorb_columns(mixer_gain, up_weight)
    hidden_units = up_weight.shape[0]
    rows = residual.shape[0]
    initial = (jnp.zeros((rows, hidden_units), jnp.float32), jnp.zeros((rows,), jnp.float32))
    pieces = gather_direct(residual, "kv")
    whole = jnp.moveaxis(pieces, 0, 1).reshape(rows, -1)
    carry = absorb(initial, whole, jnp.int32(0))
    terms = down_terms(carry, down_weight)
    share = columns // lax.axis_size("tp")
    terms = terms.reshape(rows, -1, lax.axis_size("tp"), share)
    by_core = scatter_sum_direct(jnp.moveaxis(terms, 2, 0), "tp")
    mixed_terms = scatter_sum_direct(jnp.moveaxis(by_core, 1, 0), "kv")
    own_residual = lax.dynamic_slice_in_dim(residual, head_half * share, share, 1)
    return (own_residual.astype(jnp.float32) + mixed_terms).astype(jnp.bfloat16)


def dot_nt(left, right):
    return lax.dot_general(
        left, right, (((1,), (1,)), ((), ())), preferred_element_type=jnp.float32
    )


VMEM_SPEC = pl.BlockSpec(memory_space=pltpu.VMEM)
SMEM_SPEC = pl.BlockSpec(memory_space=pltpu.SMEM)
ANY_SPEC = pl.BlockSpec(memory_space=pl.ANY)


def call(body, outs, in_specs, args, scratch=(), limit=8, flops=20000000000, aliases=None):
    return pl.pallas_call(
        body,
        out_shape=outs,
        in_specs=in_specs,
        out_specs=[VMEM_SPEC] * len(outs),
        scratch_shapes=list(scratch),
        input_output_aliases=aliases or {},
        compiler_params=pltpu.CompilerParams(vmem_limit_bytes=limit << 20),
        cost_estimate=pl.CostEstimate(flops=flops, bytes_accessed=1000000, transcendentals=0),
    )(*args)


def resident(weight):
    return pltpu.with_memory_space_constraint(weight, pltpu.VMEM)


def streamed(weight):
    return pltpu.with_memory_space_constraint(weight, pltpu.HBM)


def struct(shape, kind):
    return jax.ShapeDtypeStruct(shape, kind)


LANES = 128


def project(
    tokens,
    norm_gain,
    query_weight,
    key_weight,
    value_weight,
    gate_weight,
    forget_bias,
    state_normalizer,
    state_max,
    block_keys,
    block_values,
    block_input,
    block_logf,
):
    _, heads, dk = state_normalizer.shape
    span, dv = block_values.shape[2:]
    packed_width = dk + 2 * LANES
    rows, columns = tokens.shape
    size = lax.axis_size("kv")
    weights = (query_weight, key_weight, value_weight)
    widths = [w.shape[1] for w in weights]
    starts = [sum(widths[:i]) for i in range(3)]
    width = sum(widths)
    gate_count = gate_weight.shape[1] * gate_weight.shape[2]
    gates = jnp.transpose(gate_weight, (1, 2, 0)).reshape(gate_count, -1)
    cuts = [0, columns]
    small = (forget_bias.reshape(1, -1), state_normalizer, state_max, block_input, block_logf)

    def body(tokens_hbm, gain_hbm, q_hbm, k_hbm, v_hbm, gate_hbm, *rest):
        small_hbm, (keys_hbm, values_hbm), rest = rest[:5], rest[5:7], rest[7:]
        outs, small_out, block_out = rest[:size], rest[size], rest[size + 1]
        rest = rest[size + 2 :]
        tokens_ref, gain_ref, weight_ref, gate_ref, sums_ref = rest[:5]
        sems, gate_sem, tokens_sem, gain_sem, small_sems, block_sems = rest[5:11]
        small_refs = rest[11:]
        position = lax.axis_index("kv")
        tokens_copy = pltpu.make_async_copy(tokens_hbm, tokens_ref, tokens_sem)
        gain_copy = pltpu.make_async_copy(gain_hbm, gain_ref, gain_sem)
        tokens_copy.start()
        gain_copy.start()
        copies = []
        for c in range(len(cuts) - 1):
            at = pl.ds(cuts[c], cuts[c + 1] - cuts[c])
            for w, source in enumerate((q_hbm, k_hbm, v_hbm)):
                copy = pltpu.make_async_copy(
                    source.at[at, :],
                    weight_ref.at[at, pl.ds(starts[w], widths[w])],
                    sems.at[c, w],
                )
                copy.start()
                copies.append(copy)
        gate_copy = pltpu.make_async_copy(
            gate_hbm.at[:, pl.ds(pl.multiple_of(position * columns, columns), columns)],
            gate_ref,
            gate_sem,
        )
        gate_copy.start()
        small_copies = [
            pltpu.make_async_copy(source, target, small_sems.at[i])
            for i, (source, target) in enumerate(zip(small_hbm, small_refs))
        ]
        block_copies = [
            pltpu.make_async_copy(keys_hbm.at[0], block_out.at[:, :, pl.ds(0, dk)], block_sems.at[0]),
            pltpu.make_async_copy(
                values_hbm.at[0], block_out.at[:, :, pl.ds(dk, dv)], block_sems.at[1]
            ),
        ]
        for copy in small_copies + block_copies:
            copy.start()
        tokens_copy.wait()
        gain_copy.wait()
        widened = tokens_ref[...].astype(jnp.float32)
        squares = jnp.sum(widened * widened, axis=1, keepdims=True)
        normed = (widened * gain_ref[...]).astype(jnp.bfloat16)
        for copy in small_copies:
            copy.wait()
        bias_ref, normalizer_ref, max_ref, input_ref, logf_ref = small_refs
        lane_h = lax.broadcasted_iota(jnp.int32, (heads, heads), 1)
        head_h = lax.broadcasted_iota(jnp.int32, (heads, heads), 0)

        def column(ref):
            values = jnp.broadcast_to(ref[...], (heads, heads))
            return jnp.sum(jnp.where(lane_h == head_h, values, 0.0), axis=1, keepdims=True)

        lane = lax.broadcasted_iota(jnp.int32, (heads, LANES), 1)
        small_out[:, :dk] = normalizer_ref[0]
        small_out[:, dk : dk + LANES] = jnp.concatenate([input_ref[0], logf_ref[0]], axis=1)
        small_out[:, dk + LANES :] = jnp.where(lane == 0, column(max_ref), column(bias_ref))
        for c in range(len(cuts) - 1):
            piece = normed[:, cuts[c] : cuts[c + 1]]
            for w in range(3):
                copies[3 * c + w].wait()
                at = slice(starts[w], starts[w] + widths[w])
                product = jnp.dot(
                    piece,
                    weight_ref[cuts[c] : cuts[c + 1], at],
                    preferred_element_type=jnp.float32,
                )
                if c:
                    product = product + sums_ref[:, at]
                sums_ref[:, at] = product
        for copy in block_copies:
            copy.wait()
        gate_copy.wait()
        gate_sums = dot_nt(normed, gate_ref[...])
        pad = jnp.zeros((rows, LANES - gate_count), jnp.float32)
        extra = jnp.concatenate([gate_sums, pad], axis=1)
        lane = lax.broadcasted_iota(jnp.int32, (rows, LANES), 1)
        sums_ref[:, width:] = jnp.where(lane == gate_count, squares, extra)
        for d in range(size):
            outs[d][...] = sums_ref[pl.ds(partner_of(position, size, d, False), 1), :]

    return call(
        body,
        [struct((1, width + LANES), jnp.float32)] * size
        + [
            struct((heads, packed_width), jnp.float32),
            struct((heads, span, dk + dv), block_keys.dtype),
        ],
        [ANY_SPEC] * 13,
        [
            streamed(a)
            for a in (
                tokens,
                norm_gain.reshape(1, -1),
                *weights,
                gates,
                *small,
                block_keys,
                block_values,
            )
        ],
        [
            pltpu.VMEM(tokens.shape, tokens.dtype),
            pltpu.VMEM((1, columns), norm_gain.dtype),
            pltpu.VMEM((columns, width), query_weight.dtype),
            pltpu.VMEM((gate_count, columns), gates.dtype),
            pltpu.VMEM((rows, width + LANES), jnp.float32),
            pltpu.SemaphoreType.DMA((len(cuts) - 1, 3)),
            pltpu.SemaphoreType.DMA(()),
            pltpu.SemaphoreType.DMA(()),
            pltpu.SemaphoreType.DMA(()),
            pltpu.SemaphoreType.DMA((len(small),)),
            pltpu.SemaphoreType.DMA((2,)),
            *[pltpu.VMEM(a.shape, a.dtype) for a in small],
        ],
        limit=16,
    )


def recall(parts, small, state_matrix, blocks, lengths):
    _, heads, dv, dk = state_matrix.shape
    all_heads = heads * lax.axis_size("tp")
    scale = dk ** (-0.5)
    count = len(parts)

    def body(*refs):
        small_ref, state_ref, blocks_ref, lengths_ref, out_ref = refs[count:]
        half = 1 - lax.axis_index("tp")
        row = refs[0][...]
        for r in refs[1:count]:
            row = row + r[...]
        q_end, k_end = heads * dk, 2 * heads * dk
        v_end = k_end + heads * dv
        extra = row[:, v_end:]
        squares = extra[:, 2 * all_heads : 2 * all_heads + 1]
        row_scale = lax.rsqrt(squares / D + epsilon)
        row = row[:, :v_end] * row_scale

        def by_head(start, size):
            return jnp.concatenate(
                [row[:, start + h * size : start + (h + 1) * size] for h in range(heads)], axis=0
            ).astype(jnp.bfloat16)

        query, key, value = by_head(0, dk), by_head(q_end, dk), by_head(k_end, dv)
        gates = jnp.broadcast_to(extra * row_scale, (heads, LANES))
        lane = lax.broadcasted_iota(jnp.int32, (heads, LANES), 1)
        head = lax.broadcasted_iota(jnp.int32, (heads, LANES), 0)

        def column(values, first):
            return jnp.sum(jnp.where(lane == head + first, values, 0.0), axis=1, keepdims=True)

        small = small_ref[...]
        block_input = small[:, dk : dk + SPAN_LOCATIONS]
        block_logf = small[:, dk + SPAN_LOCATIONS : dk + 2 * SPAN_LOCATIONS]
        state_max = small[:, dk + LANES : dk + LANES + 1]
        bias = small[:, dk + LANES + 1 : dk + LANES + 2]
        span = (heads, SPAN_LOCATIONS)
        live = jnp.broadcast_to(lengths_ref[:, :1] & (SPAN_LOCATIONS - 1), span)
        inside = lax.broadcasted_iota(jnp.int32, span, 1) < live
        rest = jnp.where(inside, block_logf, 0.0)
        square = (SPAN_LOCATIONS, SPAN_LOCATIONS)
        upto = (
            lax.broadcasted_iota(jnp.int32, square, 0) <= lax.broadcasted_iota(jnp.int32, square, 1)
        ).astype(jnp.float32).astype(jnp.bfloat16)
        cumulative = jnp.zeros(span, jnp.float32)
        for _ in range(3):
            term = rest.astype(jnp.bfloat16)
            rest = rest - term.astype(jnp.float32)
            cumulative = cumulative + jnp.dot(term, upto, preferred_element_type=jnp.float32)
        logf_sum = cumulative[:, SPAN_LOCATIONS - 1 :]
        cache_base = jnp.where(inside, logf_sum - cumulative + block_input, -jnp.inf)
        new_input = column(gates, half * heads)
        new_logf = jax.nn.log_sigmoid(column(gates, all_heads + half * heads) + bias)
        carried_log = logf_sum + new_logf + state_max
        cache_log = cache_base + new_logf
        stable = jnp.maximum(
            jnp.maximum(carried_log, jnp.max(cache_log, axis=1, keepdims=True)), new_input
        )
        carried_weight = jnp.exp(carried_log - stable)
        new_weight = jnp.exp(new_input - stable)
        cache_weight = jnp.exp(cache_log - stable)

        def pick(make, size):
            rows = lax.broadcasted_iota(jnp.int32, (heads, size), 0)
            out = jnp.zeros((heads, size), jnp.float32)
            for h in range(heads):
                out = jnp.where(rows == h, make(h), out)
            return out

        scores = pick(lambda h: dot_nt(query, blocks_ref[h, :, :dk]), SPAN_LOCATIONS)
        mixing = (scores * scale * cache_weight).astype(jnp.bfloat16)
        query_wide = query.astype(jnp.float32)
        own_term = (
            jnp.sum(query_wide * key.astype(jnp.float32), axis=1, keepdims=True)
            * scale
            * new_weight
        )

        def carry(h):
            state = state_ref[0, h]
            high = state.astype(jnp.bfloat16)
            low = (state - high.astype(jnp.float32)).astype(jnp.bfloat16)
            return dot_nt(query, high) + dot_nt(query, low)

        carried = pick(carry, dv)
        from_cache = pick(
            lambda h: jnp.dot(
                mixing, blocks_ref[h, :, dk:], preferred_element_type=jnp.float32
            ), dv
        )
        numerator = carried_weight * carried + from_cache + own_term * value.astype(jnp.float32)
        normalizer = (
            carried_weight * jnp.sum(small[:, :dk] * query_wide, axis=1, keepdims=True)
            + jnp.sum(mixing.astype(jnp.float32), axis=1, keepdims=True)
            + own_term
        )
        divisor = jnp.maximum(jnp.maximum(jnp.abs(normalizer), jnp.exp(-stable)), 1.0)
        out_ref[...] = (numerator / divisor).astype(jnp.bfloat16)

    return call(
        body,
        [struct((heads, dv), jnp.bfloat16)],
        [VMEM_SPEC] * (count + 4),
        (
            *parts,
            small,
            resident(state_matrix),
            blocks,
            jnp.pad(lengths, (0, LANES - 1)).reshape(1, -1),
        ),
    )[0]


def attend(pieces, out_weight):
    size = len(pieces)
    heads, dv = pieces[0].shape

    def body(*refs):
        weight_ref, out_ref, hidden_ref = refs[size:]
        position = lax.axis_index("kv")
        for n, d in enumerate([*distances(size), 0]):
            piece = refs[n][...].astype(jnp.float32)
            at = pl.ds(partner_of(position, size, d, True), 1)
            for h in range(heads):
                hidden_ref[at, h * dv : (h + 1) * dv] = piece[h : h + 1]
        out_ref[...] = jnp.dot(
            hidden_ref[...].astype(jnp.bfloat16),
            weight_ref[...],
            preferred_element_type=jnp.float32,
        ).astype(jnp.bfloat16)

    return call(
        body,
        [struct((size, out_weight.shape[1]), jnp.bfloat16)],
        [VMEM_SPEC] * (size + 1),
        (*pieces, resident(out_weight)),
        [pltpu.VMEM((size, heads * dv), jnp.float32)],
    )[0]


def add_features(refs, partners, gain_ref, up_ref, product, squares):
    size = lax.axis_size("kv")
    for ref, d in zip(refs, partners):
        columns = ref.shape[1]
        j = partner_of(lax.axis_index("kv"), size, d, True)
        at = pl.ds(pl.multiple_of(j * columns, columns), columns)
        wide = ref[...].astype(jnp.float32)
        squares = squares + jnp.sum(wide * wide, axis=1, keepdims=True)
        mixer_in = (wide * gain_ref[:, at]).astype(jnp.bfloat16)
        product = product + dot_nt(mixer_in, up_ref[:, at])
    return product, squares


def absorb(pieces, partners, mixer_gain, up_weight):
    rows = pieces[0].shape[0]
    units = up_weight.shape[0]
    count = len(pieces)

    def body(*refs):
        gain_ref, up_ref, product_ref, squares_ref = refs[count:]
        product, squares = add_features(
            refs[:count],
            partners,
            gain_ref,
            up_ref,
            jnp.zeros((rows, units), jnp.float32),
            jnp.zeros((rows, 1), jnp.float32),
        )
        product_ref[...] = product
        squares_ref[...] = jnp.broadcast_to(squares, (rows, LANES))

    return call(
        body,
        [struct((rows, units), jnp.float32), struct((rows, LANES), jnp.float32)],
        [VMEM_SPEC] * (count + 2),
        (*pieces, mixer_gain, up_weight),
        flops=20000000000,
    )


def mix(pieces, partners, before, residual, mixer_gain, up_weight, down_weight):
    size = lax.axis_size("kv")
    count = len(pieces)
    rows, columns = residual.shape
    blocks = [*distances(size), 0]
    share = columns // 2

    def body(*refs):
        product_ref, squares_ref, residual_ref, gain_ref, up_ref, down_ref, *outs = refs[count:]
        position = lax.axis_index("kv")
        product, squares = add_features(
            refs[:count], partners, gain_ref, up_ref, product_ref[...], squares_ref[:, :1]
        )
        scaled = product * lax.rsqrt(squares / D + epsilon)
        activated = jnp.square(jnp.maximum(scaled, 0.0)).astype(jnp.bfloat16)
        for n, d in enumerate(blocks):
            j = partner_of(position, size, d, False)
            at = pl.ds(pl.multiple_of(j * columns, columns), columns)
            terms = jnp.dot(activated, down_ref[:, at], preferred_element_type=jnp.float32)
            if d == 0:
                half = lax.broadcasted_iota(jnp.int32, (rows, columns), 1) // share
                kept = residual_ref[...].astype(jnp.float32)
                terms = terms + jnp.where(half == lax.axis_index("tp"), kept, 0.0)
            outs[n][...] = terms

    return call(
        body,
        [struct((rows, columns), jnp.float32)] * len(blocks),
        [VMEM_SPEC] * (count + 6),
        (*pieces, *before, residual, mixer_gain, up_weight, down_weight),
        flops=20000000000,
    )


def exchange_pairs(size, cores, distance):
    return [
        (i * cores + t, j * cores + (cores - 1 - t))
        for i, j in partner_pairs(size, distance)
        for t in range(cores)
    ]


def distances(size):
    return [*range(size // 2, size), *range(1, size // 2)]


def to_partners(outgoing, partners):
    size, cores = lax.axis_size("kv"), lax.axis_size("tp")
    received = []
    for d in partners:
        pairs = exchange_pairs(size, cores, d)
        received.append(lax.ppermute(outgoing[d], ("kv", "tp"), pairs))
    return received


def swapped(array):
    return lax.ppermute(array, "tp", [(0, 1), (1, 0)])


def direct(mesh, arrays_shape):
    size, cores = mesh["kv"], mesh["tp"]
    sequences, features = arrays_shape
    groups = mesh["dp"] * size
    return (
        2 < size <= DIRECT_LIMIT
        and cores == 2
        and sequences == groups
        and features % (size * 2 * LANES) == 0
    )


def shards_direct(
    tokens,
    norm_gain,
    query_weight,
    key_weight,
    value_weight,
    gate_weight,
    forget_bias,
    state_matrix,
    state_normalizer,
    state_max,
    block_keys,
    block_values,
    block_input,
    block_logf,
    lengths,
    out_weight,
    mixer_gain,
    up_weight,
    down_weight,
):
    head_half = lax.axis_index("tp")
    size = lax.axis_size("kv")
    order = distances(size)
    state_matrix = swapped(state_matrix)
    *parts, small, blocks = project(
        tokens,
        norm_gain,
        query_weight,
        key_weight,
        value_weight,
        gate_weight,
        forget_bias,
        state_normalizer,
        state_max,
        block_keys,
        block_values,
        block_input,
        block_logf,
    )
    parts = to_partners(parts, [*order, 0])
    hidden = recall(parts, swapped(small), state_matrix, swapped(blocks), lengths)
    pieces = to_partners([hidden] * size, [*order, 0])
    partial_out = attend(pieces, out_weight)
    other_out = swapped(partial_out)
    attended = partial_out.astype(jnp.float32) + other_out.astype(jnp.float32)
    residual = (tokens.astype(jnp.float32) + attended).astype(jnp.bfloat16)
    gain = mixer_gain.reshape(1, -1)
    pieces = to_partners([residual] * size, order)
    order = distances(size)
    up_weight, down_weight = resident(up_weight), resident(down_weight)
    absorbed = absorb([residual, pieces[0]], [0, order[0]], gain, up_weight)
    *terms, own = mix(
        pieces[1:], order[1:], absorbed, residual, gain, up_weight, down_weight
    )
    outgoing = dict(zip(order, terms))
    total = own
    for term in to_partners(outgoing, order):
        total = total + term
    share = tokens.shape[1] // 2
    other = lax.dynamic_slice_in_dim(total, (1 - head_half) * share, share, 1)
    kept = lax.dynamic_slice_in_dim(total, head_half * share, share, 1)
    return (kept + swapped(other)).astype(jnp.bfloat16)


def mapped(mesh, function):
    return jax.shard_map(
        function,
        mesh=mesh,
        in_specs=(
            P("dp", "kv"),
            P("kv"),
            P("kv", "tp"),
            P("kv", "tp"),
            P("kv", "tp"),
            P(),
            P("tp"),
            P(("dp", "kv"), "tp", None, None),
            P(("dp", "kv"), "tp", None),
            P(("dp", "kv"), "tp"),
            P(("dp", "kv"), "tp", None, None),
            P(("dp", "kv"), "tp", None, None),
            P(("dp", "kv"), "tp", None),
            P(("dp", "kv"), "tp", None),
            P(("dp", "kv")),
            P("tp", "kv"),
            P(),
            P(("kv", "tp"), None),
            P(("kv", "tp"), None),
        ),
        out_specs=P("dp", ("kv", "tp")),
        check_vma=False,
    )


def solution(mesh):
    sizes = dict(mesh.shape)

    def whole(*arrays):
        return mapped(mesh, shards_general)(*arrays)

    def small(*arrays):
        if not direct(sizes, arrays[0].shape):
            return whole(*arrays)
        return mapped(mesh, shards_direct)(*arrays)

    if not 2 < sizes["kv"] <= DIRECT_LIMIT:
        return whole
    return small
```

```python
import jax
import jax.numpy as jnp
from jax import lax
from jax.experimental import pallas as pl
from jax.experimental.pallas import tpu as pltpu
from jax.sharding import PartitionSpec as P

D = 4096
DK = 256
DV = 512
SPAN_LOCATIONS = 64


epsilon = 1e-06
highest = lax.Precision.HIGHEST


def memory_cell(
    query,
    key,
    value,
    gates,
    forget_bias,
    state_matrix,
    state_normalizer,
    state_max,
    block_keys,
    block_values,
    block_input,
    block_logf,
    lengths,
):
    live = lengths % SPAN_LOCATIONS
    positions = lax.broadcasted_iota(jnp.int32, (1, 1, SPAN_LOCATIONS), 2)
    inside = positions < live[:, None, None]
    new_input = gates[:, 0]
    new_logf = jax.nn.log_sigmoid(gates[:, 1] + forget_bias)
    cumulative = jnp.cumsum(jnp.where(inside, block_logf, jnp.float32(0.0)), axis=2)
    total = cumulative[:, :, -1] + new_logf
    carried_log = total + state_max
    cache_log = jnp.where(inside, total[:, :, None] - cumulative + block_input, -jnp.inf)
    stable = jnp.maximum(jnp.maximum(carried_log, jnp.max(cache_log, axis=2)), new_input)
    carried_weight = jnp.exp(carried_log - stable)
    new_weight = jnp.exp(new_input - stable)
    cache_weight = jnp.exp(cache_log - stable[:, :, None])
    scores = jnp.einsum("bhk,bhsk->bhs", query, block_keys, preferred_element_type=jnp.float32)
    mixing = (scores * DK ** (-0.5) * cache_weight).astype(jnp.bfloat16)
    query_wide = query.astype(jnp.float32)
    own_term = jnp.sum(query_wide * key.astype(jnp.float32), axis=2) * DK ** (-0.5) * new_weight
    carried = jnp.einsum("bhvk,bhk->bhv", state_matrix, query_wide, precision=highest)
    from_cache = jnp.einsum(
        "bhs,bhsv->bhv", mixing, block_values, preferred_element_type=jnp.float32
    )
    numerator = (
        carried_weight[:, :, None] * carried
        + from_cache
        + own_term[:, :, None] * value.astype(jnp.float32)
    )
    normalizer = (
        carried_weight * jnp.sum(state_normalizer * query_wide, axis=2)
        + jnp.sum(mixing.astype(jnp.float32), axis=2)
        + own_term
    )
    divisor = jnp.maximum(jnp.maximum(jnp.abs(normalizer), jnp.exp(-stable)), jnp.float32(1.0))
    hidden = numerator / divisor[:, :, None]
    return hidden.astype(jnp.bfloat16)


def absorb_columns(mixer_gain, up_weight):

    def absorb(carry, piece, start):
        widened = piece.astype(jnp.float32)
        mixer_in = (widened * mixer_gain).astype(jnp.bfloat16)
        product = lax.dot_general(
            mixer_in, up_weight, (((1,), (1,)), ((), ())), preferred_element_type=jnp.float32
        )
        return (product, jnp.sum(widened * widened, axis=1))

    return absorb


def down_terms(carry, down_weight):
    accumulated, squares = carry
    scaled = accumulated * lax.rsqrt(squares / D + epsilon)[:, None]
    activated = jnp.square(jax.nn.relu(scaled)).astype(jnp.bfloat16)
    return jnp.dot(activated, down_weight, preferred_element_type=jnp.float32)


DIRECT_LIMIT = 8


def partner_pairs(size, distance):
    if size & (size - 1) == 0:
        return [(i, i ^ distance) for i in range(size)]
    return [(i, (i + distance) % size) for i in range(size)]


def partner_of(position, size, distance, receiving):
    if size & (size - 1) == 0:
        return position ^ distance
    return (position - distance) % size if receiving else (position + distance) % size


def gather_direct(piece, axis):
    size = lax.axis_size(axis)
    if size > DIRECT_LIMIT:
        return lax.all_gather(piece, axis, axis=0)
    position = lax.axis_index(axis)
    received = [piece] + [
        lax.ppermute(piece, axis, partner_pairs(size, d)) for d in range(1, size)
    ]
    stacked = jnp.stack(received)
    places = jnp.arange(size)
    if size & (size - 1) == 0:
        order = position ^ places
    else:
        order = (position - places) % size
    return stacked[order]


def scatter_sum_direct(parts, axis):
    size = lax.axis_size(axis)
    if size > DIRECT_LIMIT:
        return lax.psum_scatter(parts, axis, scatter_dimension=0, tiled=False)
    position = lax.axis_index(axis)

    def entry(index):
        return lax.dynamic_index_in_dim(parts, index, 0, keepdims=False)

    total = entry(position)
    for d in range(1, size):
        out = entry(partner_of(position, size, d, False))
        total = total + lax.ppermute(out, axis, partner_pairs(size, d))
    return total


def shards_general(
    tokens,
    norm_gain,
    query_weight,
    key_weight,
    value_weight,
    gate_weight,
    forget_bias,
    state_matrix,
    state_normalizer,
    state_max,
    block_keys,
    block_values,
    block_input,
    block_logf,
    lengths,
    out_weight,
    mixer_gain,
    up_weight,
    down_weight,
):
    position = lax.axis_index("kv")
    head_half = lax.axis_index("tp")
    columns = tokens.shape[1]
    local_heads = forget_bias.shape[0]
    local_rows = lengths.shape[0]
    widened = tokens.astype(jnp.float32)
    squares = jnp.sum(widened * widened, axis=1)
    normed = (widened * norm_gain).astype(jnp.bfloat16)
    gate_rows = lax.dynamic_slice_in_dim(gate_weight, position * columns, columns, 0)
    gate_rows = lax.dynamic_slice_in_dim(
        gate_rows, head_half * local_heads, local_heads, 2
    ).reshape(columns, 2 * local_heads)
    query_part = jnp.dot(normed, query_weight, preferred_element_type=jnp.float32)
    key_part = jnp.dot(normed, key_weight, preferred_element_type=jnp.float32)
    value_part = jnp.dot(normed, value_weight, preferred_element_type=jnp.float32)
    gate_part = jnp.dot(normed, gate_rows, preferred_element_type=jnp.float32)
    parts = jnp.concatenate(
        [query_part, key_part, value_part, gate_part, squares[:, None]], axis=1
    )
    parts = parts.reshape(-1, local_rows, parts.shape[1])
    sums = scatter_sum_direct(parts, "kv")
    q_end = query_part.shape[1]
    k_end = q_end + key_part.shape[1]
    v_end = k_end + value_part.shape[1]
    g_end = v_end + gate_part.shape[1]
    query_sum, key_sum, value_sum, gate_sum, own_squares = (
        sums[:, :q_end],
        sums[:, q_end:k_end],
        sums[:, k_end:v_end],
        sums[:, v_end:g_end],
        sums[:, g_end],
    )
    row_scale = lax.rsqrt(own_squares / D + epsilon)[:, None]
    query = (query_sum * row_scale).astype(jnp.bfloat16).reshape(local_rows, local_heads, DK)
    key = (key_sum * row_scale).astype(jnp.bfloat16).reshape(local_rows, local_heads, DK)
    value = (value_sum * row_scale).astype(jnp.bfloat16).reshape(local_rows, local_heads, DV)
    gates = (gate_sum * row_scale).reshape(local_rows, 2, local_heads)
    hidden = memory_cell(
        query,
        key,
        value,
        gates,
        forget_bias,
        state_matrix,
        state_normalizer,
        state_max,
        block_keys,
        block_values,
        block_input,
        block_logf,
        lengths,
    )
    hidden = hidden.reshape(local_rows, local_heads * DV)
    every_hidden = gather_direct(hidden, "kv").reshape(-1, hidden.shape[1])
    partial_out = jnp.dot(
        every_hidden, out_weight, preferred_element_type=jnp.float32
    ).astype(jnp.bfloat16)
    attended = jnp.sum(gather_direct(partial_out, "tp").astype(jnp.float32), axis=0)
    residual = (widened + attended).astype(jnp.bfloat16)
    absorb = absorb_columns(mixer_gain, up_weight)
    hidden_units = up_weight.shape[0]
    rows = residual.shape[0]
    initial = (jnp.zeros((rows, hidden_units), jnp.float32), jnp.zeros((rows,), jnp.float32))
    pieces = gather_direct(residual, "kv")
    whole = jnp.moveaxis(pieces, 0, 1).reshape(rows, -1)
    carry = absorb(initial, whole, jnp.int32(0))
    terms = down_terms(carry, down_weight)
    share = columns // lax.axis_size("tp")
    terms = terms.reshape(rows, -1, lax.axis_size("tp"), share)
    by_core = scatter_sum_direct(jnp.moveaxis(terms, 2, 0), "tp")
    mixed_terms = scatter_sum_direct(jnp.moveaxis(by_core, 1, 0), "kv")
    own_residual = lax.dynamic_slice_in_dim(residual, head_half * share, share, 1)
    return (own_residual.astype(jnp.float32) + mixed_terms).astype(jnp.bfloat16)


def dot_nt(left, right):
    return lax.dot_general(
        left, right, (((1,), (1,)), ((), ())), preferred_element_type=jnp.float32
    )


VMEM_SPEC = pl.BlockSpec(memory_space=pltpu.VMEM)
SMEM_SPEC = pl.BlockSpec(memory_space=pltpu.SMEM)
ANY_SPEC = pl.BlockSpec(memory_space=pl.ANY)


def call(body, outs, in_specs, args, scratch=(), limit=8, flops=20000000000, aliases=None):
    return pl.pallas_call(
        body,
        out_shape=outs,
        in_specs=in_specs,
        out_specs=[VMEM_SPEC] * len(outs),
        scratch_shapes=list(scratch),
        input_output_aliases=aliases or {},
        compiler_params=pltpu.CompilerParams(vmem_limit_bytes=limit << 20),
        cost_estimate=pl.CostEstimate(flops=flops, bytes_accessed=1000000, transcendentals=0),
    )(*args)


def resident(weight):
    return pltpu.with_memory_space_constraint(weight, pltpu.VMEM)


def streamed(weight):
    return pltpu.with_memory_space_constraint(weight, pltpu.HBM)


def struct(shape, kind):
    return jax.ShapeDtypeStruct(shape, kind)


LANES = 128


def project(
    tokens,
    norm_gain,
    query_weight,
    key_weight,
    value_weight,
    gate_weight,
    forget_bias,
    state_normalizer,
    state_max,
    block_keys,
    block_values,
    block_input,
    block_logf,
):
    _, heads, dk = state_normalizer.shape
    span, dv = block_values.shape[2:]
    packed_width = dk + 2 * LANES
    rows, columns = tokens.shape
    size = lax.axis_size("kv")
    weights = (query_weight, key_weight, value_weight)
    widths = [w.shape[1] for w in weights]
    starts = [sum(widths[:i]) for i in range(3)]
    width = sum(widths)
    gate_count = gate_weight.shape[1] * gate_weight.shape[2]
    gates = jnp.transpose(gate_weight, (1, 2, 0)).reshape(gate_count, -1)
    cuts = [0, columns]
    small = (forget_bias.reshape(1, -1), state_normalizer, state_max, block_input, block_logf)

    def body(tokens_hbm, gain_hbm, q_hbm, k_hbm, v_hbm, gate_hbm, *rest):
        small_hbm, (keys_hbm, values_hbm), rest = rest[:5], rest[5:7], rest[7:]
        outs, small_out, block_out = rest[:size], rest[size], rest[size + 1]
        rest = rest[size + 2 :]
        tokens_ref, gain_ref, weight_ref, gate_ref, sums_ref = rest[:5]
        sems, gate_sem, tokens_sem, gain_sem, small_sems, block_sems = rest[5:11]
        small_refs = rest[11:]
        position = lax.axis_index("kv")
        tokens_copy = pltpu.make_async_copy(tokens_hbm, tokens_ref, tokens_sem)
        gain_copy = pltpu.make_async_copy(gain_hbm, gain_ref, gain_sem)
        tokens_copy.start()
        gain_copy.start()
        copies = []
        for c in range(len(cuts) - 1):
            at = pl.ds(cuts[c], cuts[c + 1] - cuts[c])
            for w, source in enumerate((q_hbm, k_hbm, v_hbm)):
                copy = pltpu.make_async_copy(
                    source.at[at, :],
                    weight_ref.at[at, pl.ds(starts[w], widths[w])],
                    sems.at[c, w],
                )
                copy.start()
                copies.append(copy)
        gate_copy = pltpu.make_async_copy(
            gate_hbm.at[:, pl.ds(pl.multiple_of(position * columns, columns), columns)],
            gate_ref,
            gate_sem,
        )
        gate_copy.start()
        small_copies = [
            pltpu.make_async_copy(source, target, small_sems.at[i])
            for i, (source, target) in enumerate(zip(small_hbm, small_refs))
        ]
        block_copies = [
            pltpu.make_async_copy(keys_hbm.at[0], block_out.at[:, :, pl.ds(0, dk)], block_sems.at[0]),
            pltpu.make_async_copy(
                values_hbm.at[0], block_out.at[:, :, pl.ds(dk, dv)], block_sems.at[1]
            ),
        ]
        for copy in small_copies + block_copies:
            copy.start()
        tokens_copy.wait()
        gain_copy.wait()
        widened = tokens_ref[...].astype(jnp.float32)
        squares = jnp.sum(widened * widened, axis=1, keepdims=True)
        normed = (widened * gain_ref[...]).astype(jnp.bfloat16)
        for c in range(len(cuts) - 1):
            piece = normed[:, cuts[c] : cuts[c + 1]]
            for w in range(3):
                copies[3 * c + w].wait()
                at = slice(starts[w], starts[w] + widths[w])
                product = jnp.dot(
                    piece,
                    weight_ref[cuts[c] : cuts[c + 1], at],
                    preferred_element_type=jnp.float32,
                )
                if c:
                    product = product + sums_ref[:, at]
                sums_ref[:, at] = product
        for copy in block_copies:
            copy.wait()
        gate_copy.wait()
        gate_sums = dot_nt(normed, gate_ref[...])
        pad = jnp.zeros((rows, LANES - gate_count), jnp.float32)
        extra = jnp.concatenate([gate_sums, pad], axis=1)
        lane = lax.broadcasted_iota(jnp.int32, (rows, LANES), 1)
        sums_ref[:, width:] = jnp.where(lane == gate_count, squares, extra)
        for copy in small_copies:
            copy.wait()
        bias_ref, normalizer_ref, max_ref, input_ref, logf_ref = small_refs
        lane_h = lax.broadcasted_iota(jnp.int32, (heads, heads), 1)
        head_h = lax.broadcasted_iota(jnp.int32, (heads, heads), 0)

        def column(ref):
            values = jnp.broadcast_to(ref[...], (heads, heads))
            return jnp.sum(jnp.where(lane_h == head_h, values, 0.0), axis=1, keepdims=True)

        lane_s = lax.broadcasted_iota(jnp.int32, (heads, LANES), 1)
        small_out[:, :dk] = normalizer_ref[0]
        small_out[:, dk : dk + LANES] = jnp.concatenate([input_ref[0], logf_ref[0]], axis=1)
        small_out[:, dk + LANES :] = jnp.where(lane_s == 0, column(max_ref), column(bias_ref))
        for d in range(size):
            outs[d][...] = sums_ref[pl.ds(partner_of(position, size, d, False), 1), :]

    return call(
        body,
        [struct((1, width + LANES), jnp.float32)] * size
        + [
            struct((heads, packed_width), jnp.float32),
            struct((heads, span, dk + dv), block_keys.dtype),
        ],
        [ANY_SPEC] * 13,
        [
            streamed(a)
            for a in (
                tokens,
                norm_gain.reshape(1, -1),
                *weights,
                gates,
                *small,
                block_keys,
                block_values,
            )
        ],
        [
            pltpu.VMEM(tokens.shape, tokens.dtype),
            pltpu.VMEM((1, columns), norm_gain.dtype),
            pltpu.VMEM((columns, width), query_weight.dtype),
            pltpu.VMEM((gate_count, columns), gates.dtype),
            pltpu.VMEM((rows, width + LANES), jnp.float32),
            pltpu.SemaphoreType.DMA((len(cuts) - 1, 3)),
            pltpu.SemaphoreType.DMA(()),
            pltpu.SemaphoreType.DMA(()),
            pltpu.SemaphoreType.DMA(()),
            pltpu.SemaphoreType.DMA((len(small),)),
            pltpu.SemaphoreType.DMA((2,)),
            *[pltpu.VMEM(a.shape, a.dtype) for a in small],
        ],
        limit=16,
    )


def recall(parts, small, state_matrix, blocks, lengths):
    _, heads, dv, dk = state_matrix.shape
    all_heads = heads * lax.axis_size("tp")
    scale = dk ** (-0.5)
    count = len(parts)

    def body(*refs):
        small_ref, state_ref, blocks_ref, lengths_ref, out_ref = refs[count:]
        half = 1 - lax.axis_index("tp")
        row = refs[0][...]
        for r in refs[1:count]:
            row = row + r[...]
        q_end, k_end = heads * dk, 2 * heads * dk
        v_end = k_end + heads * dv
        extra = row[:, v_end:]
        squares = extra[:, 2 * all_heads : 2 * all_heads + 1]
        row_scale = lax.rsqrt(squares / D + epsilon)
        row = row[:, :v_end] * row_scale

        def by_head(start, size):
            return jnp.concatenate(
                [row[:, start + h * size : start + (h + 1) * size] for h in range(heads)], axis=0
            ).astype(jnp.bfloat16)

        query, key, value = by_head(0, dk), by_head(q_end, dk), by_head(k_end, dv)
        gates = jnp.broadcast_to(extra * row_scale, (heads, LANES))
        lane = lax.broadcasted_iota(jnp.int32, (heads, LANES), 1)
        head = lax.broadcasted_iota(jnp.int32, (heads, LANES), 0)

        def column(values, first):
            return jnp.sum(jnp.where(lane == head + first, values, 0.0), axis=1, keepdims=True)

        small = small_ref[...]
        block_input = small[:, dk : dk + SPAN_LOCATIONS]
        block_logf = small[:, dk + SPAN_LOCATIONS : dk + 2 * SPAN_LOCATIONS]
        state_max = small[:, dk + LANES : dk + LANES + 1]
        bias = small[:, dk + LANES + 1 : dk + LANES + 2]
        span = (heads, SPAN_LOCATIONS)
        live = jnp.broadcast_to(lengths_ref[:, :1] & (SPAN_LOCATIONS - 1), span)
        inside = lax.broadcasted_iota(jnp.int32, span, 1) < live
        rest = jnp.where(inside, block_logf, 0.0)
        square = (SPAN_LOCATIONS, SPAN_LOCATIONS)
        upto = (
            lax.broadcasted_iota(jnp.int32, square, 0) <= lax.broadcasted_iota(jnp.int32, square, 1)
        ).astype(jnp.float32).astype(jnp.bfloat16)
        cumulative = jnp.zeros(span, jnp.float32)
        for _ in range(3):
            term = rest.astype(jnp.bfloat16)
            rest = rest - term.astype(jnp.float32)
            cumulative = cumulative + jnp.dot(term, upto, preferred_element_type=jnp.float32)
        logf_sum = cumulative[:, SPAN_LOCATIONS - 1 :]
        cache_base = jnp.where(inside, logf_sum - cumulative + block_input, -jnp.inf)
        new_input = column(gates, half * heads)
        new_logf = jax.nn.log_sigmoid(column(gates, all_heads + half * heads) + bias)
        carried_log = logf_sum + new_logf + state_max
        cache_log = cache_base + new_logf
        stable = jnp.maximum(
            jnp.maximum(carried_log, jnp.max(cache_log, axis=1, keepdims=True)), new_input
        )
        carried_weight = jnp.exp(carried_log - stable)
        new_weight = jnp.exp(new_input - stable)
        cache_weight = jnp.exp(cache_log - stable)

        def pick(make, size):
            rows = lax.broadcasted_iota(jnp.int32, (heads, size), 0)
            out = jnp.zeros((heads, size), jnp.float32)
            for h in range(heads):
                out = jnp.where(rows == h, make(h), out)
            return out

        scores = pick(lambda h: dot_nt(query, blocks_ref[h, :, :dk]), SPAN_LOCATIONS)
        mixing = (scores * scale * cache_weight).astype(jnp.bfloat16)
        query_wide = query.astype(jnp.float32)
        own_term = (
            jnp.sum(query_wide * key.astype(jnp.float32), axis=1, keepdims=True)
            * scale
            * new_weight
        )

        def carry(h):
            return dot_nt(query, state_ref[0, h].astype(jnp.bfloat16))

        carried = pick(carry, dv)
        from_cache = pick(
            lambda h: jnp.dot(
                mixing, blocks_ref[h, :, dk:], preferred_element_type=jnp.float32
            ), dv
        )
        numerator = carried_weight * carried + from_cache + own_term * value.astype(jnp.float32)
        normalizer = (
            carried_weight * jnp.sum(small[:, :dk] * query_wide, axis=1, keepdims=True)
            + jnp.sum(mixing.astype(jnp.float32), axis=1, keepdims=True)
            + own_term
        )
        divisor = jnp.maximum(jnp.maximum(jnp.abs(normalizer), jnp.exp(-stable)), 1.0)
        out_ref[...] = (numerator / divisor).astype(jnp.bfloat16)

    return call(
        body,
        [struct((heads, dv), jnp.bfloat16)],
        [VMEM_SPEC] * (count + 4),
        (
            *parts,
            small,
            resident(state_matrix),
            blocks,
            jnp.pad(lengths, (0, LANES - 1)).reshape(1, -1),
        ),
    )[0]


def attend(pieces, out_weight):
    size = len(pieces)
    heads, dv = pieces[0].shape

    def body(*refs):
        weight_ref, out_ref, hidden_ref = refs[size:]
        position = lax.axis_index("kv")
        for n, d in enumerate([*distances(size), 0]):
            piece = refs[n][...].astype(jnp.float32)
            at = pl.ds(partner_of(position, size, d, True), 1)
            for h in range(heads):
                hidden_ref[at, h * dv : (h + 1) * dv] = piece[h : h + 1]
        out_ref[...] = jnp.dot(
            hidden_ref[...].astype(jnp.bfloat16),
            weight_ref[...],
            preferred_element_type=jnp.float32,
        ).astype(jnp.bfloat16)

    return call(
        body,
        [struct((size, out_weight.shape[1]), jnp.bfloat16)],
        [VMEM_SPEC] * (size + 1),
        (*pieces, resident(out_weight)),
        [pltpu.VMEM((size, heads * dv), jnp.float32)],
    )[0]


def add_features(refs, partners, gain_ref, up_ref, product, squares):
    size = lax.axis_size("kv")
    for ref, d in zip(refs, partners):
        columns = ref.shape[1]
        j = partner_of(lax.axis_index("kv"), size, d, True)
        at = pl.ds(pl.multiple_of(j * columns, columns), columns)
        wide = ref[...].astype(jnp.float32)
        squares = squares + jnp.sum(wide * wide, axis=1, keepdims=True)
        mixer_in = (wide * gain_ref[:, at]).astype(jnp.bfloat16)
        product = product + dot_nt(mixer_in, up_ref[:, at])
    return product, squares


def absorb(pieces, partners, mixer_gain, up_weight):
    rows = pieces[0].shape[0]
    units = up_weight.shape[0]
    count = len(pieces)

    def body(*refs):
        gain_ref, up_ref, product_ref, squares_ref = refs[count:]
        product, squares = add_features(
            refs[:count],
            partners,
            gain_ref,
            up_ref,
            jnp.zeros((rows, units), jnp.float32),
            jnp.zeros((rows, 1), jnp.float32),
        )
        product_ref[...] = product
        squares_ref[...] = jnp.broadcast_to(squares, (rows, LANES))

    return call(
        body,
        [struct((rows, units), jnp.float32), struct((rows, LANES), jnp.float32)],
        [VMEM_SPEC] * (count + 2),
        (*pieces, mixer_gain, up_weight),
        flops=20000000000,
    )


def mix(pieces, partners, before, residual, mixer_gain, up_weight, down_weight):
    size = lax.axis_size("kv")
    count = len(pieces)
    rows, columns = residual.shape
    blocks = [*around(size), 0]
    share = columns // 2

    def body(*refs):
        product_ref, squares_ref, residual_ref, gain_ref, up_ref, down_ref, *outs = refs[count:]
        position = lax.axis_index("kv")
        product, squares = add_features(
            refs[:count], partners, gain_ref, up_ref, product_ref[...], squares_ref[:, :1]
        )
        scaled = product * lax.rsqrt(squares / D + epsilon)
        activated = jnp.square(jnp.maximum(scaled, 0.0)).astype(jnp.bfloat16)
        for n, d in enumerate(blocks):
            j = lax.rem(position + d, size)
            at = pl.ds(pl.multiple_of(j * columns, columns), columns)
            terms = jnp.dot(activated, down_ref[:, at], preferred_element_type=jnp.float32)
            if d == 0:
                half = lax.broadcasted_iota(jnp.int32, (rows, columns), 1) // share
                kept = residual_ref[...].astype(jnp.float32)
                terms = terms + jnp.where(half == lax.axis_index("tp"), kept, 0.0)
            outs[n][...] = terms

    return call(
        body,
        [struct((rows, columns), jnp.float32)] * len(blocks),
        [VMEM_SPEC] * (count + 6),
        (*pieces, *before, residual, mixer_gain, up_weight, down_weight),
        flops=20000000000,
    )


def exchange_pairs(size, cores, distance, ring):
    chips = partner_pairs(size, distance)
    if ring:
        chips = [(i, (i + distance) % size) for i in range(size)]
    return [
        (i * cores + t, j * cores + (cores - 1 - t))
        for i, j in chips
        for t in range(cores)
    ]


def around(size):
    return [*range(1, size)]


def distances(size):
    return [*range(size // 2, size), *range(1, size // 2)]


def to_partners(outgoing, partners, ring=False):
    size, cores = lax.axis_size("kv"), lax.axis_size("tp")
    received = []
    for d in partners:
        pairs = exchange_pairs(size, cores, d, ring)
        received.append(lax.ppermute(outgoing[d], ("kv", "tp"), pairs))
    return received


def swapped(array):
    return lax.ppermute(array, "tp", [(0, 1), (1, 0)])


def direct(mesh, arrays_shape):
    size, cores = mesh["kv"], mesh["tp"]
    sequences, features = arrays_shape
    groups = mesh["dp"] * size
    return (
        2 < size <= DIRECT_LIMIT
        and cores == 2
        and sequences == groups
        and features % (size * 2 * LANES) == 0
    )


def shards_direct(
    tokens,
    norm_gain,
    query_weight,
    key_weight,
    value_weight,
    gate_weight,
    forget_bias,
    state_matrix,
    state_normalizer,
    state_max,
    block_keys,
    block_values,
    block_input,
    block_logf,
    lengths,
    out_weight,
    mixer_gain,
    up_weight,
    down_weight,
):
    head_half = lax.axis_index("tp")
    size = lax.axis_size("kv")
    order = distances(size)
    state_matrix = swapped(state_matrix)
    *parts, small, blocks = project(
        tokens,
        norm_gain,
        query_weight,
        key_weight,
        value_weight,
        gate_weight,
        forget_bias,
        state_normalizer,
        state_max,
        block_keys,
        block_values,
        block_input,
        block_logf,
    )
    parts = to_partners(parts, [*order, 0])
    hidden = recall(parts, swapped(small), state_matrix, swapped(blocks), lengths)
    pieces = to_partners([hidden] * size, [*order, 0])
    partial_out = attend(pieces, out_weight)
    other_out = swapped(partial_out)
    attended = partial_out.astype(jnp.float32) + other_out.astype(jnp.float32)
    residual = (tokens.astype(jnp.float32) + attended).astype(jnp.bfloat16)
    gain = mixer_gain.reshape(1, -1)
    pieces = to_partners([residual] * size, order)
    order = distances(size)
    up_weight, down_weight = resident(up_weight), resident(down_weight)
    absorbed = absorb([residual, pieces[0]], [0, order[0]], gain, up_weight)
    *terms, own = mix(
        pieces[1:], order[1:], absorbed, residual, gain, up_weight, down_weight
    )
    steps = around(size)
    outgoing = dict(zip(steps, terms))
    total = own
    for term in to_partners(outgoing, steps, True):
        total = total + term
    share = tokens.shape[1] // 2
    other = lax.dynamic_slice_in_dim(total, (1 - head_half) * share, share, 1)
    kept = lax.dynamic_slice_in_dim(total, head_half * share, share, 1)
    return (kept + swapped(other)).astype(jnp.bfloat16)


def mapped(mesh, function):
    return jax.shard_map(
        function,
        mesh=mesh,
        in_specs=(
            P("dp", "kv"),
            P("kv"),
            P("kv", "tp"),
            P("kv", "tp"),
            P("kv", "tp"),
            P(),
            P("tp"),
            P(("dp", "kv"), "tp", None, None),
            P(("dp", "kv"), "tp", None),
            P(("dp", "kv"), "tp"),
            P(("dp", "kv"), "tp", None, None),
            P(("dp", "kv"), "tp", None, None),
            P(("dp", "kv"), "tp", None),
            P(("dp", "kv"), "tp", None),
            P(("dp", "kv")),
            P("tp", "kv"),
            P(),
            P(("kv", "tp"), None),
            P(("kv", "tp"), None),
        ),
        out_specs=P("dp", ("kv", "tp")),
        check_vma=False,
    )


def solution(mesh):
    sizes = dict(mesh.shape)

    def whole(*arrays):
        return mapped(mesh, shards_general)(*arrays)

    def small(*arrays):
        if not direct(sizes, arrays[0].shape):
            return whole(*arrays)
        return mapped(mesh, shards_direct)(*arrays)

    if not 2 < sizes["kv"] <= DIRECT_LIMIT:
        return whole
    return small
```

```python
import jax
import jax.numpy as jnp
from jax import lax
from jax.experimental import pallas as pl
from jax.experimental.pallas import tpu as pltpu
from jax.sharding import PartitionSpec as P

D = 4096
DK = 256
DV = 512
SPAN_LOCATIONS = 64


epsilon = 1e-06
highest = lax.Precision.HIGHEST


def memory_cell(
    query,
    key,
    value,
    gates,
    forget_bias,
    state_matrix,
    state_normalizer,
    state_max,
    block_keys,
    block_values,
    block_input,
    block_logf,
    lengths,
):
    live = lengths % SPAN_LOCATIONS
    positions = lax.broadcasted_iota(jnp.int32, (1, 1, SPAN_LOCATIONS), 2)
    inside = positions < live[:, None, None]
    new_input = gates[:, 0]
    new_logf = jax.nn.log_sigmoid(gates[:, 1] + forget_bias)
    cumulative = jnp.cumsum(jnp.where(inside, block_logf, jnp.float32(0.0)), axis=2)
    total = cumulative[:, :, -1] + new_logf
    carried_log = total + state_max
    cache_log = jnp.where(inside, total[:, :, None] - cumulative + block_input, -jnp.inf)
    stable = jnp.maximum(jnp.maximum(carried_log, jnp.max(cache_log, axis=2)), new_input)
    carried_weight = jnp.exp(carried_log - stable)
    new_weight = jnp.exp(new_input - stable)
    cache_weight = jnp.exp(cache_log - stable[:, :, None])
    scores = jnp.einsum("bhk,bhsk->bhs", query, block_keys, preferred_element_type=jnp.float32)
    mixing = (scores * DK ** (-0.5) * cache_weight).astype(jnp.bfloat16)
    query_wide = query.astype(jnp.float32)
    own_term = jnp.sum(query_wide * key.astype(jnp.float32), axis=2) * DK ** (-0.5) * new_weight
    carried = jnp.einsum("bhvk,bhk->bhv", state_matrix, query_wide, precision=highest)
    from_cache = jnp.einsum(
        "bhs,bhsv->bhv", mixing, block_values, preferred_element_type=jnp.float32
    )
    numerator = (
        carried_weight[:, :, None] * carried
        + from_cache
        + own_term[:, :, None] * value.astype(jnp.float32)
    )
    normalizer = (
        carried_weight * jnp.sum(state_normalizer * query_wide, axis=2)
        + jnp.sum(mixing.astype(jnp.float32), axis=2)
        + own_term
    )
    divisor = jnp.maximum(jnp.maximum(jnp.abs(normalizer), jnp.exp(-stable)), jnp.float32(1.0))
    hidden = numerator / divisor[:, :, None]
    return hidden.astype(jnp.bfloat16)


def absorb_columns(mixer_gain, up_weight):

    def absorb(carry, piece, start):
        widened = piece.astype(jnp.float32)
        mixer_in = (widened * mixer_gain).astype(jnp.bfloat16)
        product = lax.dot_general(
            mixer_in, up_weight, (((1,), (1,)), ((), ())), preferred_element_type=jnp.float32
        )
        return (product, jnp.sum(widened * widened, axis=1))

    return absorb


def down_terms(carry, down_weight):
    accumulated, squares = carry
    scaled = accumulated * lax.rsqrt(squares / D + epsilon)[:, None]
    activated = jnp.square(jax.nn.relu(scaled)).astype(jnp.bfloat16)
    return jnp.dot(activated, down_weight, preferred_element_type=jnp.float32)


DIRECT_LIMIT = 8


def partner_pairs(size, distance):
    if size & (size - 1) == 0:
        return [(i, i ^ distance) for i in range(size)]
    return [(i, (i + distance) % size) for i in range(size)]


def partner_of(position, size, distance, receiving):
    if size & (size - 1) == 0:
        return position ^ distance
    return (position - distance) % size if receiving else (position + distance) % size


def gather_direct(piece, axis):
    size = lax.axis_size(axis)
    if size > DIRECT_LIMIT:
        return lax.all_gather(piece, axis, axis=0)
    position = lax.axis_index(axis)
    received = [piece] + [
        lax.ppermute(piece, axis, partner_pairs(size, d)) for d in range(1, size)
    ]
    stacked = jnp.stack(received)
    places = jnp.arange(size)
    if size & (size - 1) == 0:
        order = position ^ places
    else:
        order = (position - places) % size
    return stacked[order]


def scatter_sum_direct(parts, axis):
    size = lax.axis_size(axis)
    if size > DIRECT_LIMIT:
        return lax.psum_scatter(parts, axis, scatter_dimension=0, tiled=False)
    position = lax.axis_index(axis)

    def entry(index):
        return lax.dynamic_index_in_dim(parts, index, 0, keepdims=False)

    total = entry(position)
    for d in range(1, size):
        out = entry(partner_of(position, size, d, False))
        total = total + lax.ppermute(out, axis, partner_pairs(size, d))
    return total


def shards_general(
    tokens,
    norm_gain,
    query_weight,
    key_weight,
    value_weight,
    gate_weight,
    forget_bias,
    state_matrix,
    state_normalizer,
    state_max,
    block_keys,
    block_values,
    block_input,
    block_logf,
    lengths,
    out_weight,
    mixer_gain,
    up_weight,
    down_weight,
):
    position = lax.axis_index("kv")
    head_half = lax.axis_index("tp")
    columns = tokens.shape[1]
    local_heads = forget_bias.shape[0]
    local_rows = lengths.shape[0]
    widened = tokens.astype(jnp.float32)
    squares = jnp.sum(widened * widened, axis=1)
    normed = (widened * norm_gain).astype(jnp.bfloat16)
    gate_rows = lax.dynamic_slice_in_dim(gate_weight, position * columns, columns, 0)
    gate_rows = lax.dynamic_slice_in_dim(
        gate_rows, head_half * local_heads, local_heads, 2
    ).reshape(columns, 2 * local_heads)
    query_part = jnp.dot(normed, query_weight, preferred_element_type=jnp.float32)
    key_part = jnp.dot(normed, key_weight, preferred_element_type=jnp.float32)
    value_part = jnp.dot(normed, value_weight, preferred_element_type=jnp.float32)
    gate_part = jnp.dot(normed, gate_rows, preferred_element_type=jnp.float32)
    parts = jnp.concatenate(
        [query_part, key_part, value_part, gate_part, squares[:, None]], axis=1
    )
    parts = parts.reshape(-1, local_rows, parts.shape[1])
    sums = scatter_sum_direct(parts, "kv")
    q_end = query_part.shape[1]
    k_end = q_end + key_part.shape[1]
    v_end = k_end + value_part.shape[1]
    g_end = v_end + gate_part.shape[1]
    query_sum, key_sum, value_sum, gate_sum, own_squares = (
        sums[:, :q_end],
        sums[:, q_end:k_end],
        sums[:, k_end:v_end],
        sums[:, v_end:g_end],
        sums[:, g_end],
    )
    row_scale = lax.rsqrt(own_squares / D + epsilon)[:, None]
    query = (query_sum * row_scale).astype(jnp.bfloat16).reshape(local_rows, local_heads, DK)
    key = (key_sum * row_scale).astype(jnp.bfloat16).reshape(local_rows, local_heads, DK)
    value = (value_sum * row_scale).astype(jnp.bfloat16).reshape(local_rows, local_heads, DV)
    gates = (gate_sum * row_scale).reshape(local_rows, 2, local_heads)
    hidden = memory_cell(
        query,
        key,
        value,
        gates,
        forget_bias,
        state_matrix,
        state_normalizer,
        state_max,
        block_keys,
        block_values,
        block_input,
        block_logf,
        lengths,
    )
    hidden = hidden.reshape(local_rows, local_heads * DV)
    every_hidden = gather_direct(hidden, "kv").reshape(-1, hidden.shape[1])
    partial_out = jnp.dot(
        every_hidden, out_weight, preferred_element_type=jnp.float32
    ).astype(jnp.bfloat16)
    attended = jnp.sum(gather_direct(partial_out, "tp").astype(jnp.float32), axis=0)
    residual = (widened + attended).astype(jnp.bfloat16)
    absorb = absorb_columns(mixer_gain, up_weight)
    hidden_units = up_weight.shape[0]
    rows = residual.shape[0]
    initial = (jnp.zeros((rows, hidden_units), jnp.float32), jnp.zeros((rows,), jnp.float32))
    pieces = gather_direct(residual, "kv")
    whole = jnp.moveaxis(pieces, 0, 1).reshape(rows, -1)
    carry = absorb(initial, whole, jnp.int32(0))
    terms = down_terms(carry, down_weight)
    share = columns // lax.axis_size("tp")
    terms = terms.reshape(rows, -1, lax.axis_size("tp"), share)
    by_core = scatter_sum_direct(jnp.moveaxis(terms, 2, 0), "tp")
    mixed_terms = scatter_sum_direct(jnp.moveaxis(by_core, 1, 0), "kv")
    own_residual = lax.dynamic_slice_in_dim(residual, head_half * share, share, 1)
    return (own_residual.astype(jnp.float32) + mixed_terms).astype(jnp.bfloat16)


def dot_nt(left, right):
    return lax.dot_general(
        left, right, (((1,), (1,)), ((), ())), preferred_element_type=jnp.float32
    )


VMEM_SPEC = pl.BlockSpec(memory_space=pltpu.VMEM)
SMEM_SPEC = pl.BlockSpec(memory_space=pltpu.SMEM)
ANY_SPEC = pl.BlockSpec(memory_space=pl.ANY)


def call(body, outs, in_specs, args, scratch=(), limit=8, flops=20000000000, aliases=None):
    return pl.pallas_call(
        body,
        out_shape=outs,
        in_specs=in_specs,
        out_specs=[VMEM_SPEC] * len(outs),
        scratch_shapes=list(scratch),
        input_output_aliases=aliases or {},
        compiler_params=pltpu.CompilerParams(vmem_limit_bytes=limit << 20),
        cost_estimate=pl.CostEstimate(flops=flops, bytes_accessed=1000000, transcendentals=0),
    )(*args)


def resident(weight):
    return pltpu.with_memory_space_constraint(weight, pltpu.VMEM)


def streamed(weight):
    return pltpu.with_memory_space_constraint(weight, pltpu.HBM)


def struct(shape, kind):
    return jax.ShapeDtypeStruct(shape, kind)


LANES = 128


def project(
    tokens,
    norm_gain,
    query_weight,
    key_weight,
    value_weight,
    gate_weight,
    forget_bias,
    state_normalizer,
    state_max,
    block_keys,
    block_values,
    block_input,
    block_logf,
):
    _, heads, dk = state_normalizer.shape
    span, dv = block_values.shape[2:]
    packed_width = dk + 2 * LANES
    rows, columns = tokens.shape
    size = lax.axis_size("kv")
    weights = (query_weight, key_weight, value_weight)
    widths = [w.shape[1] for w in weights]
    starts = [sum(widths[:i]) for i in range(3)]
    width = sum(widths)
    gate_count = gate_weight.shape[1] * gate_weight.shape[2]
    gates = jnp.transpose(gate_weight, (1, 2, 0)).reshape(gate_count, -1)
    cuts = [0, columns]
    small = (forget_bias.reshape(1, -1), state_normalizer, state_max, block_input, block_logf)

    def body(tokens_hbm, gain_hbm, q_hbm, k_hbm, v_hbm, gate_hbm, *rest):
        small_hbm, (keys_hbm, values_hbm), rest = rest[:5], rest[5:7], rest[7:]
        outs, small_out, block_out = rest[:size], rest[size], rest[size + 1]
        rest = rest[size + 2 :]
        tokens_ref, gain_ref, weight_ref, gate_ref, sums_ref = rest[:5]
        sems, gate_sem, tokens_sem, gain_sem, small_sems, block_sems = rest[5:11]
        small_refs = rest[11:]
        position = lax.axis_index("kv")
        tokens_copy = pltpu.make_async_copy(tokens_hbm, tokens_ref, tokens_sem)
        gain_copy = pltpu.make_async_copy(gain_hbm, gain_ref, gain_sem)
        tokens_copy.start()
        gain_copy.start()
        copies = []
        for c in range(len(cuts) - 1):
            at = pl.ds(cuts[c], cuts[c + 1] - cuts[c])
            for w, source in enumerate((q_hbm, k_hbm, v_hbm)):
                copy = pltpu.make_async_copy(
                    source.at[at, :],
                    weight_ref.at[at, pl.ds(starts[w], widths[w])],
                    sems.at[c, w],
                )
                copy.start()
                copies.append(copy)
        gate_copy = pltpu.make_async_copy(
            gate_hbm.at[:, pl.ds(pl.multiple_of(position * columns, columns), columns)],
            gate_ref,
            gate_sem,
        )
        gate_copy.start()
        small_copies = [
            pltpu.make_async_copy(source, target, small_sems.at[i])
            for i, (source, target) in enumerate(zip(small_hbm, small_refs))
        ]
        block_copies = [
            pltpu.make_async_copy(keys_hbm.at[0], block_out.at[:, :, pl.ds(0, dk)], block_sems.at[0]),
            pltpu.make_async_copy(
                values_hbm.at[0], block_out.at[:, :, pl.ds(dk, dv)], block_sems.at[1]
            ),
        ]
        for copy in small_copies + block_copies:
            copy.start()
        tokens_copy.wait()
        gain_copy.wait()
        widened = tokens_ref[...].astype(jnp.float32)
        squares = jnp.sum(widened * widened, axis=1, keepdims=True)
        normed = (widened * gain_ref[...]).astype(jnp.bfloat16)
        for c in range(len(cuts) - 1):
            piece = normed[:, cuts[c] : cuts[c + 1]]
            for w in range(3):
                copies[3 * c + w].wait()
                at = slice(starts[w], starts[w] + widths[w])
                product = jnp.dot(
                    piece,
                    weight_ref[cuts[c] : cuts[c + 1], at],
                    preferred_element_type=jnp.float32,
                )
                if c:
                    product = product + sums_ref[:, at]
                sums_ref[:, at] = product
        for copy in block_copies:
            copy.wait()
        gate_copy.wait()
        gate_sums = dot_nt(normed, gate_ref[...])
        pad = jnp.zeros((rows, LANES - gate_count), jnp.float32)
        extra = jnp.concatenate([gate_sums, pad], axis=1)
        lane = lax.broadcasted_iota(jnp.int32, (rows, LANES), 1)
        sums_ref[:, width:] = jnp.where(lane == gate_count, squares, extra)
        for copy in small_copies:
            copy.wait()
        bias_ref, normalizer_ref, max_ref, input_ref, logf_ref = small_refs
        lane_h = lax.broadcasted_iota(jnp.int32, (heads, heads), 1)
        head_h = lax.broadcasted_iota(jnp.int32, (heads, heads), 0)

        def column(ref):
            values = jnp.broadcast_to(ref[...], (heads, heads))
            return jnp.sum(jnp.where(lane_h == head_h, values, 0.0), axis=1, keepdims=True)

        lane_s = lax.broadcasted_iota(jnp.int32, (heads, LANES), 1)
        small_out[:, :dk] = normalizer_ref[0]
        small_out[:, dk : dk + LANES] = jnp.concatenate([input_ref[0], logf_ref[0]], axis=1)
        small_out[:, dk + LANES :] = jnp.where(lane_s == 0, column(max_ref), column(bias_ref))
        for d in range(size):
            outs[d][...] = sums_ref[pl.ds(partner_of(position, size, d, False), 1), :]

    return call(
        body,
        [struct((1, width + LANES), jnp.float32)] * size
        + [
            struct((heads, packed_width), jnp.float32),
            struct((heads, span, dk + dv), block_keys.dtype),
        ],
        [ANY_SPEC] * 13,
        [
            streamed(a)
            for a in (
                tokens,
                norm_gain.reshape(1, -1),
                *weights,
                gates,
                *small,
                block_keys,
                block_values,
            )
        ],
        [
            pltpu.VMEM(tokens.shape, tokens.dtype),
            pltpu.VMEM((1, columns), norm_gain.dtype),
            pltpu.VMEM((columns, width), query_weight.dtype),
            pltpu.VMEM((gate_count, columns), gates.dtype),
            pltpu.VMEM((rows, width + LANES), jnp.float32),
            pltpu.SemaphoreType.DMA((len(cuts) - 1, 3)),
            pltpu.SemaphoreType.DMA(()),
            pltpu.SemaphoreType.DMA(()),
            pltpu.SemaphoreType.DMA(()),
            pltpu.SemaphoreType.DMA((len(small),)),
            pltpu.SemaphoreType.DMA((2,)),
            *[pltpu.VMEM(a.shape, a.dtype) for a in small],
        ],
        limit=16,
    )


def recall(parts, small, state_matrix, blocks, lengths):
    _, heads, dv, dk = state_matrix.shape
    all_heads = heads * lax.axis_size("tp")
    scale = dk ** (-0.5)
    count = len(parts)

    def body(*refs):
        small_ref, state_ref, blocks_ref, lengths_ref, out_ref = refs[count:]
        half = 1 - lax.axis_index("tp")
        row = refs[0][...]
        for r in refs[1:count]:
            row = row + r[...]
        q_end, k_end = heads * dk, 2 * heads * dk
        v_end = k_end + heads * dv
        extra = row[:, v_end:]
        squares = extra[:, 2 * all_heads : 2 * all_heads + 1]
        row_scale = lax.rsqrt(squares / D + epsilon)
        row = row[:, :v_end] * row_scale

        def by_head(start, size):
            return jnp.concatenate(
                [row[:, start + h * size : start + (h + 1) * size] for h in range(heads)], axis=0
            ).astype(jnp.bfloat16)

        query, key, value = by_head(0, dk), by_head(q_end, dk), by_head(k_end, dv)
        gates = jnp.broadcast_to(extra * row_scale, (heads, LANES))
        lane = lax.broadcasted_iota(jnp.int32, (heads, LANES), 1)
        head = lax.broadcasted_iota(jnp.int32, (heads, LANES), 0)

        def column(values, first):
            return jnp.sum(jnp.where(lane == head + first, values, 0.0), axis=1, keepdims=True)

        small = small_ref[...]
        block_input = small[:, dk : dk + SPAN_LOCATIONS]
        block_logf = small[:, dk + SPAN_LOCATIONS : dk + 2 * SPAN_LOCATIONS]
        state_max = small[:, dk + LANES : dk + LANES + 1]
        bias = small[:, dk + LANES + 1 : dk + LANES + 2]
        span = (heads, SPAN_LOCATIONS)
        live = jnp.broadcast_to(lengths_ref[:, :1] & (SPAN_LOCATIONS - 1), span)
        inside = lax.broadcasted_iota(jnp.int32, span, 1) < live
        rest = jnp.where(inside, block_logf, 0.0)
        square = (SPAN_LOCATIONS, SPAN_LOCATIONS)
        upto = (
            lax.broadcasted_iota(jnp.int32, square, 0) <= lax.broadcasted_iota(jnp.int32, square, 1)
        ).astype(jnp.float32).astype(jnp.bfloat16)
        cumulative = jnp.zeros(span, jnp.float32)
        for _ in range(3):
            term = rest.astype(jnp.bfloat16)
            rest = rest - term.astype(jnp.float32)
            cumulative = cumulative + jnp.dot(term, upto, preferred_element_type=jnp.float32)
        logf_sum = cumulative[:, SPAN_LOCATIONS - 1 :]
        cache_base = jnp.where(inside, logf_sum - cumulative + block_input, -jnp.inf)
        new_input = column(gates, half * heads)
        new_logf = jax.nn.log_sigmoid(column(gates, all_heads + half * heads) + bias)
        carried_log = logf_sum + new_logf + state_max
        cache_log = cache_base + new_logf
        stable = jnp.maximum(
            jnp.maximum(carried_log, jnp.max(cache_log, axis=1, keepdims=True)), new_input
        )
        carried_weight = jnp.exp(carried_log - stable)
        new_weight = jnp.exp(new_input - stable)
        cache_weight = jnp.exp(cache_log - stable)

        def pick(make, size):
            rows = lax.broadcasted_iota(jnp.int32, (heads, size), 0)
            out = jnp.zeros((heads, size), jnp.float32)
            for h in range(heads):
                out = jnp.where(rows == h, make(h), out)
            return out

        scores = pick(lambda h: dot_nt(query, blocks_ref[h, :, :dk]), SPAN_LOCATIONS)
        mixing = (scores * scale * cache_weight).astype(jnp.bfloat16)
        query_wide = query.astype(jnp.float32)
        own_term = (
            jnp.sum(query_wide * key.astype(jnp.float32), axis=1, keepdims=True)
            * scale
            * new_weight
        )

        def carry(h):
            return dot_nt(query, state_ref[0, h].astype(jnp.bfloat16))

        carried = pick(carry, dv)
        from_cache = pick(
            lambda h: jnp.dot(
                mixing, blocks_ref[h, :, dk:], preferred_element_type=jnp.float32
            ), dv
        )
        numerator = carried_weight * carried + from_cache + own_term * value.astype(jnp.float32)
        normalizer = (
            carried_weight * jnp.sum(small[:, :dk] * query_wide, axis=1, keepdims=True)
            + jnp.sum(mixing.astype(jnp.float32), axis=1, keepdims=True)
            + own_term
        )
        divisor = jnp.maximum(jnp.maximum(jnp.abs(normalizer), jnp.exp(-stable)), 1.0)
        out_ref[...] = (numerator / divisor).astype(jnp.bfloat16)

    return call(
        body,
        [struct((heads, dv), jnp.bfloat16)],
        [VMEM_SPEC] * (count + 4),
        (
            *parts,
            small,
            resident(state_matrix),
            blocks,
            jnp.pad(lengths, (0, LANES - 1)).reshape(1, -1),
        ),
    )[0]


def attend(pieces, out_weight):
    size = len(pieces)
    heads, dv = pieces[0].shape

    def body(*refs):
        weight_ref, out_ref, hidden_ref = refs[size:]
        position = lax.axis_index("kv")
        for n, d in enumerate([*distances(size), 0]):
            piece = refs[n][...].astype(jnp.float32)
            at = pl.ds(partner_of(position, size, d, True), 1)
            for h in range(heads):
                hidden_ref[at, h * dv : (h + 1) * dv] = piece[h : h + 1]
        out_ref[...] = jnp.dot(
            hidden_ref[...].astype(jnp.bfloat16),
            weight_ref[...],
            preferred_element_type=jnp.float32,
        ).astype(jnp.bfloat16)

    return call(
        body,
        [struct((size, out_weight.shape[1]), jnp.bfloat16)],
        [VMEM_SPEC] * (size + 1),
        (*pieces, resident(out_weight)),
        [pltpu.VMEM((size, heads * dv), jnp.float32)],
    )[0]


def add_features(refs, partners, gain_ref, up_ref, product, squares):
    size = lax.axis_size("kv")
    for ref, d in zip(refs, partners):
        columns = ref.shape[1]
        j = partner_of(lax.axis_index("kv"), size, d, True)
        at = pl.ds(pl.multiple_of(j * columns, columns), columns)
        wide = ref[...].astype(jnp.float32)
        squares = squares + jnp.sum(wide * wide, axis=1, keepdims=True)
        mixer_in = (wide * gain_ref[:, at]).astype(jnp.bfloat16)
        product = product + dot_nt(mixer_in, up_ref[:, at])
    return product, squares


def absorb(pieces, partners, mixer_gain, up_weight):
    rows = pieces[0].shape[0]
    units = up_weight.shape[0]
    count = len(pieces)

    def body(*refs):
        gain_ref, up_ref, product_ref, squares_ref = refs[count:]
        product, squares = add_features(
            refs[:count],
            partners,
            gain_ref,
            up_ref,
            jnp.zeros((rows, units), jnp.float32),
            jnp.zeros((rows, 1), jnp.float32),
        )
        product_ref[...] = product
        squares_ref[...] = jnp.broadcast_to(squares, (rows, LANES))

    return call(
        body,
        [struct((rows, units), jnp.float32), struct((rows, LANES), jnp.float32)],
        [VMEM_SPEC] * (count + 2),
        (*pieces, mixer_gain, up_weight),
        flops=20000000000,
    )


def mix(pieces, partners, before, mixer_gain, up_weight, down_weight):
    size = lax.axis_size("kv")
    count = len(pieces)
    rows, columns = pieces[0].shape
    blocks = around(size)
    units = up_weight.shape[0]

    def body(*refs):
        product_ref, squares_ref, gain_ref, up_ref, down_ref, *outs = refs[count:]
        position = lax.axis_index("kv")
        product, squares = add_features(
            refs[:count], partners, gain_ref, up_ref, product_ref[...], squares_ref[:, :1]
        )
        scaled = product * lax.rsqrt(squares / D + epsilon)
        activated = jnp.square(jnp.maximum(scaled, 0.0)).astype(jnp.bfloat16)
        outs[-2][...] = activated
        own = pl.ds(pl.multiple_of(position * columns, columns), columns)
        outs[-1][...] = down_ref[:, own]
        for n, d in enumerate(blocks):
            j = lax.rem(position + d, size)
            at = pl.ds(pl.multiple_of(j * columns, columns), columns)
            terms = jnp.dot(activated, down_ref[:, at], preferred_element_type=jnp.float32)
            outs[n][...] = terms.astype(outs[n].dtype)

    return call(
        body,
        [struct((rows, columns), jnp.bfloat16)] * len(blocks)
        + [
            struct((rows, units), jnp.bfloat16),
            struct((units, columns), down_weight.dtype),
        ],
        [VMEM_SPEC] * (count + 5),
        (*pieces, *before, mixer_gain, up_weight, down_weight),
        flops=20000000000,
    )


def mix_own(activated, residual, own_down):
    rows, columns = residual.shape
    share = columns // 2

    def body(activated_ref, residual_ref, down_ref, out_ref):
        terms = jnp.dot(activated_ref[...], down_ref[...], preferred_element_type=jnp.float32)
        half = lax.broadcasted_iota(jnp.int32, (rows, columns), 1) // share
        kept = residual_ref[...].astype(jnp.float32)
        out_ref[...] = terms + jnp.where(half == lax.axis_index("tp"), kept, 0.0)

    return call(
        body,
        [struct((rows, columns), jnp.float32)],
        [VMEM_SPEC] * 3,
        (activated, residual, own_down),
        flops=1000000,
    )[0]


def exchange_pairs(size, cores, distance, ring):
    chips = partner_pairs(size, distance)
    if ring:
        chips = [(i, (i + distance) % size) for i in range(size)]
    return [
        (i * cores + t, j * cores + (cores - 1 - t))
        for i, j in chips
        for t in range(cores)
    ]


def around(size):
    return [*range(1, size)]


def distances(size):
    return [*range(size // 2, size), *range(1, size // 2)]


def to_partners(outgoing, partners, ring=False):
    size, cores = lax.axis_size("kv"), lax.axis_size("tp")
    received = []
    for d in partners:
        pairs = exchange_pairs(size, cores, d, ring)
        received.append(lax.ppermute(outgoing[d], ("kv", "tp"), pairs))
    return received


def swapped(array):
    return lax.ppermute(array, "tp", [(0, 1), (1, 0)])


def direct(mesh, arrays_shape):
    size, cores = mesh["kv"], mesh["tp"]
    sequences, features = arrays_shape
    groups = mesh["dp"] * size
    return (
        2 < size <= DIRECT_LIMIT
        and cores == 2
        and sequences == groups
        and features % (size * 2 * LANES) == 0
    )


def shards_direct(
    tokens,
    norm_gain,
    query_weight,
    key_weight,
    value_weight,
    gate_weight,
    forget_bias,
    state_matrix,
    state_normalizer,
    state_max,
    block_keys,
    block_values,
    block_input,
    block_logf,
    lengths,
    out_weight,
    mixer_gain,
    up_weight,
    down_weight,
):
    head_half = lax.axis_index("tp")
    size = lax.axis_size("kv")
    order = distances(size)
    state_matrix = swapped(state_matrix)
    *parts, small, blocks = project(
        tokens,
        norm_gain,
        query_weight,
        key_weight,
        value_weight,
        gate_weight,
        forget_bias,
        state_normalizer,
        state_max,
        block_keys,
        block_values,
        block_input,
        block_logf,
    )
    parts = to_partners(parts, [*order, 0])
    hidden = recall(parts, swapped(small), state_matrix, swapped(blocks), lengths)
    pieces = to_partners([hidden] * size, [*order, 0])
    partial_out = attend(pieces, out_weight)
    other_out = swapped(partial_out)
    attended = partial_out.astype(jnp.float32) + other_out.astype(jnp.float32)
    residual = (tokens.astype(jnp.float32) + attended).astype(jnp.bfloat16)
    gain = mixer_gain.reshape(1, -1)
    pieces = to_partners([residual] * size, order)
    order = distances(size)
    up_weight, down_weight = resident(up_weight), resident(down_weight)
    absorbed = absorb([residual, pieces[0]], [0, order[0]], gain, up_weight)
    *terms, activated, own_down = mix(
        pieces[1:], order[1:], absorbed, gain, up_weight, down_weight
    )
    own = mix_own(activated, residual, own_down)
    steps = around(size)
    outgoing = dict(zip(steps, terms))
    total = own
    for term in to_partners(outgoing, steps, True):
        total = total + term.astype(jnp.float32)
    share = tokens.shape[1] // 2
    other = lax.dynamic_slice_in_dim(total, (1 - head_half) * share, share, 1)
    kept = lax.dynamic_slice_in_dim(total, head_half * share, share, 1)
    return (kept + swapped(other)).astype(jnp.bfloat16)


def mapped(mesh, function):
    return jax.shard_map(
        function,
        mesh=mesh,
        in_specs=(
            P("dp", "kv"),
            P("kv"),
            P("kv", "tp"),
            P("kv", "tp"),
            P("kv", "tp"),
            P(),
            P("tp"),
            P(("dp", "kv"), "tp", None, None),
            P(("dp", "kv"), "tp", None),
            P(("dp", "kv"), "tp"),
            P(("dp", "kv"), "tp", None, None),
            P(("dp", "kv"), "tp", None, None),
            P(("dp", "kv"), "tp", None),
            P(("dp", "kv"), "tp", None),
            P(("dp", "kv")),
            P("tp", "kv"),
            P(),
            P(("kv", "tp"), None),
            P(("kv", "tp"), None),
        ),
        out_specs=P("dp", ("kv", "tp")),
        check_vma=False,
    )


def solution(mesh):
    sizes = dict(mesh.shape)

    def whole(*arrays):
        return mapped(mesh, shards_general)(*arrays)

    def small(*arrays):
        if not direct(sizes, arrays[0].shape):
            return whole(*arrays)
        return mapped(mesh, shards_direct)(*arrays)

    if not 2 < sizes["kv"] <= DIRECT_LIMIT:
        return whole
    return small
```

```python
import jax
import jax.numpy as jnp
from jax import lax
from jax.experimental import pallas as pl
from jax.experimental.pallas import tpu as pltpu
from jax.sharding import PartitionSpec as P

D = 4096
DK = 256
DV = 512
SPAN_LOCATIONS = 64


epsilon = 1e-06
highest = lax.Precision.HIGHEST


def memory_cell(
    query,
    key,
    value,
    gates,
    forget_bias,
    state_matrix,
    state_normalizer,
    state_max,
    block_keys,
    block_values,
    block_input,
    block_logf,
    lengths,
):
    live = lengths % SPAN_LOCATIONS
    positions = lax.broadcasted_iota(jnp.int32, (1, 1, SPAN_LOCATIONS), 2)
    inside = positions < live[:, None, None]
    new_input = gates[:, 0]
    new_logf = jax.nn.log_sigmoid(gates[:, 1] + forget_bias)
    cumulative = jnp.cumsum(jnp.where(inside, block_logf, jnp.float32(0.0)), axis=2)
    total = cumulative[:, :, -1] + new_logf
    carried_log = total + state_max
    cache_log = jnp.where(inside, total[:, :, None] - cumulative + block_input, -jnp.inf)
    stable = jnp.maximum(jnp.maximum(carried_log, jnp.max(cache_log, axis=2)), new_input)
    carried_weight = jnp.exp(carried_log - stable)
    new_weight = jnp.exp(new_input - stable)
    cache_weight = jnp.exp(cache_log - stable[:, :, None])
    scores = jnp.einsum("bhk,bhsk->bhs", query, block_keys, preferred_element_type=jnp.float32)
    mixing = (scores * DK ** (-0.5) * cache_weight).astype(jnp.bfloat16)
    query_wide = query.astype(jnp.float32)
    own_term = jnp.sum(query_wide * key.astype(jnp.float32), axis=2) * DK ** (-0.5) * new_weight
    carried = jnp.einsum("bhvk,bhk->bhv", state_matrix, query_wide, precision=highest)
    from_cache = jnp.einsum(
        "bhs,bhsv->bhv", mixing, block_values, preferred_element_type=jnp.float32
    )
    numerator = (
        carried_weight[:, :, None] * carried
        + from_cache
        + own_term[:, :, None] * value.astype(jnp.float32)
    )
    normalizer = (
        carried_weight * jnp.sum(state_normalizer * query_wide, axis=2)
        + jnp.sum(mixing.astype(jnp.float32), axis=2)
        + own_term
    )
    divisor = jnp.maximum(jnp.maximum(jnp.abs(normalizer), jnp.exp(-stable)), jnp.float32(1.0))
    hidden = numerator / divisor[:, :, None]
    return hidden.astype(jnp.bfloat16)


def absorb_columns(mixer_gain, up_weight):

    def absorb(carry, piece, start):
        widened = piece.astype(jnp.float32)
        mixer_in = (widened * mixer_gain).astype(jnp.bfloat16)
        product = lax.dot_general(
            mixer_in, up_weight, (((1,), (1,)), ((), ())), preferred_element_type=jnp.float32
        )
        return (product, jnp.sum(widened * widened, axis=1))

    return absorb


def down_terms(carry, down_weight):
    accumulated, squares = carry
    scaled = accumulated * lax.rsqrt(squares / D + epsilon)[:, None]
    activated = jnp.square(jax.nn.relu(scaled)).astype(jnp.bfloat16)
    return jnp.dot(activated, down_weight, preferred_element_type=jnp.float32)


DIRECT_LIMIT = 8


def partner_pairs(size, distance):
    if size & (size - 1) == 0:
        return [(i, i ^ distance) for i in range(size)]
    return [(i, (i + distance) % size) for i in range(size)]


def partner_of(position, size, distance, receiving):
    if size & (size - 1) == 0:
        return position ^ distance
    return (position - distance) % size if receiving else (position + distance) % size


def gather_direct(piece, axis):
    size = lax.axis_size(axis)
    if size > DIRECT_LIMIT:
        return lax.all_gather(piece, axis, axis=0)
    position = lax.axis_index(axis)
    received = [piece] + [
        lax.ppermute(piece, axis, partner_pairs(size, d)) for d in range(1, size)
    ]
    stacked = jnp.stack(received)
    places = jnp.arange(size)
    if size & (size - 1) == 0:
        order = position ^ places
    else:
        order = (position - places) % size
    return stacked[order]


def scatter_sum_direct(parts, axis):
    size = lax.axis_size(axis)
    if size > DIRECT_LIMIT:
        return lax.psum_scatter(parts, axis, scatter_dimension=0, tiled=False)
    position = lax.axis_index(axis)

    def entry(index):
        return lax.dynamic_index_in_dim(parts, index, 0, keepdims=False)

    total = entry(position)
    for d in range(1, size):
        out = entry(partner_of(position, size, d, False))
        total = total + lax.ppermute(out, axis, partner_pairs(size, d))
    return total


def shards_general(
    tokens,
    norm_gain,
    query_weight,
    key_weight,
    value_weight,
    gate_weight,
    forget_bias,
    state_matrix,
    state_normalizer,
    state_max,
    block_keys,
    block_values,
    block_input,
    block_logf,
    lengths,
    out_weight,
    mixer_gain,
    up_weight,
    down_weight,
):
    position = lax.axis_index("kv")
    head_half = lax.axis_index("tp")
    columns = tokens.shape[1]
    local_heads = forget_bias.shape[0]
    local_rows = lengths.shape[0]
    widened = tokens.astype(jnp.float32)
    squares = jnp.sum(widened * widened, axis=1)
    normed = (widened * norm_gain).astype(jnp.bfloat16)
    gate_rows = lax.dynamic_slice_in_dim(gate_weight, position * columns, columns, 0)
    gate_rows = lax.dynamic_slice_in_dim(
        gate_rows, head_half * local_heads, local_heads, 2
    ).reshape(columns, 2 * local_heads)
    query_part = jnp.dot(normed, query_weight, preferred_element_type=jnp.float32)
    key_part = jnp.dot(normed, key_weight, preferred_element_type=jnp.float32)
    value_part = jnp.dot(normed, value_weight, preferred_element_type=jnp.float32)
    gate_part = jnp.dot(normed, gate_rows, preferred_element_type=jnp.float32)
    parts = jnp.concatenate(
        [query_part, key_part, value_part, gate_part, squares[:, None]], axis=1
    )
    parts = parts.reshape(-1, local_rows, parts.shape[1])
    sums = scatter_sum_direct(parts, "kv")
    q_end = query_part.shape[1]
    k_end = q_end + key_part.shape[1]
    v_end = k_end + value_part.shape[1]
    g_end = v_end + gate_part.shape[1]
    query_sum, key_sum, value_sum, gate_sum, own_squares = (
        sums[:, :q_end],
        sums[:, q_end:k_end],
        sums[:, k_end:v_end],
        sums[:, v_end:g_end],
        sums[:, g_end],
    )
    row_scale = lax.rsqrt(own_squares / D + epsilon)[:, None]
    query = (query_sum * row_scale).astype(jnp.bfloat16).reshape(local_rows, local_heads, DK)
    key = (key_sum * row_scale).astype(jnp.bfloat16).reshape(local_rows, local_heads, DK)
    value = (value_sum * row_scale).astype(jnp.bfloat16).reshape(local_rows, local_heads, DV)
    gates = (gate_sum * row_scale).reshape(local_rows, 2, local_heads)
    hidden = memory_cell(
        query,
        key,
        value,
        gates,
        forget_bias,
        state_matrix,
        state_normalizer,
        state_max,
        block_keys,
        block_values,
        block_input,
        block_logf,
        lengths,
    )
    hidden = hidden.reshape(local_rows, local_heads * DV)
    every_hidden = gather_direct(hidden, "kv").reshape(-1, hidden.shape[1])
    partial_out = jnp.dot(
        every_hidden, out_weight, preferred_element_type=jnp.float32
    ).astype(jnp.bfloat16)
    attended = jnp.sum(gather_direct(partial_out, "tp").astype(jnp.float32), axis=0)
    residual = (widened + attended).astype(jnp.bfloat16)
    absorb = absorb_columns(mixer_gain, up_weight)
    hidden_units = up_weight.shape[0]
    rows = residual.shape[0]
    initial = (jnp.zeros((rows, hidden_units), jnp.float32), jnp.zeros((rows,), jnp.float32))
    pieces = gather_direct(residual, "kv")
    whole = jnp.moveaxis(pieces, 0, 1).reshape(rows, -1)
    carry = absorb(initial, whole, jnp.int32(0))
    terms = down_terms(carry, down_weight)
    share = columns // lax.axis_size("tp")
    terms = terms.reshape(rows, -1, lax.axis_size("tp"), share)
    by_core = scatter_sum_direct(jnp.moveaxis(terms, 2, 0), "tp")
    mixed_terms = scatter_sum_direct(jnp.moveaxis(by_core, 1, 0), "kv")
    own_residual = lax.dynamic_slice_in_dim(residual, head_half * share, share, 1)
    return (own_residual.astype(jnp.float32) + mixed_terms).astype(jnp.bfloat16)


def dot_nt(left, right):
    return lax.dot_general(
        left, right, (((1,), (1,)), ((), ())), preferred_element_type=jnp.float32
    )


VMEM_SPEC = pl.BlockSpec(memory_space=pltpu.VMEM)
SMEM_SPEC = pl.BlockSpec(memory_space=pltpu.SMEM)
ANY_SPEC = pl.BlockSpec(memory_space=pl.ANY)


def call(body, outs, in_specs, args, scratch=(), limit=8, flops=20000000000, aliases=None):
    return pl.pallas_call(
        body,
        out_shape=outs,
        in_specs=in_specs,
        out_specs=[VMEM_SPEC] * len(outs),
        scratch_shapes=list(scratch),
        input_output_aliases=aliases or {},
        compiler_params=pltpu.CompilerParams(vmem_limit_bytes=limit << 20),
        cost_estimate=pl.CostEstimate(flops=flops, bytes_accessed=1000000, transcendentals=0),
    )(*args)


def resident(weight):
    return pltpu.with_memory_space_constraint(weight, pltpu.VMEM)


def streamed(weight):
    return pltpu.with_memory_space_constraint(weight, pltpu.HBM)


def struct(shape, kind):
    return jax.ShapeDtypeStruct(shape, kind)


LANES = 128


def project(
    tokens,
    norm_gain,
    query_weight,
    key_weight,
    value_weight,
    gate_weight,
    forget_bias,
    state_normalizer,
    state_max,
    block_input,
    block_logf,
):
    _, heads, dk = state_normalizer.shape
    packed_width = dk + 2 * LANES
    rows, columns = tokens.shape
    size = lax.axis_size("kv")
    weights = (query_weight, key_weight, value_weight)
    widths = [w.shape[1] for w in weights]
    starts = [sum(widths[:i]) for i in range(3)]
    width = sum(widths)
    gate_count = gate_weight.shape[1] * gate_weight.shape[2]
    gates = jnp.transpose(gate_weight, (1, 2, 0)).reshape(gate_count, -1)
    cuts = [0, columns]
    small = (forget_bias.reshape(1, -1), state_normalizer, state_max, block_input, block_logf)

    def body(tokens_hbm, gain_hbm, q_hbm, k_hbm, v_hbm, gate_hbm, *rest):
        small_hbm, rest = rest[:5], rest[5:]
        outs, small_out = rest[:size], rest[size]
        rest = rest[size + 1 :]
        tokens_ref, gain_ref, weight_ref, gate_ref, sums_ref = rest[:5]
        sems, gate_sem, tokens_sem, gain_sem, small_sems = rest[5:10]
        small_refs = rest[10:]
        position = lax.axis_index("kv")
        tokens_copy = pltpu.make_async_copy(tokens_hbm, tokens_ref, tokens_sem)
        gain_copy = pltpu.make_async_copy(gain_hbm, gain_ref, gain_sem)
        tokens_copy.start()
        gain_copy.start()
        copies = []
        for c in range(len(cuts) - 1):
            at = pl.ds(cuts[c], cuts[c + 1] - cuts[c])
            for w, source in enumerate((q_hbm, k_hbm, v_hbm)):
                copy = pltpu.make_async_copy(
                    source.at[at, :],
                    weight_ref.at[at, pl.ds(starts[w], widths[w])],
                    sems.at[c, w],
                )
                copy.start()
                copies.append(copy)
        gate_copy = pltpu.make_async_copy(
            gate_hbm.at[:, pl.ds(pl.multiple_of(position * columns, columns), columns)],
            gate_ref,
            gate_sem,
        )
        gate_copy.start()
        small_copies = [
            pltpu.make_async_copy(source, target, small_sems.at[i])
            for i, (source, target) in enumerate(zip(small_hbm, small_refs))
        ]
        for copy in small_copies:
            copy.start()
        tokens_copy.wait()
        gain_copy.wait()
        widened = tokens_ref[...].astype(jnp.float32)
        squares = jnp.sum(widened * widened, axis=1, keepdims=True)
        normed = (widened * gain_ref[...]).astype(jnp.bfloat16)
        for c in range(len(cuts) - 1):
            piece = normed[:, cuts[c] : cuts[c + 1]]
            for w in range(3):
                copies[3 * c + w].wait()
                at = slice(starts[w], starts[w] + widths[w])
                product = jnp.dot(
                    piece,
                    weight_ref[cuts[c] : cuts[c + 1], at],
                    preferred_element_type=jnp.float32,
                )
                if c:
                    product = product + sums_ref[:, at]
                sums_ref[:, at] = product
        gate_copy.wait()
        gate_sums = dot_nt(normed, gate_ref[...])
        pad = jnp.zeros((rows, LANES - gate_count), jnp.float32)
        extra = jnp.concatenate([gate_sums, pad], axis=1)
        lane = lax.broadcasted_iota(jnp.int32, (rows, LANES), 1)
        sums_ref[:, width:] = jnp.where(lane == gate_count, squares, extra)
        for copy in small_copies:
            copy.wait()
        bias_ref, normalizer_ref, max_ref, input_ref, logf_ref = small_refs
        lane_h = lax.broadcasted_iota(jnp.int32, (heads, heads), 1)
        head_h = lax.broadcasted_iota(jnp.int32, (heads, heads), 0)

        def column(ref):
            values = jnp.broadcast_to(ref[...], (heads, heads))
            return jnp.sum(jnp.where(lane_h == head_h, values, 0.0), axis=1, keepdims=True)

        lane_s = lax.broadcasted_iota(jnp.int32, (heads, LANES), 1)
        small_out[:, :dk] = normalizer_ref[0]
        small_out[:, dk : dk + LANES] = jnp.concatenate([input_ref[0], logf_ref[0]], axis=1)
        small_out[:, dk + LANES :] = jnp.where(lane_s == 0, column(max_ref), column(bias_ref))
        for d in range(size):
            outs[d][...] = sums_ref[pl.ds(partner_of(position, size, d, False), 1), :]

    return call(
        body,
        [struct((1, width + LANES), jnp.float32)] * size
        + [
            struct((heads, packed_width), jnp.float32),
        ],
        [ANY_SPEC] * 11,
        [
            streamed(a)
            for a in (
                tokens,
                norm_gain.reshape(1, -1),
                *weights,
                gates,
                *small,
            )
        ],
        [
            pltpu.VMEM(tokens.shape, tokens.dtype),
            pltpu.VMEM((1, columns), norm_gain.dtype),
            pltpu.VMEM((columns, width), query_weight.dtype),
            pltpu.VMEM((gate_count, columns), gates.dtype),
            pltpu.VMEM((rows, width + LANES), jnp.float32),
            pltpu.SemaphoreType.DMA((len(cuts) - 1, 3)),
            pltpu.SemaphoreType.DMA(()),
            pltpu.SemaphoreType.DMA(()),
            pltpu.SemaphoreType.DMA(()),
            pltpu.SemaphoreType.DMA((len(small),)),
            *[pltpu.VMEM(a.shape, a.dtype) for a in small],
        ],
        limit=16,
    )


def recall(parts, small, state_matrix, block_keys, block_values, lengths):
    _, heads, dv, dk = state_matrix.shape
    all_heads = heads * lax.axis_size("tp")
    scale = dk ** (-0.5)
    count = len(parts)

    def body(*refs):
        small_ref, state_ref, keys_ref, values_ref, lengths_ref, out_ref = refs[count:]
        half = 1 - lax.axis_index("tp")
        row = refs[0][...]
        for r in refs[1:count]:
            row = row + r[...]
        q_end, k_end = heads * dk, 2 * heads * dk
        v_end = k_end + heads * dv
        extra = row[:, v_end:]
        squares = extra[:, 2 * all_heads : 2 * all_heads + 1]
        row_scale = lax.rsqrt(squares / D + epsilon)
        row = row[:, :v_end] * row_scale

        def by_head(start, size):
            return jnp.concatenate(
                [row[:, start + h * size : start + (h + 1) * size] for h in range(heads)], axis=0
            ).astype(jnp.bfloat16)

        query, key, value = by_head(0, dk), by_head(q_end, dk), by_head(k_end, dv)
        gates = jnp.broadcast_to(extra * row_scale, (heads, LANES))
        lane = lax.broadcasted_iota(jnp.int32, (heads, LANES), 1)
        head = lax.broadcasted_iota(jnp.int32, (heads, LANES), 0)

        def column(values, first):
            return jnp.sum(jnp.where(lane == head + first, values, 0.0), axis=1, keepdims=True)

        small = small_ref[...]
        block_input = small[:, dk : dk + SPAN_LOCATIONS]
        block_logf = small[:, dk + SPAN_LOCATIONS : dk + 2 * SPAN_LOCATIONS]
        state_max = small[:, dk + LANES : dk + LANES + 1]
        bias = small[:, dk + LANES + 1 : dk + LANES + 2]
        span = (heads, SPAN_LOCATIONS)
        live = jnp.broadcast_to(lengths_ref[:, :1] & (SPAN_LOCATIONS - 1), span)
        inside = lax.broadcasted_iota(jnp.int32, span, 1) < live
        rest = jnp.where(inside, block_logf, 0.0)
        square = (SPAN_LOCATIONS, SPAN_LOCATIONS)
        upto = (
            lax.broadcasted_iota(jnp.int32, square, 0) <= lax.broadcasted_iota(jnp.int32, square, 1)
        ).astype(jnp.float32).astype(jnp.bfloat16)
        cumulative = jnp.zeros(span, jnp.float32)
        for _ in range(3):
            term = rest.astype(jnp.bfloat16)
            rest = rest - term.astype(jnp.float32)
            cumulative = cumulative + jnp.dot(term, upto, preferred_element_type=jnp.float32)
        logf_sum = cumulative[:, SPAN_LOCATIONS - 1 :]
        cache_base = jnp.where(inside, logf_sum - cumulative + block_input, -jnp.inf)
        new_input = column(gates, half * heads)
        new_logf = jax.nn.log_sigmoid(column(gates, all_heads + half * heads) + bias)
        carried_log = logf_sum + new_logf + state_max
        cache_log = cache_base + new_logf
        stable = jnp.maximum(
            jnp.maximum(carried_log, jnp.max(cache_log, axis=1, keepdims=True)), new_input
        )
        carried_weight = jnp.exp(carried_log - stable)
        new_weight = jnp.exp(new_input - stable)
        cache_weight = jnp.exp(cache_log - stable)

        def pick(make, size):
            rows = lax.broadcasted_iota(jnp.int32, (heads, size), 0)
            out = jnp.zeros((heads, size), jnp.float32)
            for h in range(heads):
                out = jnp.where(rows == h, make(h), out)
            return out

        scores = pick(lambda h: dot_nt(query, keys_ref[0, h]), SPAN_LOCATIONS)
        mixing = (scores * scale * cache_weight).astype(jnp.bfloat16)
        query_wide = query.astype(jnp.float32)
        own_term = (
            jnp.sum(query_wide * key.astype(jnp.float32), axis=1, keepdims=True)
            * scale
            * new_weight
        )

        def carry(h):
            return dot_nt(query, state_ref[0, h].astype(jnp.bfloat16))

        carried = pick(carry, dv)
        from_cache = pick(
            lambda h: jnp.dot(
                mixing, values_ref[0, h], preferred_element_type=jnp.float32
            ), dv
        )
        numerator = carried_weight * carried + from_cache + own_term * value.astype(jnp.float32)
        normalizer = (
            carried_weight * jnp.sum(small[:, :dk] * query_wide, axis=1, keepdims=True)
            + jnp.sum(mixing.astype(jnp.float32), axis=1, keepdims=True)
            + own_term
        )
        divisor = jnp.maximum(jnp.maximum(jnp.abs(normalizer), jnp.exp(-stable)), 1.0)
        out_ref[...] = (numerator / divisor).astype(jnp.bfloat16)

    return call(
        body,
        [struct((heads, dv), jnp.bfloat16)],
        [VMEM_SPEC] * (count + 5),
        (
            *parts,
            small,
            resident(state_matrix),
            block_keys,
            block_values,
            jnp.pad(lengths, (0, LANES - 1)).reshape(1, -1),
        ),
    )[0]


def attend(pieces, out_weight):
    size = len(pieces)
    heads, dv = pieces[0].shape

    def body(*refs):
        weight_ref, out_ref, hidden_ref = refs[size:]
        position = lax.axis_index("kv")
        for n, d in enumerate([*distances(size), 0]):
            piece = refs[n][...].astype(jnp.float32)
            at = pl.ds(partner_of(position, size, d, True), 1)
            for h in range(heads):
                hidden_ref[at, h * dv : (h + 1) * dv] = piece[h : h + 1]
        out_ref[...] = jnp.dot(
            hidden_ref[...].astype(jnp.bfloat16),
            weight_ref[...],
            preferred_element_type=jnp.float32,
        ).astype(jnp.bfloat16)

    return call(
        body,
        [struct((size, out_weight.shape[1]), jnp.bfloat16)],
        [VMEM_SPEC] * (size + 1),
        (*pieces, resident(out_weight)),
        [pltpu.VMEM((size, heads * dv), jnp.float32)],
    )[0]


def add_features(refs, partners, gain_ref, up_ref, product, squares):
    size = lax.axis_size("kv")
    for ref, d in zip(refs, partners):
        columns = ref.shape[1]
        j = partner_of(lax.axis_index("kv"), size, d, True)
        at = pl.ds(pl.multiple_of(j * columns, columns), columns)
        wide = ref[...].astype(jnp.float32)
        squares = squares + jnp.sum(wide * wide, axis=1, keepdims=True)
        mixer_in = (wide * gain_ref[:, at]).astype(jnp.bfloat16)
        product = product + dot_nt(mixer_in, up_ref[:, at])
    return product, squares


def absorb(pieces, partners, mixer_gain, up_weight):
    rows = pieces[0].shape[0]
    units = up_weight.shape[0]
    count = len(pieces)

    def body(*refs):
        gain_ref, up_ref, product_ref, squares_ref = refs[count:]
        product, squares = add_features(
            refs[:count],
            partners,
            gain_ref,
            up_ref,
            jnp.zeros((rows, units), jnp.float32),
            jnp.zeros((rows, 1), jnp.float32),
        )
        product_ref[...] = product
        squares_ref[...] = jnp.broadcast_to(squares, (rows, LANES))

    return call(
        body,
        [struct((rows, units), jnp.float32), struct((rows, LANES), jnp.float32)],
        [VMEM_SPEC] * (count + 2),
        (*pieces, mixer_gain, up_weight),
        flops=20000000000,
    )


def mix(pieces, partners, before, mixer_gain, up_weight, down_weight):
    size = lax.axis_size("kv")
    count = len(pieces)
    rows, columns = pieces[0].shape
    blocks = around(size)
    units = up_weight.shape[0]

    def body(*refs):
        product_ref, squares_ref, gain_ref, up_ref, down_ref, *outs = refs[count:]
        position = lax.axis_index("kv")
        product, squares = add_features(
            refs[:count], partners, gain_ref, up_ref, product_ref[...], squares_ref[:, :1]
        )
        scaled = product * lax.rsqrt(squares / D + epsilon)
        activated = jnp.square(jnp.maximum(scaled, 0.0)).astype(jnp.bfloat16)
        outs[-2][...] = activated
        own = pl.ds(pl.multiple_of(position * columns, columns), columns)
        outs[-1][...] = down_ref[:, own]
        for n, d in enumerate(blocks):
            j = lax.rem(position + d, size)
            at = pl.ds(pl.multiple_of(j * columns, columns), columns)
            terms = jnp.dot(activated, down_ref[:, at], preferred_element_type=jnp.float32)
            outs[n][...] = terms.astype(outs[n].dtype)

    return call(
        body,
        [struct((rows, columns), jnp.bfloat16)] * len(blocks)
        + [
            struct((rows, units), jnp.bfloat16),
            struct((units, columns), down_weight.dtype),
        ],
        [VMEM_SPEC] * (count + 5),
        (*pieces, *before, mixer_gain, up_weight, down_weight),
        flops=20000000000,
    )


def mix_own(activated, residual, own_down):
    rows, columns = residual.shape
    share = columns // 2

    def body(activated_ref, residual_ref, down_ref, out_ref):
        terms = jnp.dot(activated_ref[...], down_ref[...], preferred_element_type=jnp.float32)
        half = lax.broadcasted_iota(jnp.int32, (rows, columns), 1) // share
        kept = residual_ref[...].astype(jnp.float32)
        out_ref[...] = terms + jnp.where(half == lax.axis_index("tp"), kept, 0.0)

    return call(
        body,
        [struct((rows, columns), jnp.float32)],
        [VMEM_SPEC] * 3,
        (activated, residual, own_down),
        flops=1000000,
    )[0]


def exchange_pairs(size, cores, distance, ring):
    chips = partner_pairs(size, distance)
    if ring:
        chips = [(i, (i + distance) % size) for i in range(size)]
    return [
        (i * cores + t, j * cores + (cores - 1 - t))
        for i, j in chips
        for t in range(cores)
    ]


def around(size):
    return [*range(1, size)]


def distances(size):
    return [*range(size // 2, size), *range(1, size // 2)]


def to_partners(outgoing, partners, ring=False):
    size, cores = lax.axis_size("kv"), lax.axis_size("tp")
    received = []
    for d in partners:
        pairs = exchange_pairs(size, cores, d, ring)
        received.append(lax.ppermute(outgoing[d], ("kv", "tp"), pairs))
    return received


def swapped(array):
    return lax.ppermute(array, "tp", [(0, 1), (1, 0)])


def direct(mesh, arrays_shape):
    size, cores = mesh["kv"], mesh["tp"]
    sequences, features = arrays_shape
    groups = mesh["dp"] * size
    return (
        2 < size <= DIRECT_LIMIT
        and cores == 2
        and sequences == groups
        and features % (size * 2 * LANES) == 0
    )


def shards_direct(
    tokens,
    norm_gain,
    query_weight,
    key_weight,
    value_weight,
    gate_weight,
    forget_bias,
    state_matrix,
    state_normalizer,
    state_max,
    block_keys,
    block_values,
    block_input,
    block_logf,
    lengths,
    out_weight,
    mixer_gain,
    up_weight,
    down_weight,
):
    head_half = lax.axis_index("tp")
    size = lax.axis_size("kv")
    order = distances(size)
    state_matrix = swapped(state_matrix)
    *parts, small = project(
        tokens,
        norm_gain,
        query_weight,
        key_weight,
        value_weight,
        gate_weight,
        forget_bias,
        state_normalizer,
        state_max,
        block_input,
        block_logf,
    )
    parts = to_partners(parts, [*order, 0])
    hidden = recall(
        parts, swapped(small), state_matrix, swapped(block_keys), swapped(block_values), lengths
    )
    pieces = to_partners([hidden] * size, [*order, 0])
    partial_out = attend(pieces, out_weight)
    other_out = swapped(partial_out)
    attended = partial_out.astype(jnp.float32) + other_out.astype(jnp.float32)
    residual = (tokens.astype(jnp.float32) + attended).astype(jnp.bfloat16)
    gain = mixer_gain.reshape(1, -1)
    pieces = to_partners([residual] * size, order)
    order = distances(size)
    up_weight, down_weight = resident(up_weight), resident(down_weight)
    absorbed = absorb([residual, pieces[0]], [0, order[0]], gain, up_weight)
    *terms, activated, own_down = mix(
        pieces[1:], order[1:], absorbed, gain, up_weight, down_weight
    )
    own = mix_own(activated, residual, own_down)
    steps = around(size)
    outgoing = dict(zip(steps, terms))
    total = own
    for term in to_partners(outgoing, steps, True):
        total = total + term.astype(jnp.float32)
    share = tokens.shape[1] // 2
    other = lax.dynamic_slice_in_dim(total, (1 - head_half) * share, share, 1)
    kept = lax.dynamic_slice_in_dim(total, head_half * share, share, 1)
    return (kept + swapped(other)).astype(jnp.bfloat16)


def mapped(mesh, function):
    return jax.shard_map(
        function,
        mesh=mesh,
        in_specs=(
            P("dp", "kv"),
            P("kv"),
            P("kv", "tp"),
            P("kv", "tp"),
            P("kv", "tp"),
            P(),
            P("tp"),
            P(("dp", "kv"), "tp", None, None),
            P(("dp", "kv"), "tp", None),
            P(("dp", "kv"), "tp"),
            P(("dp", "kv"), "tp", None, None),
            P(("dp", "kv"), "tp", None, None),
            P(("dp", "kv"), "tp", None),
            P(("dp", "kv"), "tp", None),
            P(("dp", "kv")),
            P("tp", "kv"),
            P(),
            P(("kv", "tp"), None),
            P(("kv", "tp"), None),
        ),
        out_specs=P("dp", ("kv", "tp")),
        check_vma=False,
    )


def solution(mesh):
    sizes = dict(mesh.shape)

    def whole(*arrays):
        return mapped(mesh, shards_general)(*arrays)

    def small(*arrays):
        if not direct(sizes, arrays[0].shape):
            return whole(*arrays)
        return mapped(mesh, shards_direct)(*arrays)

    if not 2 < sizes["kv"] <= DIRECT_LIMIT:
        return whole
    return small
```
